512 devices in a mesh: ep: 32 (over z, core), tp: 16 (over y, x).
Axes of the slice: x: 4, y: 4, z: 16, core: 2. Of those that a mesh axis runs over, the one named last changes fastest.
Arguments:
- receptance: bfloat16 [8192, 2048], P('ep', 'tp'), may hold values from -6 to 6
- key_tensor: bfloat16 [8192, 2048], P('ep', 'tp'), may hold values from -6 to 6
- value_tensor: bfloat16 [8192, 2048], P('ep', 'tp'), may hold values from -6 to 6
- decay_data_input: bfloat16 [8192, 2048], P('ep', 'tp'), may hold values from -4 to 4
- correction_rate_input: bfloat16 [8192, 2048], P('ep', 'tp'), may hold values from -16 to 6
- mixer_output_gate: bfloat16 [8192, 2048], P('ep', 'tp'), may hold values from -6 to 6
- decay_channel_offset: float32 [2048], P('tp'), may hold values from -16 to -3
- head_norm_gain: float32 [2048], P('tp'), may hold values from 0.1 to 1.9
- self_key_weight: float32 [2048], P('tp'), may hold values from -2 to 2
- mixer_output_weight: bfloat16 [2048, 2048], P('tp'), may hold values from -0.125 to 0.125
- second_batch_rows: bfloat16 [4096, 2048], P('ep'), may hold values from -6 to 6
- routed_expert_index: int32 [4096, 4], P('ep'), may hold values from 0 to 31, all different within a row; in each aligned block of 128 rows (0 to 127, 128 to 255, ...) at most 24 rows name the same one
- routing_output_weight: float32 [4096, 4], P('ep'), may hold values from 0.1 to 1
- expert_norm_gain: float32 [2048], replicated, may hold values from 0.1 to 1.9
- expert_gate_weight: bfloat16 [32, 1024, 2048], P('ep', 'tp'), may hold values from -0.125 to 0.125
- expert_up_weight: bfloat16 [32, 1024, 2048], P('ep', 'tp'), may hold values from -0.125 to 0.125
- expert_down_weight: bfloat16 [32, 1024, 2048], P('ep', None, 'tp'), may hold values from -0.1875 to 0.1875
- common_expert_gate: bfloat16 [1024, 2048], P('tp'), may hold values from -0.125 to 0.125
- common_expert_up: bfloat16 [1024, 2048], P('tp'), may hold values from -0.125 to 0.125
- common_expert_down: bfloat16 [1024, 2048], P(None, 'tp'), may hold values from -0.1875 to 0.1875
Outputs:
- token_mixer_output: bfloat16 [8192, 2048], P(('ep', 'tp'))
- expert_out: bfloat16 [4096, 2048], P('ep', 'tp')
The draws below stay inside these ranges and needn't reach their ends.
Inputs may be any that keep to these rules, and one draw needn't show every extreme that they name: `routed_expert_index`: each row names 4 different experts. Within the rows of one index of ep no expert is named by more than 24 rows, and that bound is met in some index's rows.
All inputs are finite; a program needn't handle non-finite values.
Results may differ from the reference program's by a relative error of at most 0.017.
Values may be sent and summed in bfloat16 or wider, within the bound.
A program may use at most 64 MiB of HBM per device.

```python
import math
import jax
import jax.numpy as jnp
import numpy as np
from jax import lax

MODEL_WIDTH = 2048
HEADS = 32
HEAD_CHANNELS = 64
FF = 1024
TOP = 4
ROWS_EXP = 128
SEQ_MIX = 8192
TOKENS_EXP = 4096
EXPERTS = 32
CAP = 24
N_EP = 32
N_TP = 16


def slow_marks(key):
    picks = jax.random.randint(jax.random.fold_in(key, 7), (HEADS,), 0, 10)
    return picks < 5


def draw_decay_channel_offset(key, part):
    slow_heads = slow_marks(key)
    spread = jax.random.uniform(jax.random.fold_in(key, 11), (HEADS, HEAD_CHANNELS), jnp.float32)
    slow_base = jnp.log(0.4 / SEQ_MIX) + 0.5 - spread
    fast_base = -4.0 + spread
    return jnp.where(slow_heads[:, None], slow_base, fast_base).reshape(MODEL_WIDTH).astype(jnp.float32)


def draw_correction_rate_input(key, part):
    slow_heads = slow_marks(key)
    offset = jnp.where(slow_heads, jnp.log(0.3 * HEAD_CHANNELS / SEQ_MIX), 0.0)
    jitter = jnp.clip(jax.random.normal(jax.random.fold_in(key, 13), (SEQ_MIX, HEADS, HEAD_CHANNELS), jnp.float32), -6.0, 6.0)
    return (jitter + offset[None, :, None]).reshape(SEQ_MIX, MODEL_WIDTH).astype(jnp.bfloat16)


def draw_decay_data_input(key, part):
    blocks = SEQ_MIX // 64
    shifts = jax.random.uniform(jax.random.fold_in(key, 17), (blocks, 1, MODEL_WIDTH), jnp.float32, -1.0, 1.0)
    jitter = 0.6 * jnp.clip(jax.random.normal(jax.random.fold_in(key, 19), (blocks, 64, MODEL_WIDTH), jnp.float32), -5.0, 5.0)
    return (jitter + shifts).reshape(SEQ_MIX, MODEL_WIDTH).astype(jnp.bfloat16)


def level_of(own_key, shape, shards, least, top_value):
    loudness, own = 1.0, jax.random.fold_in(own_key, 6)
    for axis_at, blocks in shards:
        draws = jnp.exp(jax.random.uniform(jax.random.fold_in(own, axis_at), (blocks,), jnp.float32, least / len(shards), top_value / len(shards)))
        loudness = loudness * jnp.repeat(draws, shape[axis_at] // blocks).reshape([-1 if axis == axis_at else 1 for axis in range(len(shape))])
    return loudness


def deal_out(own_key, own, number, rows, count, top, reach, slope):
    order = jax.random.permutation(own_key, count)
    crowded, ordinary = portions_of(count, rows * top, reach, slope, True), portions_of(count, rows * top, reach, slope, False)
    places = jnp.arange(count)

    def named(lengths, rotation):
        used = int((lengths > 0).sum())
        fixed = max(1, used // 4)
        moved = fixed + (places - fixed + rotation * (used - fixed)) % max(1, count - fixed)
        return jnp.zeros((count,), jnp.int32).at[order[jnp.where(places < fixed, places, moved)]].set(jnp.asarray(lengths, jnp.int32))

    lengths = jnp.where(number % 4 == 0, named(crowded, number // 4), named(ordinary, number - number // 4 - 1))
    mixed = jax.random.permutation(jax.random.fold_in(own, 3), count)
    source_of, taker = mixed[0:count // 2 * 2:2], mixed[1:count // 2 * 2:2]
    slack = jnp.minimum(lengths[source_of] - 1, reach - lengths[taker]) // 2
    slack = jnp.where((source_of == order[0]) | (taker == order[0]) | (lengths[taker] == 0), 0, jnp.maximum(slack, 0))
    moved = jax.random.randint(jax.random.fold_in(own, 4), (count // 2,), 0, 1 << 20) % (slack + 1)
    lengths = lengths.at[source_of].add(-moved).at[taker].add(moved)
    labels = jnp.searchsorted(jnp.cumsum(lengths), jnp.arange(rows * top), side="right").astype(jnp.int32)
    grid = labels.reshape(top, rows).T
    grid = grid[jax.random.permutation(jax.random.fold_in(own, 1), rows)]
    rotation = jax.random.randint(jax.random.fold_in(own, 2), (rows, 1), 0, top)
    return jnp.take_along_axis(grid, (jnp.arange(top)[None, :] + rotation) % top, axis=1)


def portions_of(amount, total, bound, skew, full):
    loads = [(1 << 20) // math.isqrt(grade ** skew) + 1 for grade in range(1, amount + 1)]
    largest = bound if full else min(bound, max(-(-total // amount), total * loads[0] // sum(loads)))
    least = 1 if total - largest >= amount - 1 else 0
    given, rest = [largest] + [least] * (amount - 1), total - largest - least * (amount - 1)
    while rest > 0:
        candidates = [i for i in range(1, amount) if given[i] < largest] or [i for i in range(1, amount) if given[i] < bound]
        whole, budget = sum([loads[i] for i in candidates]), rest
        for i in candidates:
            extra = min(bound - given[i], max(1, budget * loads[i] // whole), rest)
            given[i] = given[i] + extra
            rest = rest - extra
    return np.array(given)


def noise(own_key, extent, deviation, bound, cuts=(), kind=jnp.bfloat16):
    gain = level_of(own_key, extent, cuts, -0.22, 0.18) if cuts else 1.0
    values = jax.random.normal(own_key, extent, jnp.float32) * deviation * gain
    return jnp.minimum(jnp.maximum(values, -bound), bound).astype(kind)


def setup_inputs(seed: int = 0) -> dict:
    keys = jax.random.split(jax.random.key(seed), 21)
    receptance = noise(keys[0], (SEQ_MIX, MODEL_WIDTH), 1.0, 6.0, ((0, 32), (1, 16)))
    key_tensor = noise(keys[1], (SEQ_MIX, MODEL_WIDTH), 1.0, 6.0, ((0, 32), (1, 16)))
    value_tensor = noise(keys[2], (SEQ_MIX, MODEL_WIDTH), 1.0, 6.0, ((0, 32), (1, 16)))
    decay_data_input = draw_decay_data_input(jax.random.fold_in(keys[20], 71), 0)
    correction_rate_input = draw_correction_rate_input(jax.random.fold_in(keys[20], 71), 0)
    mixer_output_gate = noise(keys[5], (SEQ_MIX, MODEL_WIDTH), 1.0, 6.0, ((0, 32), (1, 16)))
    decay_channel_offset = draw_decay_channel_offset(jax.random.fold_in(keys[20], 71), 0)
    head_norm_gain = jnp.clip(1.0 + 0.18 * jax.random.normal(keys[7], (MODEL_WIDTH,), jnp.float32), 0.1, 1.9)
    self_key_weight = noise(keys[8], (MODEL_WIDTH,), 0.15, 2.0, ((0, 16),), jnp.float32)
    mixer_output_weight = noise(keys[9], (MODEL_WIDTH, MODEL_WIDTH), MODEL_WIDTH ** -0.5, 0.125, ((0, 16),))
    second_batch_rows = noise(keys[10], (TOKENS_EXP, MODEL_WIDTH), 1.0, 6.0, ((0, 32),))
    routed_expert_index_keys = jax.random.split(jax.random.fold_in(keys[11], 1), TOKENS_EXP // ROWS_EXP)
    routed_expert_index_turns = jax.random.permutation(jax.random.fold_in(keys[11], 3), TOKENS_EXP // ROWS_EXP)
    routed_expert_index = jax.vmap(lambda own, number: deal_out(jax.random.fold_in(keys[11], 2), own, number, ROWS_EXP, EXPERTS, TOP, CAP, 1))(routed_expert_index_keys, routed_expert_index_turns).reshape((TOKENS_EXP, TOP))
    routing_output_weight = jnp.clip(0.1 + 0.9 * jax.random.uniform(keys[12], (TOKENS_EXP, TOP), jnp.float32) ** level_of(keys[12], (TOKENS_EXP, TOP), ((0, 32),), -0.2, 0.2), 0.1, 1.0)
    expert_norm_gain = jnp.clip(1.0 + 0.18 * jax.random.normal(keys[13], (MODEL_WIDTH,), jnp.float32), 0.1, 1.9)
    expert_gate_weight = noise(keys[14], (EXPERTS, FF, MODEL_WIDTH), MODEL_WIDTH ** -0.5, 0.125, ((0, 32), (1, 16)))
    expert_up_weight = noise(keys[15], (EXPERTS, FF, MODEL_WIDTH), MODEL_WIDTH ** -0.5, 0.125, ((0, 32), (1, 16)))
    expert_down_weight = noise(keys[16], (EXPERTS, FF, MODEL_WIDTH), FF ** -0.5, 0.1875, ((0, 32), (2, 16)))
    common_expert_gate = noise(keys[17], (FF, MODEL_WIDTH), MODEL_WIDTH ** -0.5, 0.125, ((0, 16),))
    common_expert_up = noise(keys[18], (FF, MODEL_WIDTH), MODEL_WIDTH ** -0.5, 0.125, ((0, 16),))
    common_expert_down = noise(keys[19], (FF, MODEL_WIDTH), FF ** -0.5, 0.1875, ((1, 16),))
    return dict(receptance=receptance, key_tensor=key_tensor, value_tensor=value_tensor, decay_data_input=decay_data_input, correction_rate_input=correction_rate_input, mixer_output_gate=mixer_output_gate, decay_channel_offset=decay_channel_offset, head_norm_gain=head_norm_gain, self_key_weight=self_key_weight, mixer_output_weight=mixer_output_weight, second_batch_rows=second_batch_rows, routed_expert_index=routed_expert_index, routing_output_weight=routing_output_weight, expert_norm_gain=expert_norm_gain, expert_gate_weight=expert_gate_weight, expert_up_weight=expert_up_weight, expert_down_weight=expert_down_weight, common_expert_gate=common_expert_gate, common_expert_up=common_expert_up, common_expert_down=common_expert_down)


HIGHEST = lax.Precision.HIGHEST
NORM_FLOOR = 1.0

def decay_terms(decay_data_input, correction_rate_input, decay_channel_offset):
    pre_log = -jax.nn.softplus(-(decay_channel_offset + decay_data_input.astype(jnp.float32))) - 0.5
    return (jnp.exp(-jnp.exp(pre_log)), jax.nn.sigmoid(correction_rate_input.astype(jnp.float32)))

def head_view(matrix):
    return matrix.astype(jnp.float32).reshape(matrix.shape[0], -1, HEAD_CHANNELS)

def complete_head_outputs(state_readout, receptance_rows, key_row_block, value_row_block, head_norm_gain, self_key_weight, mixer_output_gate):
    mean_part = lax.optimization_barrier(jnp.mean(state_readout, axis=-1, keepdims=True))
    spread = lax.optimization_barrier(jnp.mean(jnp.square(state_readout - mean_part), axis=-1, keepdims=True))
    normalized_rows = (state_readout - mean_part) * lax.rsqrt(spread + NORM_FLOOR)
    sequence_length = state_readout.shape[0]
    normalized_rows = normalized_rows.reshape(sequence_length, -1) * head_norm_gain
    self_key_term = lax.optimization_barrier(jnp.sum(receptance_rows * key_row_block * self_key_weight.reshape(-1, HEAD_CHANNELS), axis=-1, keepdims=True)) * value_row_block
    mixer_result = (normalized_rows + self_key_term.reshape(sequence_length, -1)) * mixer_output_gate.astype(jnp.float32)
    return mixer_result.astype(jnp.bfloat16)

def token_mixer_baseline(receptance, key_tensor, value_tensor, decay_data_input, correction_rate_input, mixer_output_gate, decay_channel_offset, head_norm_gain, self_key_weight, mixer_output_weight):
    decays, rates = decay_terms(decay_data_input, correction_rate_input, decay_channel_offset)
    receptance_rows = head_view(receptance)
    key_row_block = head_view(key_tensor)
    value_row_block = head_view(value_tensor)
    unit_keys = key_row_block * lax.rsqrt(lax.optimization_barrier(jnp.sum(key_row_block * key_row_block, axis=-1, keepdims=True)) + 1.0)
    decays = decays.reshape(key_row_block.shape)
    rates = rates.reshape(key_row_block.shape)

    def advance(memory, inputs):
        recept_now, decay_now, key_now, value_now, unit_now, rate_now = inputs
        projected = jnp.einsum('hij,hj->hi', memory, unit_now, precision=HIGHEST)
        memory = memory * decay_now[:, None, :] - projected[:, :, None] * (unit_now * rate_now)[:, None, :] + value_now[:, :, None] * key_now[:, None, :]
        return (memory, jnp.einsum('hij,hj->hi', memory, recept_now, precision=HIGHEST))
    head_count = key_row_block.shape[1]
    initial = jnp.zeros((head_count, HEAD_CHANNELS, HEAD_CHANNELS), jnp.float32)
    _, state_readout = lax.scan(advance, initial, (receptance_rows, decays, key_row_block, value_row_block, unit_keys, rates))
    mixer_result = complete_head_outputs(state_readout, receptance_rows, key_row_block, value_row_block, head_norm_gain, self_key_weight, mixer_output_gate)
    groups = mixer_result.reshape(SEQ_MIX, N_TP, MODEL_WIDTH // N_TP).transpose(1, 0, 2)
    weights = mixer_output_weight.reshape(N_TP, MODEL_WIDTH // N_TP, MODEL_WIDTH)

    def add_group(running, blocks):
        mixed_part, weight_part = blocks
        partial_sum = jnp.dot(mixed_part, weight_part, preferred_element_type=jnp.float32).astype(jnp.bfloat16)
        partial_sum = lax.optimization_barrier(partial_sum)
        return (running + partial_sum.astype(jnp.float32), None)
    summed, _ = lax.scan(add_group, jnp.zeros((SEQ_MIX, MODEL_WIDTH), jnp.float32), (groups, weights))
    return summed.astype(jnp.bfloat16)

def expert_unit(rows_in, gate_part, up_part, down_part):
    pre_gate = jnp.dot(rows_in, gate_part.T, preferred_element_type=jnp.float32)
    pre_up = jnp.dot(rows_in, up_part.T, preferred_element_type=jnp.float32)
    hidden = (jax.nn.silu(pre_gate) * pre_up).astype(jnp.bfloat16)
    return jnp.dot(hidden, down_part, preferred_element_type=jnp.float32)

def experts_reference(second_batch_rows, routed_expert_index, routing_output_weight, expert_norm_gain, expert_gate_weight, expert_up_weight, expert_down_weight, common_expert_gate, common_expert_up, common_expert_down):
    widened = second_batch_rows.astype(jnp.float32)
    normalized_rows = (widened * lax.rsqrt(lax.optimization_barrier(jnp.mean(widened * widened, axis=-1, keepdims=True)) + NORM_FLOOR) * expert_norm_gain).astype(jnp.bfloat16)
    shared_out = expert_unit(normalized_rows, common_expert_gate, common_expert_up, common_expert_down)
    flat_ids = routed_expert_index.reshape(-1).astype(jnp.int32)
    ordering = jnp.argsort(flat_ids, stable=True).astype(jnp.int32)
    counts = lax.optimization_barrier(jnp.sum((flat_ids[:, None] == jnp.arange(EXPERTS, dtype=jnp.int32)[None, :]).astype(jnp.int32), axis=0))
    firsts = (jnp.cumsum(counts) - counts).astype(jnp.int32)
    capacity = N_EP * CAP
    padded_order = jnp.concatenate([ordering, jnp.zeros((capacity,), jnp.int32)])
    flat_weights = routing_output_weight.reshape(-1)

    def visit(summed, expert):
        chosen = lax.dynamic_slice_in_dim(padded_order, firsts[expert], capacity)
        usable = jnp.arange(capacity) < counts[expert]
        tokens = chosen // TOP
        copies = expert_unit(normalized_rows[tokens], expert_gate_weight[expert], expert_up_weight[expert], expert_down_weight[expert]).astype(jnp.bfloat16)
        copies = lax.optimization_barrier(copies).astype(jnp.float32)
        factor = jnp.where(usable, flat_weights[chosen], 0.0)
        return (summed.at[tokens].add(copies * factor[:, None]), None)
    routed, _ = lax.scan(visit, jnp.zeros((TOKENS_EXP, MODEL_WIDTH), jnp.float32), jnp.arange(EXPERTS))
    return (routed + shared_out).astype(jnp.bfloat16)

def reference(receptance, key_tensor, value_tensor, decay_data_input, correction_rate_input, mixer_output_gate, decay_channel_offset, head_norm_gain, self_key_weight, mixer_output_weight, second_batch_rows, routed_expert_index, routing_output_weight, expert_norm_gain, expert_gate_weight, expert_up_weight, expert_down_weight, common_expert_gate, common_expert_up, common_expert_down):
    token_mixer_output = token_mixer_baseline(receptance, key_tensor, value_tensor, decay_data_input, correction_rate_input, mixer_output_gate, decay_channel_offset, head_norm_gain, self_key_weight, mixer_output_weight)
    expert_out = experts_reference(second_batch_rows, routed_expert_index, routing_output_weight, expert_norm_gain, expert_gate_weight, expert_up_weight, expert_down_weight, common_expert_gate, common_expert_up, common_expert_down)
    return (token_mixer_output, expert_out)
```

```python
import functools

import jax
import jax.numpy as jnp
from jax import lax
from jax.experimental import pallas as pl
from jax.experimental.pallas import tpu as pltpu
from jax.sharding import Mesh
from jax.sharding import PartitionSpec as P

F32 = jnp.float32
BF16 = jnp.bfloat16
HEAD = 64
CHUNK = 64
RING = 4
CAP = 24
EXPERTS = 32
SOURCES = 8
MESH = pl.DeviceIdType.MESH
EP = ("z", "c")
TP = ("y", "x")
NN = (((1,), (0,)), ((), ()))
NT = (((1,), (1,)), ((), ()))
TN = (((0,), (0,)), ((), ()))


def dot(a, b, dims=NN):
    return lax.dot_general(a, b, dims, preferred_element_type=F32)


def halves(a):
    high = a.astype(BF16)
    return high, (a - high.astype(F32)).astype(BF16)


def dot3(a, b, dims=NN):
    (ah, al), (bh, bl) = a, b
    return dot(ah, bh, dims) + (dot(ah, bl, dims) + dot(al, bh, dims))


def dot_exact_left(a, b):
    b1 = b.astype(BF16)
    rest = b - b1.astype(F32)
    b2 = rest.astype(BF16)
    b3 = (rest - b2.astype(F32)).astype(BF16)
    return dot(a, b1) + (dot(a, b2) + dot(a, b3))


def dot_exact_right(a, b):
    ah, al = halves(a)
    return dot(ah, b) + dot(al, b)


def iota(shape, dim):
    return lax.broadcasted_iota(jnp.int32, shape, dim)


def copy_to(src, dst, send_sem, recv_sem, device):
    return pltpu.make_async_remote_copy(
        src_ref=src,
        dst_ref=dst,
        send_sem=send_sem,
        recv_sem=recv_sem,
        device_id=device,
        device_id_type=MESH,
    )


def silu(v):
    return v / (1.0 + jnp.exp(-v))


def local_mixer(rec_ref, key_ref, val_ref, dec_ref, rate_ref, off_ref, xg, yf, poll):
    n = 2 * CHUNK
    rows = rec_ref.shape[0]
    chunks = rows // CHUNK
    lane_head = iota((1, 128), 1) >> 6
    m0 = (lane_head == 0).astype(F32)
    m1 = 1.0 - m0
    same_head = ((iota((128, 128), 0) >> 6) == (iota((128, 128), 1) >> 6)).astype(BF16)
    i, j = iota((n, n), 0), iota((n, n), 1)
    eye = (i == j).astype(F32)
    same = (i >> 6) == (j >> 6)
    below = (i > j) & same
    upto = (i >= j) & same
    ri, rj = iota((rows, rows), 0), iota((rows, rows), 1)
    tri = ((ri >= rj) & ((ri >> 6) == (rj >> 6))).astype(F32).astype(BF16)

    key = key_ref[...].astype(F32)
    logw = -0.6065306597126334 / (1.0 + jnp.exp(-(off_ref[...] + dec_ref[...].astype(F32))))
    cum = dot_exact_left(tri, logw)
    rate = 1.0 / (1.0 + jnp.exp(-rate_ref[...].astype(F32)))
    unit = key * lax.rsqrt(dot_exact_right(key * key, same_head) + 1.0)
    b = unit * rate
    up = jnp.exp(cum)
    down = jnp.exp(-cum)
    u_t = unit * jnp.exp(cum - logw)
    r_t = rec_ref[...].astype(F32) * up
    k_t = key * down
    b_t = b * down
    value = val_ref[...].astype(F32)

    def part(a, at):
        return a[at * CHUNK : (at + 1) * CHUNK]

    def both(a):
        return jnp.concatenate([a * m0, a * m1], axis=0)

    every = range(chunks)
    end = [jnp.exp(part(cum, at)[CHUNK - 1 :]) for at in every]
    v2 = [both(part(value, at)) for at in every]
    v2h = [a.astype(BF16) for a in v2]
    u2 = [both(part(u_t, at)) for at in every]
    r2 = [both(part(r_t, at)) for at in every]
    b2 = [both(part(b_t, at)) for at in every]
    k2 = [both(part(k_t, at)) for at in every]
    left = [halves(jnp.concatenate([u2[at], r2[at]], axis=0)) for at in every]
    right = [halves(jnp.concatenate([b2[at], k2[at]], axis=0)) for at in every]
    pairs = [dot3(left[at], right[at], NT) for at in every]
    lower = [jnp.where(below, pairs[at][:n, :n], 0.0) for at in every]
    m_uk = [halves(jnp.where(below, pairs[at][:n, n:], 0.0)) for at in every]
    a_b = [halves(jnp.where(upto, pairs[at][n:, :n], 0.0)) for at in every]
    a_k = [halves(jnp.where(upto, pairs[at][n:, n:], 0.0)) for at in every]
    poll(0)
    mv = [dot(m_uk[at][0], v2h[at]) + dot(m_uk[at][1], v2h[at]) for at in every]
    akv = [dot(a_k[at][0], v2h[at]) + dot(a_k[at][1], v2h[at]) for at in every]
    inverse = None
    for level in range(6):
        half = (
            ((i >> (level + 1)) == (j >> (level + 1)))
            & (((i >> level) & 1) == 1)
            & (((j >> level) & 1) == 0)
        )
        step = [jnp.where(half, lower[at], 0.0) for at in every]
        if inverse is None:
            inverse = [eye - step[at] for at in every]
        else:
            split = [halves(inverse[at]) for at in every]
            mid = [dot3(halves(step[at]), split[at]) for at in every]
            inverse = [
                inverse[at] - dot3(split[at], halves(mid[at])) for at in every
            ]
    poll(1)
    ez = [
        halves(dot3(halves(inverse[at]), halves(jnp.concatenate([u2[at], mv[at]], axis=1))))
        for at in every
    ]
    aez = [dot3(a_b[at], ez[at]) for at in every]
    b_end = [halves(b2[at] * end[at]) for at in every]
    k_end = [halves(k2[at] * end[at]) for at in every]
    bez = [dot3(b_end[at], ez[at], TN) for at in every]
    kv = [dot(k_end[at][0], v2h[at], TN) + dot(k_end[at][1], v2h[at], TN) for at in every]
    poll(2)
    total = None
    for at in every:
        xo = r2[at] - aez[at][:, :128]
        yo = akv[at] - aez[at][:, 128:]
        xo = xo[:CHUNK] + xo[CHUNK:]
        yo = yo[:CHUNK] + yo[CHUNK:]
        moves = eye * end[at] - bez[at][:, :128]
        sums = kv[at] - bez[at][:, 128:]
        if total is None:
            xg[pl.ds(at * CHUNK, CHUNK), :] = xo
            yf[pl.ds(at * CHUNK, CHUNK), :] = yo
            total = jnp.concatenate([moves, sums], axis=1)
        else:
            ahead = halves(total)
            read = dot3(halves(xo), ahead)
            xg[pl.ds(at * CHUNK, CHUNK), :] = read[:, :128]
            yf[pl.ds(at * CHUNK, CHUNK), :] = read[:, 128:] + yo
            moved = dot3(halves(moves), ahead)
            total = jnp.concatenate([moved[:, :128], moved[:, 128:] + sums], axis=1)
    return total[:, :128], total[:, 128:]


def kernel(
    rec_ref,
    key_ref,
    val_ref,
    dec_ref,
    rate_ref,
    gate_ref,
    off_ref,
    gain_ref,
    self_ref,
    wout_hbm,
    rows_ref,
    idx_ref,
    wgt_ref,
    egain_ref,
    eg_hbm,
    eu_hbm,
    ed_hbm,
    cg_hbm,
    cu_hbm,
    cd_hbm,
    out0,
    out1,
    wout,
    gu,
    wd,
    cgu,
    cd,
    xn,
    sbuf,
    rbuf,
    hid,
    obuf,
    retb,
    pbuf,
    rcv,
    shb,
    q_hi,
    q_lo,
    onehot,
    xg,
    yf,
    cmap,
    pmap,
    zmine,
    zmap,
    sts,
    keep,
    ld,
    dsp_s,
    dsp_r,
    ys,
    yr,
    ws,
    wr,
    hs,
    hr,
    ret_s,
    ret_r,
    mx_s,
    mx_r,
    sh_s,
    sh_r,
    zs,
    zr,
    ps,
    pr,
):
    z, c = lax.axis_index("z"), lax.axis_index("c")
    y, x = lax.axis_index("y"), lax.axis_index("x")
    nz = lax.axis_size("z")
    ep, tp = 2 * z + c, RING * y + x
    home = ep % RING
    own = home == x
    mine = jnp.where(own, 1, 0)

    def at(z_=None, c_=None, y_=None, x_=None):
        return {
            "z": z if z_ is None else z_,
            "c": c if c_ is None else c_,
            "y": y if y_ is None else y_,
            "x": x if x_ is None else x_,
        }

    def place(e, y_=None, x_=None):
        return at(e // 2, e % 2, y_, x_)

    loads = [
        pltpu.make_async_copy(eg_hbm.at[0], gu.at[x, pl.ds(0, 64)], ld.at[0]),
        pltpu.make_async_copy(eu_hbm.at[0], gu.at[x, pl.ds(64, 64)], ld.at[1]),
        pltpu.make_async_copy(ed_hbm.at[0], wd.at[x], ld.at[2]),
        pltpu.make_async_copy(cg_hbm, cgu.at[pl.ds(0, 64)], ld.at[3]),
        pltpu.make_async_copy(cu_hbm, cgu.at[pl.ds(64, 64)], ld.at[4]),
        pltpu.make_async_copy(cd_hbm, cd, ld.at[5]),
        pltpu.make_async_copy(wout_hbm, wout, ld.at[6]),
    ]
    for load in loads:
        load.start()

    barrier = pltpu.get_barrier_semaphore()

    def tell(device):
        pl.semaphore_signal(barrier, inc=1, device_id=device, device_id_type=MESH)

    def tell_plane(k, _):
        @pl.when(k != tp)
        def _():
            tell(at(y_=k // RING, x_=k % RING))

        return 0

    lax.fori_loop(0, 16, tell_plane, 0)
    tell(at(c_=1 - c))

    def tell_later(k, _):
        tell(at(z_=k))
        return 0

    lax.fori_loop(0, z, tell_later, 0)

    def tell_source(k, _):
        @pl.when(RING * k + x != ep)
        def _():
            tell(place(RING * k + x))

        return 0

    lax.fori_loop(0, SOURCES, tell_source, 0)

    def tell_expert(e, _):
        @pl.when(jnp.logical_not((e == ep) & own))
        def _():
            tell(place(e, x_=home))

        return 0

    lax.fori_loop(0, EXPERTS, tell_expert, 0)

    rows = rows_ref[...].astype(F32)
    scale = lax.rsqrt(jnp.mean(rows * rows, axis=-1, keepdims=True) + 1.0)
    xn[...] = (rows * scale * egain_ref[...]).astype(BF16)

    row_count = rows_ref.shape[0]
    slots = EXPERTS * CAP
    lane_e = iota((row_count, EXPERTS), 1)
    chosen = jnp.zeros((row_count, EXPERTS), F32)
    weight = jnp.zeros((row_count, EXPERTS), F32)
    for k in range(4):
        hit = idx_ref[:, k : k + 1] == lane_e
        chosen = jnp.where(hit, 1.0, chosen)
        weight = jnp.where(hit, wgt_ref[:, k : k + 1], weight)
    earlier = (iota((row_count, row_count), 0) > iota((row_count, row_count), 1))
    rank = dot(earlier.astype(F32).astype(BF16), chosen.astype(BF16))
    label = jnp.where(chosen > 0.0, rank, -1.0).astype(BF16)
    slot_e, slot_s = iota((EXPERTS, slots), 0), iota((EXPERTS, slots), 1)
    spread = ((slot_s >= slot_e * CAP) & (slot_s < slot_e * CAP + CAP)).astype(F32)
    within = jnp.sum(spread * (slot_s - slot_e * CAP).astype(F32), axis=0, keepdims=True)
    spread = spread.astype(BF16)
    placed = (dot(label, spread) == within).astype(F32)
    w_hi, w_lo = halves(weight)
    q_hi[...] = (placed * dot(w_hi, spread)).astype(BF16)
    q_lo[...] = (placed * dot(w_lo, spread)).astype(BF16)

    onehot[...] = placed.astype(BF16)

    @pl.when(own)
    def _():
        features = xn[:, pl.ds(pl.multiple_of(512 * y, 512), 512)]
        packed = dot(onehot[...], features, TN)
        sbuf[...] = packed.reshape(EXPERTS, CAP, 512).astype(BF16)
        rbuf[y, ep // RING] = sbuf[ep]

    pl.semaphore_wait(barrier, 15 + 1 + (nz - 1 - z) + 31 * mine + 32 - mine)

    def dispatch(e):
        return copy_to(
            sbuf.at[e], rbuf.at[y, ep // RING], dsp_s.at[e], dsp_r.at[ep // RING], place(e)
        )

    @pl.when(own)
    def _():
        def send(k, _):
            dispatch((ep + k) % EXPERTS).start()
            return 0

        lax.fori_loop(1, EXPERTS, send, 0)

    def ring(piece, first_half, send_sem, recv_sem, p, axis):
        me = y if axis == "y" else x
        right, left, across = (me + 1) % RING, (me + 3) % RING, (me + 2) % RING

        def move(slot, way, to):
            device = at(y_=to) if axis == "y" else at(x_=to)
            return copy_to(piece(slot), piece(slot), send_sem.at[way, p], recv_sem.at[way, p], device)

        def start():
            move(me, 0, right).start()
            move(me, 1, left).start()

        def relay():
            if first_half:
                move(left, 0, right).wait_recv()
                move(left, 2, right).start()
            else:
                move(right, 1, left).wait_recv()
                move(right, 2, left).start()

        def near():
            if first_half:
                move(right, 1, left).wait_recv()
            else:
                move(left, 0, right).wait_recv()

        def far():
            move(across, 2, right).wait_recv()

        def sent():
            for way in range(3):
                move(me, way, right).wait_send()

        return start, relay, near, far, sent

    weights = [
        ring(lambda s: gu.at[s, pl.ds(0, 64)], True, ws, wr, 0, "x"),
        ring(lambda s: gu.at[s, pl.ds(64, 64)], False, ws, wr, 1, "x"),
        ring(lambda s: wd.at[s, pl.ds(0, 512)], True, ws, wr, 2, "x"),
        ring(lambda s: wd.at[s, pl.ds(512, 512)], False, ws, wr, 3, "x"),
    ]
    row_ring = [
        ring(lambda s, k=k: rbuf.at[s, k], k < SOURCES // 2, ys, yr, k, "y")
        for k in range(SOURCES)
    ]
    hid_ring = [
        ring(lambda s: hid.at[s, pl.ds(0, 96)], True, hs, hr, 0, "y"),
        ring(lambda s: hid.at[s, pl.ds(96, 96)], False, hs, hr, 1, "y"),
    ]
    for load in loads[:3]:
        load.wait()
    weights[0][0]()
    weights[1][0]()

    for load in loads[3:]:
        load.wait()
    pre = dot(cgu[...], xn[...], NT)
    shb[tp] = (silu(pre[:64]) * pre[64:]).astype(BF16)

    def share(k):
        return copy_to(
            shb.at[tp], shb.at[tp], sh_s.at[k], sh_r.at[tp], at(y_=k // RING, x_=k % RING)
        )

    def share_send(k, _):
        share((tp + k) % 16).start()
        return 0

    lax.fori_loop(1, 16, share_send, 0)

    def forward_rows():
        for k in range(SOURCES):
            @pl.when(RING * k + x != ep)
            def _():
                copy_to(
                    rbuf.at[y, k], rbuf.at[y, k], dsp_s.at[0], dsp_r.at[k], place(RING * k + x)
                ).wait_recv()

            row_ring[k][0]()

    def poll(stage):
        if stage == 0:
            pass
        elif stage == 1:
            weights[0][1]()
            weights[1][1]()
            weights[2][0]()
            weights[3][0]()
        else:
            forward_rows()

    moves, sums = local_mixer(
        rec_ref, key_ref, val_ref, dec_ref, rate_ref, off_ref, xg, yf, poll
    )
    cmap[0] = moves[:64] + pltpu.roll(sums[:64], 64, 1)
    cmap[1] = pltpu.roll(moves[64:], 64, 1) + sums[64:]

    swap = copy_to(cmap.at[1 - c], pmap, ps.at[0], pr.at[0], at(c_=1 - c))
    swap.start()
    for ring_of in row_ring:
        ring_of[1]()
    swap.wait_recv()
    lane = iota((64, 128), 1)
    first = jnp.where(c == 0, cmap[0], pmap[...])
    second = jnp.where(c == 0, pmap[...], cmap[1])

    def compose(later, earlier):
        stacked = jnp.concatenate([earlier, jnp.zeros_like(earlier)], axis=0)
        moved = dot3(halves(jnp.where(lane < 64, later, 0.0)), halves(stacked))
        return moved + jnp.where(lane < 64, 0.0, later)

    zmine[...] = compose(second, first).astype(BF16)

    def to_later(k):
        return copy_to(zmine, zmap.at[z], zs.at[k], zr.at[z], at(z_=k))

    def send_later(k, _):
        to_later(k).start()
        return 0

    lax.fori_loop(z + 1, nz, send_later, 0)

    weights[0][2]()
    weights[1][2]()
    weights[0][3]()
    weights[1][3]()

    def product(slot):
        taken = rbuf[slot].astype(F32).reshape(SOURCES * CAP, 512).astype(BF16)
        span = pl.ds(pl.multiple_of(512 * slot, 512), 512)
        g = gu[:, 0:64, span].reshape(256, 512)
        u = gu[:, 64:128, span].reshape(256, 512)
        return dot(taken, g, NT), dot(taken, u, NT)

    g0, u0 = product(y)
    for ring_of in row_ring:
        ring_of[2]()
    g1, u1 = product((y + 1) % RING)
    g2, u2 = product((y + 3) % RING)
    for ring_of in row_ring:
        ring_of[3]()
    g3, u3 = product((y + 2) % RING)
    hidden = silu((g0 + g1) + (g2 + g3)) * ((u0 + u1) + (u2 + u3))
    hid[y] = hidden.astype(BF16)
    hid_ring[0][0]()
    hid_ring[1][0]()
    weights[2][1]()
    weights[3][1]()

    keep[...] = jnp.zeros((64, 128), F32)

    def advance(k, _):
        copy_to(zmine, zmap.at[k], zs.at[0], zr.at[k], at(z_=k)).wait_recv()
        step = zmap[k].astype(F32)
        low = jnp.where(lane < 64, step, 0.0)
        twice = (low + pltpu.roll(low, 64, 1)).astype(BF16)
        s_hi, s_lo = halves(keep[...])
        moved = dot(twice, jnp.concatenate([s_hi, s_lo], axis=0))
        keep[...] = moved + jnp.where(lane < 64, 0.0, step)
        return 0

    lax.fori_loop(0, z, advance, 0)
    state = keep[...]
    passed = jnp.where(lane < 64, 0.0, compose(first, state))
    sts[c] = jnp.where(c == 0, state, passed)
    keep[...] = jnp.where(c == 0, passed, state)
    hand = copy_to(keep, sts.at[c], ps.at[1], pr.at[1], at(c_=1 - c))
    hand.start()
    hid_ring[0][1]()
    hid_ring[1][1]()
    copy_to(keep, sts.at[1 - c], ps.at[1], pr.at[1], at(c_=1 - c)).wait_recv()

    start = jnp.concatenate([pltpu.roll(sts[0], 64, 1), sts[1]], axis=0)
    readout = dot3(halves(xg[...]), halves(start)) + yf[...]
    same_head = ((iota((128, 128), 0) >> 6) == (iota((128, 128), 1) >> 6)).astype(F32)
    mean_of = (same_head * (1.0 / HEAD)).astype(BF16)
    same_head = same_head.astype(BF16)
    centred = readout - dot_exact_right(readout, mean_of)
    variance = dot_exact_right(centred * centred, mean_of)
    key = key_ref[...].astype(F32)
    bonus = dot_exact_right(rec_ref[...].astype(F32) * key * self_ref[...], same_head)
    mixed = (
        centred * lax.rsqrt(variance + 1.0) * gain_ref[...] + bonus * val_ref[...].astype(F32)
    ) * gate_ref[...].astype(F32)
    mixed = mixed.astype(BF16)

    def give(k):
        return copy_to(
            pbuf.at[k], rcv.at[tp], mx_s.at[k], mx_r.at[tp], at(y_=k // RING, x_=k % RING)
        )

    for group in range(4):
        partial = dot(mixed[64 * group : 64 * group + 64], wout[...])
        pbuf[4 * group : 4 * group + 4] = partial.reshape(4, 16, 2048).astype(BF16)
        for k in range(4 * group, 4 * group + 4):
            @pl.when(k != tp)
            def _():
                give(k).start()

    rcv[tp] = pbuf[tp]

    weights[2][2]()
    weights[3][2]()
    weights[2][3]()
    weights[3][3]()
    for ring_of in hid_ring:
        ring_of[2]()
        ring_of[3]()
    for s in range(RING):
        made = dot(hid[0], wd[s, 0:256])
        for part in range(1, RING):
            made = made + dot(hid[part], wd[s, 256 * part : 256 * part + 256])
        obuf[s] = made.reshape(SOURCES, CAP, 128).astype(BF16)

    def give_back(k, s):
        return copy_to(
            obuf.at[s, k],
            retb.at[ep],
            ret_s.at[RING * k + s],
            ret_r.at[ep],
            place(RING * k + x, x_=s),
        )

    def send_back(n, _):
        k, s = n // RING, n % RING
        @pl.when(jnp.logical_not((RING * k + x == ep) & (s == x)))
        def _():
            give_back(k, s).start()

        return 0

    lax.fori_loop(0, EXPERTS, send_back, 0)

    @pl.when(own)
    def _():
        retb[ep] = obuf[x, ep // RING]

    def take(k, _):
        copy_to(
            pbuf.at[0], rcv.at[k], mx_s.at[0], mx_r.at[k], at(y_=k // RING, x_=k % RING)
        ).wait_recv()
        return 0

    def take_other(k, _):
        @pl.when(k != tp)
        def _():
            take(k, 0)

        return 0

    lax.fori_loop(0, 16, take_other, 0)
    summed = rcv[0].astype(F32)
    for k in range(1, 16):
        summed = summed + rcv[k].astype(F32)
    out0[...] = summed.astype(BF16)

    def shared_in(k, _):
        @pl.when(k != tp)
        def _():
            copy_to(
                shb.at[k], shb.at[k], sh_s.at[0], sh_r.at[k], at(y_=k // RING, x_=k % RING)
            ).wait_recv()

        return 0

    lax.fori_loop(0, 16, shared_in, 0)
    shared = dot(shb[...].reshape(1024, 128), cd[...], TN)

    def back_in(e, _):
        @pl.when(jnp.logical_not((e == ep) & own))
        def _():
            copy_to(
                retb.at[e], retb.at[e], ret_s.at[0], ret_r.at[e], place(e, x_=home)
            ).wait_recv()

        return 0

    lax.fori_loop(0, EXPERTS, back_in, 0)
    copies = retb[...].astype(F32).reshape(slots, 128).astype(BF16)
    merged = dot(q_hi[...], copies) + dot(q_lo[...], copies) + shared
    out1[...] = merged.astype(BF16)

    @pl.when(own)
    def _():
        def sent(k, _):
            dispatch((ep + k) % EXPERTS).wait_send()
            return 0

        lax.fori_loop(1, EXPERTS, sent, 0)

    for ring_of in weights + row_ring + hid_ring:
        ring_of[4]()
    swap.wait_send()
    hand.wait_send()

    def later_sent(k, _):
        to_later(k).wait_send()
        return 0

    lax.fori_loop(z + 1, nz, later_sent, 0)

    def plane_sent(k, _):
        @pl.when(k != tp)
        def _():
            give(k).wait_send()
            share(k).wait_send()

        return 0

    lax.fori_loop(0, 16, plane_sent, 0)

    def back_sent(n, _):
        k, s = n // RING, n % RING
        @pl.when(jnp.logical_not((RING * k + x == ep) & (s == x)))
        def _():
            give_back(k, s).wait_send()

        return 0

    lax.fori_loop(0, EXPERTS, back_sent, 0)


def on_device(
    receptance,
    key_tensor,
    value_tensor,
    decay_data_input,
    correction_rate_input,
    mixer_output_gate,
    decay_channel_offset,
    head_norm_gain,
    self_key_weight,
    mixer_output_weight,
    second_batch_rows,
    routed_expert_index,
    routing_output_weight,
    expert_norm_gain,
    expert_gate_weight,
    expert_up_weight,
    expert_down_weight,
    common_expert_gate,
    common_expert_up,
    common_expert_down,
):
    vmem = pl.BlockSpec(memory_space=pltpu.VMEM)
    hbm = pl.BlockSpec(memory_space=pl.ANY)
    dma = pltpu.SemaphoreType.DMA
    scratch = [
        pltpu.VMEM((128, 2048), BF16),
        pltpu.VMEM((RING, 128, 2048), BF16),
        pltpu.VMEM((RING, 1024, 128), BF16),
        pltpu.VMEM((128, 2048), BF16),
        pltpu.VMEM((1024, 128), BF16),
        pltpu.VMEM((128, 2048), BF16),
        pltpu.VMEM((EXPERTS, CAP, 512), BF16),
        pltpu.VMEM((RING, SOURCES, CAP, 512), BF16),
        pltpu.VMEM((RING, SOURCES * CAP, 256), BF16),
        pltpu.VMEM((RING, SOURCES, CAP, 128), BF16),
        pltpu.VMEM((EXPERTS, CAP, 128), BF16),
        pltpu.VMEM((16, 16, 2048), BF16),
        pltpu.VMEM((16, 16, 2048), BF16),
        pltpu.VMEM((16, 64, 128), BF16),
        pltpu.VMEM((128, EXPERTS * CAP), BF16),
        pltpu.VMEM((128, EXPERTS * CAP), BF16),
        pltpu.VMEM((128, EXPERTS * CAP), BF16),
        pltpu.VMEM((256, 128), F32),
        pltpu.VMEM((256, 128), F32),
        pltpu.VMEM((2, 64, 128), F32),
        pltpu.VMEM((64, 128), F32),
        pltpu.VMEM((64, 128), BF16),
        pltpu.VMEM((16, 64, 128), BF16),
        pltpu.VMEM((2, 64, 128), F32),
        pltpu.VMEM((64, 128), F32),
        dma((8,)),
        dma((EXPERTS,)),
        dma((SOURCES,)),
        dma((3, SOURCES)),
        dma((3, SOURCES)),
        dma((3, 4)),
        dma((3, 4)),
        dma((3, 2)),
        dma((3, 2)),
        dma((EXPERTS,)),
        dma((EXPERTS,)),
        dma((16,)),
        dma((16,)),
        dma((16,)),
        dma((16,)),
        dma((16,)),
        dma((16,)),
        dma((2,)),
        dma((2,)),
    ]
    return pl.pallas_call(
        kernel,
        out_shape=(
            jax.ShapeDtypeStruct((16, 2048), BF16),
            jax.ShapeDtypeStruct((128, 128), BF16),
        ),
        in_specs=[vmem] * 9 + [hbm] + [vmem] * 4 + [hbm] * 6,
        out_specs=(vmem, vmem),
        scratch_shapes=scratch,
        compiler_params=pltpu.CompilerParams(
            collective_id=0, has_side_effects=True, vmem_limit_bytes=60 * 1024 * 1024
        ),
        name="mixer_and_experts",
    )(
        receptance,
        key_tensor,
        value_tensor,
        decay_data_input,
        correction_rate_input,
        mixer_output_gate,
        decay_channel_offset.reshape(1, 128),
        head_norm_gain.reshape(1, 128),
        self_key_weight.reshape(1, 128),
        mixer_output_weight,
        second_batch_rows,
        routed_expert_index,
        routing_output_weight,
        expert_norm_gain.reshape(1, 2048),
        expert_gate_weight,
        expert_up_weight,
        expert_down_weight,
        common_expert_gate,
        common_expert_up,
        common_expert_down,
    )


def solution(mesh):
    split = Mesh(mesh.devices.reshape(16, 2, 4, 4), ("z", "c", "y", "x"))
    in_specs = (
        P(EP, TP),
        P(EP, TP),
        P(EP, TP),
        P(EP, TP),
        P(EP, TP),
        P(EP, TP),
        P(TP),
        P(TP),
        P(TP),
        P(TP, None),
        P(EP, None),
        P(EP, None),
        P(EP, None),
        P(),
        P(EP, TP, None),
        P(EP, TP, None),
        P(EP, None, TP),
        P(TP, None),
        P(TP, None),
        P(None, TP),
    )
    out_specs = (P(EP + TP, None), P(EP, TP))
    return jax.shard_map(
        on_device, mesh=split, in_specs=in_specs, out_specs=out_specs, check_vma=False
    )
```

```python
import functools

import jax
import jax.numpy as jnp
from jax import lax
from jax.experimental import pallas as pl
from jax.experimental.pallas import tpu as pltpu
from jax.sharding import Mesh
from jax.sharding import PartitionSpec as P

F32 = jnp.float32
BF16 = jnp.bfloat16
HEAD = 64
CHUNK = 64
RING = 4
CAP = 24
EXPERTS = 32
SOURCES = 8
MESH = pl.DeviceIdType.MESH
EP = ("z", "c")
TP = ("y", "x")
NN = (((1,), (0,)), ((), ()))
NT = (((1,), (1,)), ((), ()))
TN = (((0,), (0,)), ((), ()))


def dot(a, b, dims=NN):
    return lax.dot_general(a, b, dims, preferred_element_type=F32)


def halves(a):
    high = a.astype(BF16)
    return high, (a - high.astype(F32)).astype(BF16)


def dot3(a, b, dims=NN):
    (ah, al), (bh, bl) = a, b
    return dot(ah, bh, dims) + (dot(ah, bl, dims) + dot(al, bh, dims))


def dot_exact_left(a, b):
    b1 = b.astype(BF16)
    rest = b - b1.astype(F32)
    b2 = rest.astype(BF16)
    b3 = (rest - b2.astype(F32)).astype(BF16)
    return dot(a, b1) + (dot(a, b2) + dot(a, b3))


def dot_exact_right(a, b):
    ah, al = halves(a)
    return dot(ah, b) + dot(al, b)


def iota(shape, dim):
    return lax.broadcasted_iota(jnp.int32, shape, dim)


def copy_to(src, dst, send_sem, recv_sem, device):
    return pltpu.make_async_remote_copy(
        src_ref=src,
        dst_ref=dst,
        send_sem=send_sem,
        recv_sem=recv_sem,
        device_id=device,
        device_id_type=MESH,
    )


def silu(v):
    return v / (1.0 + jnp.exp(-v))


def local_mixer(rec_ref, key_ref, val_ref, dec_ref, rate_ref, off_ref, xg, yf):
    n = 2 * CHUNK
    rows = rec_ref.shape[0]
    chunks = rows // CHUNK
    lane_head = iota((1, 128), 1) >> 6
    m0 = (lane_head == 0).astype(F32)
    m1 = 1.0 - m0
    same_head = ((iota((128, 128), 0) >> 6) == (iota((128, 128), 1) >> 6)).astype(BF16)
    i, j = iota((n, n), 0), iota((n, n), 1)
    eye = (i == j).astype(F32)
    same = (i >> 6) == (j >> 6)
    below = (i > j) & same
    upto = (i >= j) & same
    ri, rj = iota((rows, rows), 0), iota((rows, rows), 1)
    tri = ((ri >= rj) & ((ri >> 6) == (rj >> 6))).astype(F32).astype(BF16)

    key = key_ref[...].astype(F32)
    logw = -0.6065306597126334 / (1.0 + jnp.exp(-(off_ref[...] + dec_ref[...].astype(F32))))
    cum = dot_exact_left(tri, logw)
    rate = 1.0 / (1.0 + jnp.exp(-rate_ref[...].astype(F32)))
    unit = key * lax.rsqrt(dot_exact_right(key * key, same_head) + 1.0)
    b = unit * rate
    up = jnp.exp(cum)
    down = jnp.exp(-cum)
    u_t = unit * jnp.exp(cum - logw)
    r_t = rec_ref[...].astype(F32) * up
    k_t = key * down
    b_t = b * down
    value = val_ref[...].astype(F32)

    def part(a, at):
        return a[at * CHUNK : (at + 1) * CHUNK]

    def both(a):
        return jnp.concatenate([a * m0, a * m1], axis=0)

    every = range(chunks)
    end = [jnp.exp(part(cum, at)[CHUNK - 1 :]) for at in every]
    v2 = [both(part(value, at)) for at in every]
    v2h = [a.astype(BF16) for a in v2]
    u2 = [both(part(u_t, at)) for at in every]
    r2 = [both(part(r_t, at)) for at in every]
    b2 = [both(part(b_t, at)) for at in every]
    k2 = [both(part(k_t, at)) for at in every]
    left = [halves(jnp.concatenate([u2[at], r2[at]], axis=0)) for at in every]
    right = [halves(jnp.concatenate([b2[at], k2[at]], axis=0)) for at in every]
    pairs = [dot3(left[at], right[at], NT) for at in every]
    lower = [jnp.where(below, pairs[at][:n, :n], 0.0) for at in every]
    m_uk = [halves(jnp.where(below, pairs[at][:n, n:], 0.0)) for at in every]
    a_b = [halves(jnp.where(upto, pairs[at][n:, :n], 0.0)) for at in every]
    a_k = [halves(jnp.where(upto, pairs[at][n:, n:], 0.0)) for at in every]
    mv = [dot(m_uk[at][0], v2h[at]) + dot(m_uk[at][1], v2h[at]) for at in every]
    akv = [dot(a_k[at][0], v2h[at]) + dot(a_k[at][1], v2h[at]) for at in every]
    inverse = None
    for level in range(6):
        half = (
            ((i >> (level + 1)) == (j >> (level + 1)))
            & (((i >> level) & 1) == 1)
            & (((j >> level) & 1) == 0)
        )
        step = [jnp.where(half, lower[at], 0.0) for at in every]
        if inverse is None:
            inverse = [eye - step[at] for at in every]
        else:
            split = [halves(inverse[at]) for at in every]
            mid = [dot3(halves(step[at]), split[at]) for at in every]
            inverse = [
                inverse[at] - dot3(split[at], halves(mid[at])) for at in every
            ]
    ez = [
        halves(dot3(halves(inverse[at]), halves(jnp.concatenate([u2[at], mv[at]], axis=1))))
        for at in every
    ]
    aez = [dot3(a_b[at], ez[at]) for at in every]
    b_end = [halves(b2[at] * end[at]) for at in every]
    k_end = [halves(k2[at] * end[at]) for at in every]
    bez = [dot3(b_end[at], ez[at], TN) for at in every]
    kv = [dot(k_end[at][0], v2h[at], TN) + dot(k_end[at][1], v2h[at], TN) for at in every]
    total = None
    for at in every:
        xo = r2[at] - aez[at][:, :128]
        yo = akv[at] - aez[at][:, 128:]
        xo = xo[:CHUNK] + xo[CHUNK:]
        yo = yo[:CHUNK] + yo[CHUNK:]
        moves = eye * end[at] - bez[at][:, :128]
        sums = kv[at] - bez[at][:, 128:]
        if total is None:
            xg[pl.ds(at * CHUNK, CHUNK), :] = xo
            yf[pl.ds(at * CHUNK, CHUNK), :] = yo
            total = jnp.concatenate([moves, sums], axis=1)
        else:
            ahead = halves(total)
            read = dot3(halves(xo), ahead)
            xg[pl.ds(at * CHUNK, CHUNK), :] = read[:, :128]
            yf[pl.ds(at * CHUNK, CHUNK), :] = read[:, 128:] + yo
            moved = dot3(halves(moves), ahead)
            total = jnp.concatenate([moved[:, :128], moved[:, 128:] + sums], axis=1)
    return total[:, :128], total[:, 128:]


def kernel(*refs):
    (
        rec_in,
        key_in,
        val_in,
        dec_in,
        rate_in,
        gate_in,
        off_in,
        gain_in,
        self_in,
        wout_in,
        rows_in,
        idx_in,
        wgt_in,
        egain_in,
        eg_in,
        eu_in,
        ed_in,
        cg_in,
        cu_in,
        cd_in,
        out0,
        out1,
    ) = refs[:22]
    (
        rec_ref,
        key_ref,
        val_ref,
        dec_ref,
        rate_ref,
        gate_ref,
        off_ref,
        gain_ref,
        self_ref,
        rows_ref,
        idx_ref,
        wgt_ref,
        egain_ref,
        wout,
        gu,
        wd,
        cgu,
        cd,
        xn,
        sbuf,
        rbuf,
        hid,
        obuf,
        retb,
        pb0,
        pb1,
        qb0,
        qb1,
        gh0,
        gh1,
        gh2,
        gh3,
        gp0,
        gp1,
        gp2,
        gp3,
        shb,
        q_hi,
        q_lo,
        onehot,
        xg,
        yf,
        cmap,
        pmap,
        zmine,
        zmap,
        zlast,
        zall,
        sts,
        keep,
        ahead,
        res0,
        res1,
    ) = refs[22:75]
    (
        ld,
        dsp_s,
        dsp_r,
        ys,
        yr,
        ws,
        wr,
        hs,
        hr,
        ret_s,
        ret_r,
        rs_s,
        rs_h,
        rs_p,
        sh_s,
        sh_r,
        zs,
        zr,
        zls,
        zlr,
        od,
        ps,
        pr,
    ) = refs[75:]
    z, c = lax.axis_index("z"), lax.axis_index("c")
    y, x = lax.axis_index("y"), lax.axis_index("x")
    nz = lax.axis_size("z")
    ep, tp = 2 * z + c, RING * y + x
    home = ep % RING
    own = home == x
    mine = jnp.where(own, 1, 0)
    group, inner = z // RING, z % RING
    last = inner == RING - 1
    later = nz - RING * (group + 1)

    def at(z_=None, c_=None, y_=None, x_=None):
        return {
            "z": z if z_ is None else z_,
            "c": c if c_ is None else c_,
            "y": y if y_ is None else y_,
            "x": x if x_ is None else x_,
        }

    def place(e, y_=None, x_=None):
        return at(e // 2, e % 2, y_, x_)

    loads = []
    for source, target in (
        (rows_in, rows_ref),
        (egain_in, egain_ref),
        (idx_in, idx_ref),
        (wgt_in, wgt_ref),
        (key_in, key_ref),
        (dec_in, dec_ref),
        (off_in, off_ref),
        (rate_in, rate_ref),
        (rec_in, rec_ref),
        (val_in, val_ref),
        (eg_in.at[0], gu.at[x, pl.ds(0, 64)]),
        (eu_in.at[0], gu.at[x, pl.ds(64, 64)]),
        (cg_in, cgu.at[pl.ds(0, 64)]),
        (cu_in, cgu.at[pl.ds(64, 64)]),
        (ed_in.at[0], wd.at[x]),
        (cd_in, cd),
        (wout_in, wout),
        (gate_in, gate_ref),
        (gain_in, gain_ref),
        (self_in, self_ref),
    ):
        loads.append(pltpu.make_async_copy(source, target, ld.at[len(loads)]))
        loads[-1].start()

    barrier = pltpu.get_barrier_semaphore()

    def tell(device):
        pl.semaphore_signal(barrier, inc=1, device_id=device, device_id_type=MESH)

    def tell_source(k, _):
        source = RING * ((ep // RING + 4 + k) % SOURCES) + x

        @pl.when(source != ep)
        def _():
            tell(place(source))

        return 0

    lax.fori_loop(0, SOURCES, tell_source, 0)

    def tell_expert(k, _):
        expert = (ep + 16 + k) % EXPERTS

        @pl.when(jnp.logical_not((expert == ep) & own))
        def _():
            tell(place(expert, x_=home))

        return 0

    lax.fori_loop(0, EXPERTS, tell_expert, 0)

    def tell_groups(k, _):
        tell(at(z_=RING * k + 3))
        return 0

    def tell_group(k, _):
        tell(at(z_=RING * group + k))
        return 0

    lax.fori_loop(0, group, tell_groups, 0)
    lax.fori_loop(0, inner, tell_group, 0)
    for k in range(1, 16):
        tell(at(y_=(y + k // RING) % RING, x_=(x + k % RING) % RING))
    tell(at(c_=1 - c))

    for load in loads[:4]:
        load.wait()
    rows = rows_ref[...].astype(F32)
    scale = lax.rsqrt(jnp.mean(rows * rows, axis=-1, keepdims=True) + 1.0)
    xn[...] = (rows * scale * egain_ref[...]).astype(BF16)

    row_count = rows_ref.shape[0]
    slots = EXPERTS * CAP
    expert_at = iota((EXPERTS, row_count), 0)
    chosen = jnp.zeros((EXPERTS, row_count), F32)
    weight = jnp.zeros((EXPERTS, row_count), F32)
    for k in range(4):
        hit = idx_ref[k : k + 1, :] == expert_at
        chosen = jnp.where(hit, 1.0, chosen)
        weight = jnp.where(hit, wgt_ref[k : k + 1, :], weight)
    earlier = iota((row_count, row_count), 0) < iota((row_count, row_count), 1)
    rank = dot(chosen.astype(BF16), earlier.astype(F32).astype(BF16))
    label = jnp.where(chosen > 0.0, rank, -1.0).astype(BF16)
    slot_s, slot_e = iota((slots, EXPERTS), 0), iota((slots, EXPERTS), 1)
    spread = ((slot_s >= slot_e * CAP) & (slot_s < slot_e * CAP + CAP)).astype(F32)
    within = jnp.sum(spread * (slot_s - slot_e * CAP).astype(F32), axis=1, keepdims=True)
    spread = spread.astype(BF16)
    placed = (dot(spread, label) == within).astype(F32)
    w_hi, w_lo = halves(weight)
    q_hi[...] = (placed * dot(spread, w_hi)).astype(BF16)
    q_lo[...] = (placed * dot(spread, w_lo)).astype(BF16)
    onehot[...] = placed.astype(BF16)

    @pl.when(own)
    def _():
        features = xn[:, pl.ds(pl.multiple_of(512 * y, 512), 512)]
        packed = dot(onehot[...], features)
        sbuf[...] = packed.reshape(EXPERTS, CAP, 512).astype(BF16)
        rbuf[y, ep // RING] = sbuf[ep]

    for load in loads[10:14]:
        load.wait()

    pl.semaphore_wait(barrier, 15 + 1 + (3 - inner) + jnp.where(last, later, 0) + 31 * mine + 32 - mine)

    def dispatch(e):
        return copy_to(
            sbuf.at[e], rbuf.at[y, ep // RING], dsp_s.at[0], dsp_r.at[ep // RING], place(e)
        )

    @pl.when(own)
    def _():
        dispatch((ep + 16) % EXPERTS).start()

        def send(k, _):
            dispatch((ep + 16 - k) % EXPERTS).start()
            dispatch((ep + 16 + k) % EXPERTS).start()
            return 0

        lax.fori_loop(1, 16, send, 0)

    def ring(piece, first_half, send_sem, recv_sem, p, axis):
        me = y if axis == "y" else x
        right, left, across = (me + 1) % RING, (me + 3) % RING, (me + 2) % RING

        def move(slot, way, to):
            device = at(y_=to) if axis == "y" else at(x_=to)
            return copy_to(piece(slot), piece(slot), send_sem, recv_sem.at[way, p], device)

        def start(way):
            move(me, way, left if way else right).start()

        def relay():
            if first_half:
                move(left, 0, right).wait_recv()
                move(left, 2, right).start()
            else:
                move(right, 1, left).wait_recv()
                move(right, 2, left).start()

        def near():
            if first_half:
                move(right, 1, left).wait_recv()
            else:
                move(left, 0, right).wait_recv()

        def far():
            move(across, 2, right).wait_recv()

        return start, relay, near, far

    weights = [
        ring(lambda s: gu.at[s, pl.ds(0, 64)], True, ws.at[0], wr, 0, "x"),
        ring(lambda s: gu.at[s, pl.ds(64, 64)], False, ws.at[0], wr, 1, "x"),
        ring(lambda s: wd.at[s, pl.ds(0, 512)], True, ws.at[1], wr, 2, "x"),
        ring(lambda s: wd.at[s, pl.ds(512, 512)], False, ws.at[1], wr, 3, "x"),
    ]
    row_ring, row_from = [], []
    for j, away in enumerate((4, 3, 5, 2, 6, 1, 7, 0)):
        k = (ep // RING + away) % SOURCES
        row_ring.append(ring(lambda s, k=k: rbuf.at[s, k], j % 2 == 0, ys.at[0], yr, j, "y"))
        row_from.append(k)
    hid_ring = [
        ring(lambda s: hid.at[s, pl.ds(0, 96)], True, hs.at[0], hr, 0, "y"),
        ring(lambda s: hid.at[s, pl.ds(96, 96)], False, hs.at[0], hr, 1, "y"),
    ]
    weights[0][0](0)
    weights[1][0](1)
    weights[1][0](0)
    weights[0][0](1)

    for load in loads[4:10]:
        load.wait()
    moves, sums = local_mixer(rec_ref, key_ref, val_ref, dec_ref, rate_ref, off_ref, xg, yf)
    cmap[0] = moves[:64] + pltpu.roll(sums[:64], 64, 1)
    cmap[1] = pltpu.roll(moves[64:], 64, 1) + sums[64:]
    swap = copy_to(cmap.at[1 - c], pmap, ps.at[0], pr.at[0], at(c_=1 - c))
    swap.start()

    pre = dot(cgu[...], xn[...], NT)
    shb[tp] = (silu(pre[:64]) * pre[64:]).astype(BF16)

    def share(k):
        return copy_to(
            shb.at[tp], shb.at[tp], sh_s.at[0], sh_r.at[0], at(y_=k // RING, x_=k % RING)
        )

    def share_send(k, _):
        share((tp + k) % 16).start()
        return 0

    lax.fori_loop(1, 16, share_send, 0)

    swap.wait_recv()
    lane = iota((64, 128), 1)
    first = jnp.where(c == 0, cmap[0], pmap[...])
    second = jnp.where(c == 0, pmap[...], cmap[1])

    def compose(later, earlier):
        stacked = jnp.concatenate([earlier, jnp.zeros_like(earlier)], axis=0)
        moved = dot3(halves(jnp.where(lane < 64, later, 0.0)), halves(stacked))
        return moved + jnp.where(lane < 64, 0.0, later)

    zmine[...] = compose(second, first).astype(BF16)

    def to_group(k):
        return copy_to(zmine, zmap.at[inner], zs.at[k], zr.at[inner], at(z_=RING * group + k))

    def send_group(k, _):
        to_group(k).start()
        return 0

    lax.fori_loop(inner + 1, RING, send_group, 0)

    def forward_rows(j):
        k = row_from[j]

        @pl.when(RING * k + x != ep)
        def _():
            copy_to(
                rbuf.at[y, k], rbuf.at[y, k], dsp_s.at[0], dsp_r.at[k], place(RING * k + x)
            ).wait_recv()

        row_ring[j][0](0)
        row_ring[j][0](1)

    weights[0][1]()
    weights[1][1]()
    for j in range(4):
        forward_rows(j)
    def advance(step):
        step = step.astype(F32)
        low = jnp.where(lane < 64, step, 0.0)
        twice = (low + pltpu.roll(low, 64, 1)).astype(BF16)
        k_hi, k_lo = halves(keep[...])
        moved = dot(twice, jnp.concatenate([k_hi, k_lo], axis=0))
        keep[...] = moved + jnp.where(lane < 64, 0.0, step)

    def in_group(k, _):
        copy_to(zmine, zmap.at[k], zs.at[0], zr.at[k], at(z_=RING * group + k)).wait_recv()
        advance(zmap[k])
        return 0

    def to_later(k):
        return copy_to(zlast, zall.at[group], zls.at[0], zlr.at[group], at(z_=k))

    keep[...] = (iota((64, 128), 0) == lane).astype(F32)
    lax.fori_loop(0, inner, in_group, 0)
    ahead[...] = keep[...]

    @pl.when(last)
    def _():
        advance(zmine[...])
        zlast[...] = keep[...].astype(BF16)

        def send_later(k, _):
            to_later(k).start()
            return 0

        lax.fori_loop(RING * (group + 1), nz, send_later, 0)

    for j in range(4, 8):
        forward_rows(j)
    for ring_of in row_ring:
        ring_of[1]()
    for load in loads[14:]:
        load.wait()
    weights[2][0](0)
    weights[3][0](1)
    weights[3][0](0)
    weights[2][0](1)

    for part in (0, 1):
        weights[part][2]()
        weights[part][3]()

    def product(slot):
        taken = rbuf[slot].astype(F32).reshape(SOURCES * CAP, 512).astype(BF16)
        span = pl.ds(pl.multiple_of(512 * slot, 512), 512)
        g = gu[:, 0:64, span].reshape(256, 512)
        u = gu[:, 64:128, span].reshape(256, 512)
        return dot(taken, g, NT), dot(taken, u, NT)

    g0, u0 = product(y)
    for ring_of in row_ring:
        ring_of[2]()
    g1, u1 = product((y + 1) % RING)
    g2, u2 = product((y + 3) % RING)
    for ring_of in row_ring:
        ring_of[3]()
    g3, u3 = product((y + 2) % RING)
    hidden = silu((g0 + g1) + (g2 + g3)) * ((u0 + u1) + (u2 + u3))
    hid[y] = hidden.astype(BF16)
    hid_ring[0][0](0)
    hid_ring[1][0](1)
    hid_ring[1][0](0)
    hid_ring[0][0](1)
    weights[2][1]()
    weights[3][1]()

    def over_groups(k, _):
        copy_to(zlast, zall.at[k], zls.at[0], zlr.at[k], at(z_=RING * k + 3)).wait_recv()
        advance(zall[k])
        return 0

    keep[...] = jnp.zeros((64, 128), F32)
    lax.fori_loop(0, group, over_groups, 0)
    state = jnp.where(lane < 64, 0.0, compose(ahead[...], keep[...]))
    passed = jnp.where(lane < 64, 0.0, compose(first, state))
    sts[c] = jnp.where(c == 0, state, passed)
    keep[...] = jnp.where(c == 0, passed, state)
    hand = copy_to(keep, sts.at[c], ps.at[1], pr.at[1], at(c_=1 - c))
    hand.start()
    copy_to(keep, sts.at[1 - c], ps.at[1], pr.at[1], at(c_=1 - c)).wait_recv()

    start = jnp.concatenate([pltpu.roll(sts[0], 64, 1), sts[1]], axis=0)
    readout = dot3(halves(xg[...]), halves(start)) + yf[...]
    same_head = ((iota((128, 128), 0) >> 6) == (iota((128, 128), 1) >> 6)).astype(F32)
    mean_of = (same_head * (1.0 / HEAD)).astype(BF16)
    same_head = same_head.astype(BF16)
    centred = readout - dot_exact_right(readout, mean_of)
    variance = dot_exact_right(centred * centred, mean_of)
    key = key_ref[...].astype(F32)
    bonus = dot_exact_right(rec_ref[...].astype(F32) * key * self_ref[...], same_head)
    mixed = (
        centred * lax.rsqrt(variance + 1.0) * gain_ref[...] + bonus * val_ref[...].astype(F32)
    ) * gate_ref[...].astype(F32)
    mixed = mixed.astype(BF16)

    def reduce_along(n, axis, piece, half, got_half, got_piece):
        me = y if axis == "y" else x
        right, left, across = (me + 1) % RING, (me + 3) % RING, (me + 2) % RING

        def to(way):
            side = left if way else right
            return at(y_=side) if axis == "y" else at(x_=side)

        def far(way):
            return copy_to(
                half(across, way), got_half.at[way], rs_s.at[n], rs_h.at[n, way], to(way)
            )

        def near(way):
            block = piece(left if way else right)
            return copy_to(block, got_piece.at[way], rs_s.at[n], rs_p.at[n, way], to(way))

        def first():
            far(0).start()
            far(1).start()

        def second():
            for way in range(2):
                far(way).wait_recv()
                mine_half = half(left if way else right, way)
                mine_half[...] = (
                    mine_half[...].astype(F32) + got_half[way].astype(F32)
                ).astype(BF16)
                near(way).start()

        def third():
            near(0).wait_recv()
            near(1).wait_recv()
            own_block = piece(me)[...].astype(F32)
            return own_block + got_piece[0].astype(F32) + got_piece[1].astype(F32)

        return first, second, third

    x_first = reduce_along(
        0, "x", lambda t: pb0.at[t], lambda t, h: pb0.at[t, pl.ds(2 * h, 2)], gh0, gp0
    )
    y_first = reduce_along(
        1, "y", lambda t: pb1.at[t], lambda t, h: pb1.at[t, pl.ds(2 * h, 2)], gh1, gp1
    )
    y_then = reduce_along(
        2, "y", lambda t: qb0.at[t], lambda t, h: qb0.at[t, :, pl.ds(512 * h, 512)], gh2, gp2
    )
    x_then = reduce_along(
        3, "x", lambda t: qb1.at[t], lambda t, h: qb1.at[t, :, pl.ds(512 * h, 512)], gh3, gp3
    )

    for block in range(4):
        partial = dot(mixed[64 * block : 64 * block + 64], wout[...])
        partial = partial.reshape(4, 16, 2048).astype(BF16)
        pb1[block] = partial[:, :, 1024:]
        for side in range(4):
            pb0[side, block] = partial[side, :, :1024]
    x_first[0]()
    y_first[0]()
    hid_ring[0][1]()
    hid_ring[1][1]()

    weights[2][2]()
    weights[3][2]()
    weights[2][3]()
    weights[3][3]()
    for ring_of in hid_ring:
        ring_of[2]()
        ring_of[3]()
    def give_back(k, s):
        return copy_to(
            obuf.at[s, k],
            retb.at[ep],
            ret_s.at[0],
            ret_r.at[0],
            place(RING * k + x, x_=s),
        )

    every_hidden = jnp.concatenate([hid[part] for part in range(RING)], axis=1)

    def send_back(s, away):
        k = (ep // RING + away) % SOURCES

        @pl.when(jnp.logical_not((RING * k + x == ep) & (s == x)))
        def _():
            give_back(k, s).start()

    for s in range(RING):
        made = dot(every_hidden, wd[s])
        obuf[s] = made.reshape(SOURCES, CAP, 128).astype(BF16)
        for away in (4, 3, 5, 2):
            send_back(s, away)
    for away in (6, 1, 7, 0):
        for s in range(RING):
            send_back(s, away)

    @pl.when(own)
    def _():
        retb[ep] = obuf[x, ep // RING]

    x_first[1]()
    y_first[1]()
    qb0[...] = x_first[2]().astype(BF16)
    y_then[0]()
    qb1[...] = y_first[2]().astype(BF16)
    x_then[0]()
    y_then[1]()
    x_then[1]()
    res0[:, :1024] = y_then[2]().astype(BF16)
    res0[:, 1024:] = x_then[2]().astype(BF16)
    put0 = pltpu.make_async_copy(res0, out0, od.at[0])
    put0.start()

    def whole(ref, send_sem, recv_sem):
        return copy_to(ref, ref, send_sem, recv_sem, at(c_=1 - c))

    others = shb.at[pl.ds(0, 15)]
    whole(others, sh_s.at[0], sh_r.at[0]).wait_recv()
    shared = dot(shb[...].reshape(1024, 128), cd[...], TN)

    @pl.when(own)
    def _():
        whole(sbuf.at[pl.ds(0, EXPERTS - 1)], dsp_s.at[0], dsp_r.at[0]).wait_send()

    for sent, sem in (
        (others, sh_s.at[0]),
        (gu.at[pl.ds(0, 3)], ws.at[0]),
        (wd.at[pl.ds(0, 3)], ws.at[1]),
        (rbuf.at[pl.ds(0, 3)], ys.at[0]),
        (hid.at[pl.ds(0, 3)], hs.at[0]),
        (pb0.at[pl.ds(0, 3)], rs_s.at[0]),
        (pb1.at[pl.ds(0, 3)], rs_s.at[1]),
        (qb0.at[pl.ds(0, 3)], rs_s.at[2]),
        (qb1.at[pl.ds(0, 3)], rs_s.at[3]),
    ):
        whole(sent, sem, dsp_r.at[0]).wait_send()
    swap.wait_send()
    hand.wait_send()

    def group_sent(k, _):
        to_group(k).wait_send()
        return 0

    lax.fori_loop(inner + 1, RING, group_sent, 0)
    for k in range(RING - 1):
        @pl.when(last & (group == k))
        def _():
            maps = q_hi.at[pl.ds(0, 64 * (12 - 4 * k))]
            whole(maps, zls.at[0], zlr.at[0]).wait_send()

    @pl.when(own)
    def _():
        whole(retb.at[pl.ds(0, EXPERTS - 1)], ret_s.at[0], ret_r.at[0]).wait()

    @pl.when(jnp.logical_not(own))
    def _():
        whole(retb, ret_s.at[0], ret_r.at[0]).wait()

    copies = retb[...].astype(F32).reshape(slots, 128).astype(BF16)
    merged = dot(q_hi[...], copies, TN) + dot(q_lo[...], copies, TN) + shared
    res1[...] = merged.astype(BF16)
    put1 = pltpu.make_async_copy(res1, out1, od.at[1])
    put1.start()
    put0.wait()

    put1.wait()


def on_device(
    receptance,
    key_tensor,
    value_tensor,
    decay_data_input,
    correction_rate_input,
    mixer_output_gate,
    decay_channel_offset,
    head_norm_gain,
    self_key_weight,
    mixer_output_weight,
    second_batch_rows,
    routed_expert_index,
    routing_output_weight,
    expert_norm_gain,
    expert_gate_weight,
    expert_up_weight,
    expert_down_weight,
    common_expert_gate,
    common_expert_up,
    common_expert_down,
):
    hbm = pl.BlockSpec(memory_space=pl.ANY)
    dma = pltpu.SemaphoreType.DMA
    rows = receptance.shape[0]
    scratch = [
        *(pltpu.VMEM((rows, 128), BF16) for _ in range(6)),
        *(pltpu.VMEM((1, 128), F32) for _ in range(3)),
        pltpu.VMEM((128, 2048), BF16),
        pltpu.VMEM((4, 128), jnp.int32),
        pltpu.VMEM((4, 128), F32),
        pltpu.VMEM((1, 2048), F32),
        pltpu.VMEM((128, 2048), BF16),
        pltpu.VMEM((RING, 128, 2048), BF16),
        pltpu.VMEM((RING, 1024, 128), BF16),
        pltpu.VMEM((128, 2048), BF16),
        pltpu.VMEM((1024, 128), BF16),
        pltpu.VMEM((128, 2048), BF16),
        pltpu.VMEM((EXPERTS, CAP, 512), BF16),
        pltpu.VMEM((RING, SOURCES, CAP, 512), BF16),
        pltpu.VMEM((RING, SOURCES * CAP, 256), BF16),
        pltpu.VMEM((RING, SOURCES, CAP, 128), BF16),
        pltpu.VMEM((EXPERTS, CAP, 128), BF16),
        pltpu.VMEM((RING, RING, 16, 1024), BF16),
        pltpu.VMEM((RING, RING, 16, 1024), BF16),
        pltpu.VMEM((RING, 16, 1024), BF16),
        pltpu.VMEM((RING, 16, 1024), BF16),
        pltpu.VMEM((2, 2, 16, 1024), BF16),
        pltpu.VMEM((2, 2, 16, 1024), BF16),
        pltpu.VMEM((2, 16, 512), BF16),
        pltpu.VMEM((2, 16, 512), BF16),
        pltpu.VMEM((2, RING, 16, 1024), BF16),
        pltpu.VMEM((2, RING, 16, 1024), BF16),
        pltpu.VMEM((2, 16, 1024), BF16),
        pltpu.VMEM((2, 16, 1024), BF16),
        pltpu.VMEM((16, 64, 128), BF16),
        pltpu.VMEM((EXPERTS * CAP, 128), BF16),
        pltpu.VMEM((EXPERTS * CAP, 128), BF16),
        pltpu.VMEM((EXPERTS * CAP, 128), BF16),
        pltpu.VMEM((256, 128), F32),
        pltpu.VMEM((256, 128), F32),
        pltpu.VMEM((2, 64, 128), F32),
        pltpu.VMEM((64, 128), F32),
        pltpu.VMEM((64, 128), BF16),
        pltpu.VMEM((RING, 64, 128), BF16),
        pltpu.VMEM((64, 128), BF16),
        pltpu.VMEM((RING, 64, 128), BF16),
        pltpu.VMEM((2, 64, 128), F32),
        pltpu.VMEM((64, 128), F32),
        pltpu.VMEM((64, 128), F32),
        pltpu.VMEM((16, 2048), BF16),
        pltpu.VMEM((128, 128), BF16),
        dma((20,)),
        dma((1,)),
        dma((SOURCES,)),
        dma((1,)),
        dma((3, SOURCES)),
        dma((2,)),
        dma((3, 4)),
        dma((1,)),
        dma((3, 2)),
        dma((1,)),
        dma((1,)),
        dma((4,)),
        dma((4, 2)),
        dma((4, 2)),
        dma((1,)),
        dma((1,)),
        dma((RING,)),
        dma((RING,)),
        dma((1,)),
        dma((RING,)),
        dma((2,)),
        dma((2,)),
        dma((2,)),
    ]
    return pl.pallas_call(
        kernel,
        out_shape=(
            jax.ShapeDtypeStruct((16, 2048), BF16),
            jax.ShapeDtypeStruct((128, 128), BF16),
        ),
        in_specs=[hbm] * 20,
        out_specs=(hbm, hbm),
        scratch_shapes=scratch,
        compiler_params=pltpu.CompilerParams(
            collective_id=0, has_side_effects=True, vmem_limit_bytes=60 * 1024 * 1024
        ),
        name="mixer_and_experts",
    )(
        receptance,
        key_tensor,
        value_tensor,
        decay_data_input,
        correction_rate_input,
        mixer_output_gate,
        decay_channel_offset.reshape(1, 128),
        head_norm_gain.reshape(1, 128),
        self_key_weight.reshape(1, 128),
        mixer_output_weight,
        second_batch_rows,
        routed_expert_index.T,
        routing_output_weight.T,
        expert_norm_gain.reshape(1, 2048),
        expert_gate_weight,
        expert_up_weight,
        expert_down_weight,
        common_expert_gate,
        common_expert_up,
        common_expert_down,
    )


def solution(mesh):
    split = Mesh(mesh.devices.reshape(16, 2, 4, 4), ("z", "c", "y", "x"))
    in_specs = (
        P(EP, TP),
        P(EP, TP),
        P(EP, TP),
        P(EP, TP),
        P(EP, TP),
        P(EP, TP),
        P(TP),
        P(TP),
        P(TP),
        P(TP, None),
        P(EP, None),
        P(EP, None),
        P(EP, None),
        P(),
        P(EP, TP, None),
        P(EP, TP, None),
        P(EP, None, TP),
        P(TP, None),
        P(TP, None),
        P(None, TP),
    )
    out_specs = (P(EP + TP, None), P(EP, TP))
    return jax.shard_map(
        on_device, mesh=split, in_specs=in_specs, out_specs=out_specs, check_vma=False
    )
```

```python
import functools

import jax
import jax.numpy as jnp
from jax import lax
from jax.experimental import pallas as pl
from jax.experimental.pallas import tpu as pltpu
from jax.sharding import Mesh
from jax.sharding import PartitionSpec as P

F32 = jnp.float32
BF16 = jnp.bfloat16
HEAD = 64
CHUNK = 64
RING = 4
CAP = 24
EXPERTS = 32
SOURCES = 8
MESH = pl.DeviceIdType.MESH
EP = ("z", "c")
TP = ("y", "x")
NN = (((1,), (0,)), ((), ()))
NT = (((1,), (1,)), ((), ()))
TN = (((0,), (0,)), ((), ()))


def dot(a, b, dims=NN):
    return lax.dot_general(a, b, dims, preferred_element_type=F32)


def halves(a):
    high = a.astype(BF16)
    return high, (a - high.astype(F32)).astype(BF16)


def dot3(a, b, dims=NN):
    (ah, al), (bh, bl) = a, b
    return dot(ah, bh, dims) + (dot(ah, bl, dims) + dot(al, bh, dims))


def dot_exact_left(a, b):
    b1 = b.astype(BF16)
    rest = b - b1.astype(F32)
    b2 = rest.astype(BF16)
    b3 = (rest - b2.astype(F32)).astype(BF16)
    return dot(a, b1) + (dot(a, b2) + dot(a, b3))


def dot_exact_right(a, b):
    ah, al = halves(a)
    return dot(ah, b) + dot(al, b)


def iota(shape, dim):
    return lax.broadcasted_iota(jnp.int32, shape, dim)


def copy_to(src, dst, send_sem, recv_sem, device):
    return pltpu.make_async_remote_copy(
        src_ref=src,
        dst_ref=dst,
        send_sem=send_sem,
        recv_sem=recv_sem,
        device_id=device,
        device_id_type=MESH,
    )


def silu(v):
    return v / (1.0 + jnp.exp(-v))


def local_mixer(rec_ref, key_ref, val_ref, dec_ref, rate_ref, off_ref, xg, yf):
    n = 2 * CHUNK
    rows = rec_ref.shape[0]
    chunks = rows // CHUNK
    lane_head = iota((1, 128), 1) >> 6
    m0 = (lane_head == 0).astype(F32)
    m1 = 1.0 - m0
    same_head = ((iota((128, 128), 0) >> 6) == (iota((128, 128), 1) >> 6)).astype(BF16)
    i, j = iota((n, n), 0), iota((n, n), 1)
    eye = (i == j).astype(F32)
    same = (i >> 6) == (j >> 6)
    below = (i > j) & same
    upto = (i >= j) & same
    ri, rj = iota((rows, rows), 0), iota((rows, rows), 1)
    tri = ((ri >= rj) & ((ri >> 6) == (rj >> 6))).astype(F32).astype(BF16)

    key = key_ref[...].astype(F32)
    logw = -0.6065306597126334 / (1.0 + jnp.exp(-(off_ref[...] + dec_ref[...].astype(F32))))
    cum = dot_exact_left(tri, logw)
    rate = 1.0 / (1.0 + jnp.exp(-rate_ref[...].astype(F32)))
    unit = key * lax.rsqrt(dot_exact_right(key * key, same_head) + 1.0)
    b = unit * rate
    up = jnp.exp(cum)
    down = jnp.exp(-cum)
    u_t = unit * jnp.exp(cum - logw)
    r_t = rec_ref[...].astype(F32) * up
    k_t = key * down
    b_t = b * down
    value = val_ref[...].astype(F32)

    def part(a, at):
        return a[at * CHUNK : (at + 1) * CHUNK]

    def both(a):
        return jnp.concatenate([a * m0, a * m1], axis=0)

    every = range(chunks)
    end = [jnp.exp(part(cum, at)[CHUNK - 1 :]) for at in every]
    v2 = [both(part(value, at)) for at in every]
    v2h = [a.astype(BF16) for a in v2]
    u2 = [both(part(u_t, at)) for at in every]
    r2 = [both(part(r_t, at)) for at in every]
    b2 = [both(part(b_t, at)) for at in every]
    k2 = [both(part(k_t, at)) for at in every]
    left = [halves(jnp.concatenate([u2[at], r2[at]], axis=0)) for at in every]
    right = [halves(jnp.concatenate([b2[at], k2[at]], axis=0)) for at in every]
    pairs = [dot3(left[at], right[at], NT) for at in every]
    lower = [jnp.where(below, pairs[at][:n, :n], 0.0) for at in every]
    m_uk = [halves(jnp.where(below, pairs[at][:n, n:], 0.0)) for at in every]
    a_b = [halves(jnp.where(upto, pairs[at][n:, :n], 0.0)) for at in every]
    a_k = [halves(jnp.where(upto, pairs[at][n:, n:], 0.0)) for at in every]
    mv = [dot(m_uk[at][0], v2h[at]) + dot(m_uk[at][1], v2h[at]) for at in every]
    akv = [dot(a_k[at][0], v2h[at]) + dot(a_k[at][1], v2h[at]) for at in every]
    inverse = None
    for level in range(6):
        half = (
            ((i >> (level + 1)) == (j >> (level + 1)))
            & (((i >> level) & 1) == 1)
            & (((j >> level) & 1) == 0)
        )
        step = [jnp.where(half, lower[at], 0.0) for at in every]
        if inverse is None:
            inverse = [eye - step[at] for at in every]
        else:
            split = [halves(inverse[at]) for at in every]
            mid = [dot3(halves(step[at]), split[at]) for at in every]
            inverse = [
                inverse[at] - dot3(split[at], halves(mid[at])) for at in every
            ]
    ez = [
        halves(dot3(halves(inverse[at]), halves(jnp.concatenate([u2[at], mv[at]], axis=1))))
        for at in every
    ]
    aez = [dot3(a_b[at], ez[at]) for at in every]
    b_end = [halves(b2[at] * end[at]) for at in every]
    k_end = [halves(k2[at] * end[at]) for at in every]
    bez = [dot3(b_end[at], ez[at], TN) for at in every]
    kv = [dot(k_end[at][0], v2h[at], TN) + dot(k_end[at][1], v2h[at], TN) for at in every]
    total = None
    for at in every:
        xo = r2[at] - aez[at][:, :128]
        yo = akv[at] - aez[at][:, 128:]
        xo = xo[:CHUNK] + xo[CHUNK:]
        yo = yo[:CHUNK] + yo[CHUNK:]
        moves = eye * end[at] - bez[at][:, :128]
        sums = kv[at] - bez[at][:, 128:]
        if total is None:
            xg[pl.ds(at * CHUNK, CHUNK), :] = xo
            yf[pl.ds(at * CHUNK, CHUNK), :] = yo
            total = jnp.concatenate([moves, sums], axis=1)
        else:
            ahead = halves(total)
            read = dot3(halves(xo), ahead)
            xg[pl.ds(at * CHUNK, CHUNK), :] = read[:, :128]
            yf[pl.ds(at * CHUNK, CHUNK), :] = read[:, 128:] + yo
            moved = dot3(halves(moves), ahead)
            total = jnp.concatenate([moved[:, :128], moved[:, 128:] + sums], axis=1)
    return total[:, :128], total[:, 128:]


def kernel(*refs):
    (
        rec_in,
        key_in,
        val_in,
        dec_in,
        rate_in,
        gate_in,
        off_in,
        gain_in,
        self_in,
        wout_in,
        rows_in,
        idx_in,
        wgt_in,
        egain_in,
        eg_in,
        eu_in,
        ed_in,
        cg_in,
        cu_in,
        cd_in,
        out0,
        out1,
    ) = refs[:22]
    (
        rec_ref,
        key_ref,
        val_ref,
        dec_ref,
        rate_ref,
        gate_ref,
        off_ref,
        gain_ref,
        self_ref,
        rows_ref,
        idx_ref,
        wgt_ref,
        egain_ref,
        wout,
        gu,
        wd,
        cgu,
        cd,
        xn,
        sbuf,
        rbuf,
        hid,
        obuf,
        retb,
        pb0,
        pb1,
        qb0,
        qb1,
        gh0,
        gh1,
        gh2,
        gh3,
        gp0,
        gp1,
        gp2,
        gp3,
        shb,
        q_hi,
        q_lo,
        onehot,
        xg,
        yf,
        cmap,
        pmap,
        zmine,
        zmap,
        zlast,
        zall,
        sts,
        keep,
        ahead,
    ) = refs[22:73]
    (
        ld,
        dsp_s,
        dsp_r,
        ys,
        yr,
        ws,
        wr,
        hs,
        hr,
        ret_s,
        ret_r,
        rs_s,
        rs_h,
        rs_p,
        sh_s,
        sh_r,
        zs,
        zr,
        zls,
        zlr,
        ps,
        pr,
    ) = refs[73:]
    z, c = lax.axis_index("z"), lax.axis_index("c")
    y, x = lax.axis_index("y"), lax.axis_index("x")
    nz = lax.axis_size("z")
    ep, tp = 2 * z + c, RING * y + x
    home = ep % RING
    own = home == x
    mine = jnp.where(own, 1, 0)
    group, inner = z // RING, z % RING
    last = inner == RING - 1
    later = nz - RING * (group + 1)

    def at(z_=None, c_=None, y_=None, x_=None):
        return {
            "z": z if z_ is None else z_,
            "c": c if c_ is None else c_,
            "y": y if y_ is None else y_,
            "x": x if x_ is None else x_,
        }

    def place(e, y_=None, x_=None):
        return at(e // 2, e % 2, y_, x_)

    def whole(ref, send_sem, recv_sem):
        return copy_to(ref, ref, send_sem, recv_sem, at(c_=1 - c))

    loads = []
    for source, target in (
        (rows_in, rows_ref),
        (egain_in, egain_ref),
        (idx_in, idx_ref),
        (wgt_in, wgt_ref),
        (key_in, key_ref),
        (dec_in, dec_ref),
        (off_in, off_ref),
        (rate_in, rate_ref),
        (rec_in, rec_ref),
        (val_in, val_ref),
        (eg_in.at[0], gu.at[x, pl.ds(0, 64)]),
        (eu_in.at[0], gu.at[x, pl.ds(64, 64)]),
        (cg_in, cgu.at[pl.ds(0, 64)]),
        (cu_in, cgu.at[pl.ds(64, 64)]),
        (ed_in.at[0], wd.at[x]),
        (cd_in, cd),
        (wout_in, wout),
        (gate_in, gate_ref),
        (gain_in, gain_ref),
        (self_in, self_ref),
    ):
        loads.append(pltpu.make_async_copy(source, target, ld.at[len(loads)]))
        loads[-1].start()

    barrier = pltpu.get_barrier_semaphore()

    def tell(device):
        pl.semaphore_signal(barrier, inc=1, device_id=device, device_id_type=MESH)

    def tell_source(k, _):
        source = RING * ((ep // RING + 4 + k) % SOURCES) + x

        @pl.when(source != ep)
        def _():
            tell(place(source))

        return 0

    lax.fori_loop(0, SOURCES, tell_source, 0)

    def tell_groups(k, _):
        tell(at(z_=RING * k + 3))
        return 0

    def tell_group(k, _):
        tell(at(z_=RING * group + k))
        return 0

    lax.fori_loop(0, group, tell_groups, 0)
    lax.fori_loop(0, inner, tell_group, 0)
    for k in range(1, 16):
        tell(at(y_=(y + k // RING) % RING, x_=(x + k % RING) % RING))
    tell(at(c_=1 - c))

    for load in loads[:4]:
        load.wait()
    rows = rows_ref[...].astype(F32)
    scale = lax.rsqrt(jnp.mean(rows * rows, axis=-1, keepdims=True) + 1.0)
    xn[...] = (rows * scale * egain_ref[...]).astype(BF16)

    row_count = rows_ref.shape[0]
    slots = EXPERTS * CAP
    expert_at = iota((EXPERTS, row_count), 0)
    chosen = jnp.zeros((EXPERTS, row_count), F32)
    weight = jnp.zeros((EXPERTS, row_count), F32)
    for k in range(4):
        hit = idx_ref[k : k + 1, :] == expert_at
        chosen = jnp.where(hit, 1.0, chosen)
        weight = jnp.where(hit, wgt_ref[k : k + 1, :], weight)
    earlier = iota((row_count, row_count), 0) < iota((row_count, row_count), 1)
    rank = dot(chosen.astype(BF16), earlier.astype(F32).astype(BF16))
    label = jnp.where(chosen > 0.0, rank, -1.0).astype(BF16)
    slot_s, slot_e = iota((slots, EXPERTS), 0), iota((slots, EXPERTS), 1)
    spread = ((slot_s >= slot_e * CAP) & (slot_s < slot_e * CAP + CAP)).astype(F32)
    within = jnp.sum(spread * (slot_s - slot_e * CAP).astype(F32), axis=1, keepdims=True)
    spread = spread.astype(BF16)
    placed = (dot(spread, label) == within).astype(F32)
    w_hi, w_lo = halves(weight)
    q_hi[...] = (placed * dot(spread, w_hi)).astype(BF16)
    q_lo[...] = (placed * dot(spread, w_lo)).astype(BF16)
    onehot[...] = placed.astype(BF16)

    @pl.when(own)
    def _():
        features = xn[:, pl.ds(pl.multiple_of(512 * y, 512), 512)]
        packed = dot(onehot[...], features)
        sbuf[...] = packed.reshape(EXPERTS, CAP, 512).astype(BF16)
        rbuf[y, ep // RING] = sbuf[ep]

    for load in loads[10:14]:
        load.wait()

    pl.semaphore_wait(barrier, 15 + 1 + (3 - inner) + jnp.where(last, later, 0) + 31 * mine)

    def dispatch(e):
        return copy_to(
            sbuf.at[e], rbuf.at[y, ep // RING], dsp_s.at[0], dsp_r.at[ep // RING], place(e)
        )

    @pl.when(own)
    def _():
        dispatch((ep + 16) % EXPERTS).start()

        def send(k, _):
            dispatch((ep + 16 - k) % EXPERTS).start()
            dispatch((ep + 16 + k) % EXPERTS).start()
            return 0

        lax.fori_loop(1, 16, send, 0)

    def ring(piece, first_half, send_sem, recv_sem, p, axis):
        me = y if axis == "y" else x
        right, left, across = (me + 1) % RING, (me + 3) % RING, (me + 2) % RING

        def move(slot, way, to):
            device = at(y_=to) if axis == "y" else at(x_=to)
            return copy_to(piece(slot), piece(slot), send_sem, recv_sem.at[way, p], device)

        def start(way):
            move(me, way, left if way else right).start()

        def relay():
            if first_half:
                move(left, 0, right).wait_recv()
                move(left, 2, right).start()
            else:
                move(right, 1, left).wait_recv()
                move(right, 2, left).start()

        def near():
            if first_half:
                move(right, 1, left).wait_recv()
            else:
                move(left, 0, right).wait_recv()

        def far():
            move(across, 2, right).wait_recv()

        return start, relay, near, far

    weights = [
        ring(lambda s: gu.at[s, pl.ds(0, 64)], True, ws.at[0], wr, 0, "x"),
        ring(lambda s: gu.at[s, pl.ds(64, 64)], False, ws.at[0], wr, 1, "x"),
        ring(lambda s: wd.at[s, pl.ds(0, 512)], True, ws.at[1], wr, 2, "x"),
        ring(lambda s: wd.at[s, pl.ds(512, 512)], False, ws.at[1], wr, 3, "x"),
    ]
    row_ring, row_from = [], []
    for j, away in enumerate((4, 3, 5, 2, 6, 1, 7, 0)):
        k = (ep // RING + away) % SOURCES
        row_ring.append(ring(lambda s, k=k: rbuf.at[s, k], j % 2 == 0, ys.at[0], yr, j, "y"))
        row_from.append(k)
    hid_ring = [
        ring(lambda s: hid.at[s, pl.ds(0, 96)], True, hs.at[0], hr, 0, "y"),
        ring(lambda s: hid.at[s, pl.ds(96, 96)], False, hs.at[0], hr, 1, "y"),
    ]
    weights[0][0](0)
    weights[1][0](1)
    weights[1][0](0)
    weights[0][0](1)

    for load in loads[4:10]:
        load.wait()
    moves, sums = local_mixer(rec_ref, key_ref, val_ref, dec_ref, rate_ref, off_ref, xg, yf)
    cmap[0] = moves[:64] + pltpu.roll(sums[:64], 64, 1)
    cmap[1] = pltpu.roll(moves[64:], 64, 1) + sums[64:]
    swap = copy_to(cmap.at[1 - c], pmap, ps.at[0], pr.at[0], at(c_=1 - c))
    swap.start()

    pre = dot(cgu[...], xn[...], NT)
    shb[y, x] = (silu(pre[:64]) * pre[64:]).astype(BF16)
    share_x = [
        ring(lambda s: shb.at[y, s, pl.ds(0, 32)], True, sh_s.at[0], sh_r.at[0], 0, "x"),
        ring(lambda s: shb.at[y, s, pl.ds(32, 32)], False, sh_s.at[0], sh_r.at[0], 1, "x"),
    ]
    share_y = [
        ring(lambda s: shb.at[s, pl.ds(0, 2)], True, sh_s.at[1], sh_r.at[1], 0, "y"),
        ring(lambda s: shb.at[s, pl.ds(2, 2)], False, sh_s.at[1], sh_r.at[1], 1, "y"),
    ]

    def start_both(pair):
        pair[0][0](0)
        pair[1][0](1)
        pair[1][0](0)
        pair[0][0](1)

    start_both(share_x)

    swap.wait_recv()
    lane = iota((64, 128), 1)
    first = jnp.where(c == 0, cmap[0], pmap[...])
    second = jnp.where(c == 0, pmap[...], cmap[1])

    def compose(later, earlier):
        stacked = jnp.concatenate([earlier, jnp.zeros_like(earlier)], axis=0)
        moved = dot3(halves(jnp.where(lane < 64, later, 0.0)), halves(stacked))
        return moved + jnp.where(lane < 64, 0.0, later)

    zmine[...] = compose(second, first).astype(BF16)

    def to_group(k):
        return copy_to(zmine, zmap.at[inner], zs.at[k], zr.at[inner], at(z_=RING * group + k))

    def send_group(k, _):
        to_group(k).start()
        return 0

    lax.fori_loop(inner + 1, RING, send_group, 0)

    def forward_rows(j):
        k = row_from[j]

        @pl.when(RING * k + x != ep)
        def _():
            copy_to(
                rbuf.at[y, k], rbuf.at[y, k], dsp_s.at[0], dsp_r.at[k], place(RING * k + x)
            ).wait_recv()

        row_ring[j][0](0)
        row_ring[j][0](1)

    weights[0][1]()
    weights[1][1]()
    for j in range(4):
        forward_rows(j)
    def advance(step):
        step = step.astype(F32)
        low = jnp.where(lane < 64, step, 0.0)
        twice = (low + pltpu.roll(low, 64, 1)).astype(BF16)
        k_hi, k_lo = halves(keep[...])
        moved = dot(twice, jnp.concatenate([k_hi, k_lo], axis=0))
        keep[...] = moved + jnp.where(lane < 64, 0.0, step)

    def in_group(k, _):
        copy_to(zmine, zmap.at[k], zs.at[0], zr.at[k], at(z_=RING * group + k)).wait_recv()
        advance(zmap[k])
        return 0

    def to_later(k):
        return copy_to(zlast, zall.at[group], zls.at[0], zlr.at[group], at(z_=k))

    keep[...] = (iota((64, 128), 0) == lane).astype(F32)
    lax.fori_loop(0, inner, in_group, 0)
    ahead[...] = keep[...]

    @pl.when(last)
    def _():
        advance(zmine[...])
        zlast[...] = keep[...].astype(BF16)

        def send_later(k, _):
            to_later(k).start()
            return 0

        lax.fori_loop(RING * (group + 1), nz, send_later, 0)

    share_x[0][1]()
    share_x[1][1]()
    for j in range(4, 8):
        forward_rows(j)
    for ring_of in row_ring:
        ring_of[1]()
    for ring_of in share_x:
        ring_of[2]()
        ring_of[3]()
    for load in loads[14:]:
        load.wait()
    weights[2][0](0)
    weights[3][0](1)
    weights[3][0](0)
    weights[2][0](1)

    for part in (0, 1):
        weights[part][2]()
        weights[part][3]()

    def product(slot):
        taken = rbuf[slot].astype(F32).reshape(SOURCES * CAP, 512).astype(BF16)
        span = pl.ds(pl.multiple_of(512 * slot, 512), 512)
        g = gu[:, 0:64, span].reshape(256, 512)
        u = gu[:, 64:128, span].reshape(256, 512)
        return dot(taken, g, NT), dot(taken, u, NT)

    g0, u0 = product(y)
    for ring_of in row_ring:
        ring_of[2]()
    g1, u1 = product((y + 1) % RING)
    g2, u2 = product((y + 3) % RING)
    for ring_of in row_ring:
        ring_of[3]()
    g3, u3 = product((y + 2) % RING)
    hidden = silu((g0 + g1) + (g2 + g3)) * ((u0 + u1) + (u2 + u3))
    hid[y] = hidden.astype(BF16)
    hid_ring[0][0](0)
    hid_ring[1][0](1)
    hid_ring[1][0](0)
    hid_ring[0][0](1)
    start_both(share_y)

    def over_groups(k, _):
        copy_to(zlast, zall.at[k], zls.at[0], zlr.at[k], at(z_=RING * k + 3)).wait_recv()
        advance(zall[k])
        return 0

    keep[...] = jnp.zeros((64, 128), F32)
    lax.fori_loop(0, group, over_groups, 0)
    state = jnp.where(lane < 64, 0.0, compose(ahead[...], keep[...]))
    passed = jnp.where(lane < 64, 0.0, compose(first, state))
    sts[c] = jnp.where(c == 0, state, passed)
    keep[...] = jnp.where(c == 0, passed, state)
    hand = copy_to(keep, sts.at[c], ps.at[1], pr.at[1], at(c_=1 - c))
    hand.start()
    hid_ring[0][1]()
    hid_ring[1][1]()
    weights[2][1]()
    weights[3][1]()
    share_y[0][1]()
    share_y[1][1]()
    copy_to(keep, sts.at[1 - c], ps.at[1], pr.at[1], at(c_=1 - c)).wait_recv()

    start = jnp.concatenate([pltpu.roll(sts[0], 64, 1), sts[1]], axis=0)
    readout = dot3(halves(xg[...]), halves(start)) + yf[...]
    same_head = ((iota((128, 128), 0) >> 6) == (iota((128, 128), 1) >> 6)).astype(F32)
    mean_of = (same_head * (1.0 / HEAD)).astype(BF16)
    same_head = same_head.astype(BF16)
    centred = readout - dot_exact_right(readout, mean_of)
    variance = dot_exact_right(centred * centred, mean_of)
    key = key_ref[...].astype(F32)
    bonus = dot_exact_right(rec_ref[...].astype(F32) * key * self_ref[...], same_head)
    mixed = (
        centred * lax.rsqrt(variance + 1.0) * gain_ref[...] + bonus * val_ref[...].astype(F32)
    ) * gate_ref[...].astype(F32)
    mixed = mixed.astype(BF16)

    def reduce_along(n, axis, piece, half, got_half, got_piece):
        me = y if axis == "y" else x
        right, left, across = (me + 1) % RING, (me + 3) % RING, (me + 2) % RING

        def to(way):
            side = left if way else right
            return at(y_=side) if axis == "y" else at(x_=side)

        def far(way):
            return copy_to(
                half(across, way), got_half.at[way], rs_s.at[n], rs_h.at[n, way], to(way)
            )

        def near(way):
            block = piece(left if way else right)
            return copy_to(block, got_piece.at[way], rs_s.at[n], rs_p.at[n, way], to(way))

        def first():
            far(0).start()
            far(1).start()

        def second():
            for way in range(2):
                far(way).wait_recv()
                mine_half = half(left if way else right, way)
                mine_half[...] = (
                    mine_half[...].astype(F32) + got_half[way].astype(F32)
                ).astype(BF16)
                near(way).start()

        def third():
            near(0).wait_recv()
            near(1).wait_recv()
            own_block = piece(me)[...].astype(F32)
            return own_block + got_piece[0].astype(F32) + got_piece[1].astype(F32)

        return first, second, third

    x_first = reduce_along(
        0, "x", lambda t: pb0.at[t], lambda t, h: pb0.at[t, pl.ds(2 * h, 2)], gh0, gp0
    )
    y_first = reduce_along(
        1, "y", lambda t: pb1.at[t], lambda t, h: pb1.at[t, pl.ds(2 * h, 2)], gh1, gp1
    )
    y_then = reduce_along(
        2, "y", lambda t: qb0.at[t], lambda t, h: qb0.at[t, :, pl.ds(512 * h, 512)], gh2, gp2
    )
    x_then = reduce_along(
        3, "x", lambda t: qb1.at[t], lambda t, h: qb1.at[t, :, pl.ds(512 * h, 512)], gh3, gp3
    )

    for block in range(4):
        partial = dot(mixed[64 * block : 64 * block + 64], wout[...])
        partial = partial.reshape(4, 16, 2048).astype(BF16)
        pb1[block] = partial[:, :, 1024:]
        for side in range(4):
            pb0[side, block] = partial[side, :, :1024]
    x_first[0]()
    y_first[0]()

    weights[2][2]()
    weights[3][2]()
    weights[2][3]()
    weights[3][3]()
    for ring_of in hid_ring:
        ring_of[2]()
        ring_of[3]()
    def give_back(k, s):
        return copy_to(
            obuf.at[s, k],
            retb.at[ep],
            ret_s.at[0],
            ret_r.at[0],
            place(RING * k + x, x_=s),
        )

    x_first[1]()
    y_first[1]()
    every_hidden = jnp.concatenate([hid[part] for part in range(RING)], axis=1)

    def send_back(s, away):
        k = (ep // RING + away) % SOURCES

        @pl.when(jnp.logical_not((RING * k + x == ep) & (s == x)))
        def _():
            give_back(k, s).start()

    for s in range(RING):
        made = dot(every_hidden, wd[s])
        obuf[s] = made.reshape(SOURCES, CAP, 128).astype(BF16)
        for away in (4, 3, 5, 2):
            send_back(s, away)
    for away in (6, 1, 7, 0):
        for s in range(RING):
            send_back(s, away)

    @pl.when(own)
    def _():
        retb[ep] = obuf[x, ep // RING]

    qb0[...] = x_first[2]().astype(BF16)
    y_then[0]()
    qb1[...] = y_first[2]().astype(BF16)
    x_then[0]()
    y_then[1]()
    x_then[1]()
    out0[:, :1024] = y_then[2]().astype(BF16)
    out0[:, 1024:] = x_then[2]().astype(BF16)

    for ring_of in share_y:
        ring_of[2]()
        ring_of[3]()
    shared = dot(shb[...].reshape(1024, 128), cd[...], TN)

    @pl.when(own)
    def _():
        whole(sbuf.at[pl.ds(0, EXPERTS - 1)], dsp_s.at[0], dsp_r.at[0]).wait_send()

    for sent, sem in (
        (shb.at[y, pl.ds(0, 3)], sh_s.at[0]),
        (shb.at[pl.ds(0, 3)], sh_s.at[1]),
        (gu.at[pl.ds(0, 3)], ws.at[0]),
        (wd.at[pl.ds(0, 3)], ws.at[1]),
        (rbuf.at[pl.ds(0, 3)], ys.at[0]),
        (hid.at[pl.ds(0, 3)], hs.at[0]),
        (pb0.at[pl.ds(0, 3)], rs_s.at[0]),
        (pb1.at[pl.ds(0, 3)], rs_s.at[1]),
        (qb0.at[pl.ds(0, 3)], rs_s.at[2]),
        (qb1.at[pl.ds(0, 3)], rs_s.at[3]),
    ):
        whole(sent, sem, dsp_r.at[0]).wait_send()
    swap.wait_send()
    hand.wait_send()

    def group_sent(k, _):
        to_group(k).wait_send()
        return 0

    lax.fori_loop(inner + 1, RING, group_sent, 0)
    for k in range(RING - 1):
        @pl.when(last & (group == k))
        def _():
            maps = q_hi.at[pl.ds(0, 64 * (12 - 4 * k))]
            whole(maps, zls.at[0], zlr.at[0]).wait_send()

    @pl.when(own)
    def _():
        whole(retb.at[pl.ds(0, EXPERTS - 1)], ret_s.at[0], ret_r.at[0]).wait()

    @pl.when(jnp.logical_not(own))
    def _():
        whole(retb, ret_s.at[0], ret_r.at[0]).wait()

    copies = retb[...].astype(F32).reshape(slots, 128).astype(BF16)
    merged = dot(q_hi[...], copies, TN) + dot(q_lo[...], copies, TN) + shared
    out1[...] = merged.astype(BF16)


def on_device(
    receptance,
    key_tensor,
    value_tensor,
    decay_data_input,
    correction_rate_input,
    mixer_output_gate,
    decay_channel_offset,
    head_norm_gain,
    self_key_weight,
    mixer_output_weight,
    second_batch_rows,
    routed_expert_index,
    routing_output_weight,
    expert_norm_gain,
    expert_gate_weight,
    expert_up_weight,
    expert_down_weight,
    common_expert_gate,
    common_expert_up,
    common_expert_down,
):
    hbm = pl.BlockSpec(memory_space=pl.ANY)
    vmem = pl.BlockSpec(memory_space=pltpu.VMEM)
    dma = pltpu.SemaphoreType.DMA
    rows = receptance.shape[0]
    scratch = [
        *(pltpu.VMEM((rows, 128), BF16) for _ in range(6)),
        *(pltpu.VMEM((1, 128), F32) for _ in range(3)),
        pltpu.VMEM((128, 2048), BF16),
        pltpu.VMEM((4, 128), jnp.int32),
        pltpu.VMEM((4, 128), F32),
        pltpu.VMEM((1, 2048), F32),
        pltpu.VMEM((128, 2048), BF16),
        pltpu.VMEM((RING, 128, 2048), BF16),
        pltpu.VMEM((RING, 1024, 128), BF16),
        pltpu.VMEM((128, 2048), BF16),
        pltpu.VMEM((1024, 128), BF16),
        pltpu.VMEM((128, 2048), BF16),
        pltpu.VMEM((EXPERTS, CAP, 512), BF16),
        pltpu.VMEM((RING, SOURCES, CAP, 512), BF16),
        pltpu.VMEM((RING, SOURCES * CAP, 256), BF16),
        pltpu.VMEM((RING, SOURCES, CAP, 128), BF16),
        pltpu.VMEM((EXPERTS, CAP, 128), BF16),
        pltpu.VMEM((RING, RING, 16, 1024), BF16),
        pltpu.VMEM((RING, RING, 16, 1024), BF16),
        pltpu.VMEM((RING, 16, 1024), BF16),
        pltpu.VMEM((RING, 16, 1024), BF16),
        pltpu.VMEM((2, 2, 16, 1024), BF16),
        pltpu.VMEM((2, 2, 16, 1024), BF16),
        pltpu.VMEM((2, 16, 512), BF16),
        pltpu.VMEM((2, 16, 512), BF16),
        pltpu.VMEM((2, RING, 16, 1024), BF16),
        pltpu.VMEM((2, RING, 16, 1024), BF16),
        pltpu.VMEM((2, 16, 1024), BF16),
        pltpu.VMEM((2, 16, 1024), BF16),
        pltpu.VMEM((RING, RING, 64, 128), BF16),
        pltpu.VMEM((EXPERTS * CAP, 128), BF16),
        pltpu.VMEM((EXPERTS * CAP, 128), BF16),
        pltpu.VMEM((EXPERTS * CAP, 128), BF16),
        pltpu.VMEM((256, 128), F32),
        pltpu.VMEM((256, 128), F32),
        pltpu.VMEM((2, 64, 128), F32),
        pltpu.VMEM((64, 128), F32),
        pltpu.VMEM((64, 128), BF16),
        pltpu.VMEM((RING, 64, 128), BF16),
        pltpu.VMEM((64, 128), BF16),
        pltpu.VMEM((RING, 64, 128), BF16),
        pltpu.VMEM((2, 64, 128), F32),
        pltpu.VMEM((64, 128), F32),
        pltpu.VMEM((64, 128), F32),
        dma((20,)),
        dma((1,)),
        dma((SOURCES,)),
        dma((1,)),
        dma((3, SOURCES)),
        dma((2,)),
        dma((3, 4)),
        dma((1,)),
        dma((3, 2)),
        dma((1,)),
        dma((1,)),
        dma((4,)),
        dma((4, 2)),
        dma((4, 2)),
        dma((2,)),
        dma((2, 3, 2)),
        dma((RING,)),
        dma((RING,)),
        dma((1,)),
        dma((RING,)),
        dma((2,)),
        dma((2,)),
    ]
    return pl.pallas_call(
        kernel,
        out_shape=(
            pltpu.VMEM((16, 2048), BF16),
            pltpu.VMEM((128, 128), BF16),
        ),
        in_specs=[hbm] * 20,
        out_specs=(vmem, vmem),
        scratch_shapes=scratch,
        compiler_params=pltpu.CompilerParams(
            collective_id=0, has_side_effects=True, vmem_limit_bytes=60 * 1024 * 1024
        ),
        name="mixer_and_experts",
    )(
        receptance,
        key_tensor,
        value_tensor,
        decay_data_input,
        correction_rate_input,
        mixer_output_gate,
        decay_channel_offset.reshape(1, 128),
        head_norm_gain.reshape(1, 128),
        self_key_weight.reshape(1, 128),
        mixer_output_weight,
        second_batch_rows,
        routed_expert_index.T,
        routing_output_weight.T,
        expert_norm_gain.reshape(1, 2048),
        expert_gate_weight,
        expert_up_weight,
        expert_down_weight,
        common_expert_gate,
        common_expert_up,
        common_expert_down,
    )


def solution(mesh):
    split = Mesh(mesh.devices.reshape(16, 2, 4, 4), ("z", "c", "y", "x"))
    in_specs = (
        P(EP, TP),
        P(EP, TP),
        P(EP, TP),
        P(EP, TP),
        P(EP, TP),
        P(EP, TP),
        P(TP),
        P(TP),
        P(TP),
        P(TP, None),
        P(EP, None),
        P(EP, None),
        P(EP, None),
        P(),
        P(EP, TP, None),
        P(EP, TP, None),
        P(EP, None, TP),
        P(TP, None),
        P(TP, None),
        P(None, TP),
    )
    out_specs = (P(EP + TP, None), P(EP, TP))
    return jax.shard_map(
        on_device, mesh=split, in_specs=in_specs, out_specs=out_specs, check_vma=False
    )
```

```python
import functools

import jax
import jax.numpy as jnp
from jax import lax
from jax.experimental import pallas as pl
from jax.experimental.pallas import tpu as pltpu
from jax.sharding import Mesh
from jax.sharding import PartitionSpec as P

F32 = jnp.float32
BF16 = jnp.bfloat16
HEAD = 64
CHUNK = 64
RING = 4
CAP = 24
EXPERTS = 32
SOURCES = 8
MESH = pl.DeviceIdType.MESH
EP = ("z", "c")
TP = ("y", "x")
NN = (((1,), (0,)), ((), ()))
NT = (((1,), (1,)), ((), ()))
TN = (((0,), (0,)), ((), ()))


def dot(a, b, dims=NN):
    return lax.dot_general(a, b, dims, preferred_element_type=F32)


def halves(a):
    high = a.astype(BF16)
    return high, (a - high.astype(F32)).astype(BF16)


def dot3(a, b, dims=NN):
    (ah, al), (bh, bl) = a, b
    return dot(ah, bh, dims) + (dot(ah, bl, dims) + dot(al, bh, dims))


def dot_exact_left(a, b):
    b1 = b.astype(BF16)
    rest = b - b1.astype(F32)
    b2 = rest.astype(BF16)
    b3 = (rest - b2.astype(F32)).astype(BF16)
    return dot(a, b1) + (dot(a, b2) + dot(a, b3))


def dot_exact_right(a, b):
    ah, al = halves(a)
    return dot(ah, b) + dot(al, b)


def iota(shape, dim):
    return lax.broadcasted_iota(jnp.int32, shape, dim)


def copy_to(src, dst, send_sem, recv_sem, device):
    return pltpu.make_async_remote_copy(
        src_ref=src,
        dst_ref=dst,
        send_sem=send_sem,
        recv_sem=recv_sem,
        device_id=device,
        device_id_type=MESH,
    )


def silu(v):
    return v / (1.0 + jnp.exp(-v))


def local_mixer(rec_ref, key_ref, val_ref, dec_ref, rate_ref, off_ref, xg, yf):
    n = 2 * CHUNK
    rows = rec_ref.shape[0]
    chunks = rows // CHUNK
    lane_head = iota((1, 128), 1) >> 6
    m0 = (lane_head == 0).astype(F32)
    m1 = 1.0 - m0
    same_head = ((iota((128, 128), 0) >> 6) == (iota((128, 128), 1) >> 6)).astype(BF16)
    i, j = iota((n, n), 0), iota((n, n), 1)
    eye = (i == j).astype(F32)
    same = (i >> 6) == (j >> 6)
    below = (i > j) & same
    upto = (i >= j) & same
    ri, rj = iota((rows, rows), 0), iota((rows, rows), 1)
    tri = ((ri >= rj) & ((ri >> 6) == (rj >> 6))).astype(F32).astype(BF16)

    key = key_ref[...].astype(F32)
    logw = -0.6065306597126334 / (1.0 + jnp.exp(-(off_ref[...] + dec_ref[...].astype(F32))))
    cum = dot_exact_left(tri, logw)
    rate = 1.0 / (1.0 + jnp.exp(-rate_ref[...].astype(F32)))
    unit = key * lax.rsqrt(dot_exact_right(key * key, same_head) + 1.0)
    b = unit * rate
    up = jnp.exp(cum)
    down = jnp.exp(-cum)
    u_t = unit * jnp.exp(cum - logw)
    r_t = rec_ref[...].astype(F32) * up
    k_t = key * down
    b_t = b * down
    value = val_ref[...].astype(F32)

    def part(a, at):
        return a[at * CHUNK : (at + 1) * CHUNK]

    def both(a):
        return jnp.concatenate([a * m0, a * m1], axis=0)

    every = range(chunks)
    end = [jnp.exp(part(cum, at)[CHUNK - 1 :]) for at in every]
    v2 = [both(part(value, at)) for at in every]
    v2h = [a.astype(BF16) for a in v2]
    u2 = [both(part(u_t, at)) for at in every]
    r2 = [both(part(r_t, at)) for at in every]
    b2 = [both(part(b_t, at)) for at in every]
    k2 = [both(part(k_t, at)) for at in every]
    left = [halves(jnp.concatenate([u2[at], r2[at]], axis=0)) for at in every]
    right = [halves(jnp.concatenate([b2[at], k2[at]], axis=0)) for at in every]
    pairs = [dot3(left[at], right[at], NT) for at in every]
    lower = [jnp.where(below, pairs[at][:n, :n], 0.0) for at in every]
    m_uk = [halves(jnp.where(below, pairs[at][:n, n:], 0.0)) for at in every]
    a_b = [halves(jnp.where(upto, pairs[at][n:, :n], 0.0)) for at in every]
    a_k = [halves(jnp.where(upto, pairs[at][n:, n:], 0.0)) for at in every]
    mv = [dot(m_uk[at][0], v2h[at]) + dot(m_uk[at][1], v2h[at]) for at in every]
    akv = [dot(a_k[at][0], v2h[at]) + dot(a_k[at][1], v2h[at]) for at in every]
    inverse = None
    for level in range(6):
        half = (
            ((i >> (level + 1)) == (j >> (level + 1)))
            & (((i >> level) & 1) == 1)
            & (((j >> level) & 1) == 0)
        )
        step = [jnp.where(half, lower[at], 0.0) for at in every]
        if inverse is None:
            inverse = [eye - step[at] for at in every]
        else:
            split = [halves(inverse[at]) for at in every]
            mid = [dot3(halves(step[at]), split[at]) for at in every]
            inverse = [
                inverse[at] - dot3(split[at], halves(mid[at])) for at in every
            ]
    ez = [
        halves(dot3(halves(inverse[at]), halves(jnp.concatenate([u2[at], mv[at]], axis=1))))
        for at in every
    ]
    aez = [dot3(a_b[at], ez[at]) for at in every]
    b_end = [halves(b2[at] * end[at]) for at in every]
    k_end = [halves(k2[at] * end[at]) for at in every]
    bez = [dot3(b_end[at], ez[at], TN) for at in every]
    kv = [dot(k_end[at][0], v2h[at], TN) + dot(k_end[at][1], v2h[at], TN) for at in every]
    total = None
    for at in every:
        xo = r2[at] - aez[at][:, :128]
        yo = akv[at] - aez[at][:, 128:]
        xo = xo[:CHUNK] + xo[CHUNK:]
        yo = yo[:CHUNK] + yo[CHUNK:]
        moves = eye * end[at] - bez[at][:, :128]
        sums = kv[at] - bez[at][:, 128:]
        if total is None:
            xg[pl.ds(at * CHUNK, CHUNK), :] = xo
            yf[pl.ds(at * CHUNK, CHUNK), :] = yo
            total = jnp.concatenate([moves, sums], axis=1)
        else:
            ahead = halves(total)
            read = dot3(halves(xo), ahead)
            xg[pl.ds(at * CHUNK, CHUNK), :] = read[:, :128]
            yf[pl.ds(at * CHUNK, CHUNK), :] = read[:, 128:] + yo
            moved = dot3(halves(moves), ahead)
            total = jnp.concatenate([moved[:, :128], moved[:, 128:] + sums], axis=1)
    return total[:, :128], total[:, 128:]


def kernel(*refs):
    (
        rec_in,
        key_in,
        val_in,
        dec_in,
        rate_in,
        gate_in,
        off_in,
        gain_in,
        self_in,
        wout_in,
        rows_in,
        idx_in,
        wgt_in,
        egain_in,
        eg_in,
        eu_in,
        ed_in,
        cg_in,
        cu_in,
        cd_in,
        out0,
        out1,
    ) = refs[:22]
    (
        rec_ref,
        key_ref,
        val_ref,
        dec_ref,
        rate_ref,
        gate_ref,
        off_ref,
        gain_ref,
        self_ref,
        rows_ref,
        idx_ref,
        wgt_ref,
        egain_ref,
        wout,
        gu,
        wd,
        cgu,
        cd,
        xn,
        sbuf,
        rbuf,
        hid,
        obuf,
        retb,
        pb0,
        pb1,
        qb0,
        qb1,
        gh0,
        gh1,
        gp0,
        gp1,
        gp2,
        gp3,
        shb,
        q_hi,
        q_lo,
        onehot,
        xg,
        yf,
        cmap,
        pmap,
        zmine,
        zmap,
        zlast,
        zall,
        sts,
        keep,
        ahead,
    ) = refs[22:71]
    (
        ld,
        dsp_s,
        dsp_r,
        ys,
        yr,
        ws,
        wr,
        hs,
        hr,
        ret_s,
        ret_r,
        rs_s,
        rs_h,
        rs_p,
        sh_s,
        sh_r,
        zs,
        zr,
        zls,
        zlr,
        ps,
        pr,
    ) = refs[71:]
    z, c = lax.axis_index("z"), lax.axis_index("c")
    y, x = lax.axis_index("y"), lax.axis_index("x")
    nz = lax.axis_size("z")
    ep, tp = 2 * z + c, RING * y + x
    home = ep % RING
    own = home == x
    mine = jnp.where(own, 1, 0)
    group, inner = z // RING, z % RING
    last = inner == RING - 1

    def at(z_=None, c_=None, y_=None, x_=None):
        return {
            "z": z if z_ is None else z_,
            "c": c if c_ is None else c_,
            "y": y if y_ is None else y_,
            "x": x if x_ is None else x_,
        }

    def place(e, y_=None, x_=None):
        return at(e // 2, e % 2, y_, x_)

    def whole(ref, send_sem, recv_sem):
        return copy_to(ref, ref, send_sem, recv_sem, at(c_=1 - c))

    loads = []
    for source, target in (
        (rows_in, rows_ref),
        (egain_in, egain_ref),
        (idx_in, idx_ref),
        (wgt_in, wgt_ref),
        (key_in, key_ref),
        (dec_in, dec_ref),
        (off_in, off_ref),
        (rate_in, rate_ref),
        (rec_in, rec_ref),
        (val_in, val_ref),
        (eg_in.at[0], gu.at[x, pl.ds(0, 64)]),
        (eu_in.at[0], gu.at[x, pl.ds(64, 64)]),
        (cg_in, cgu.at[pl.ds(0, 64)]),
        (cu_in, cgu.at[pl.ds(64, 64)]),
        (ed_in.at[0], wd.at[x]),
        (cd_in, cd),
        (wout_in, wout),
        (gate_in, gate_ref),
        (gain_in, gain_ref),
        (self_in, self_ref),
    ):
        count = len(loads)
        slot = count if count < 10 else 10 if count < 14 else 11 if count < 17 else count - 5
        loads.append(pltpu.make_async_copy(source, target, ld.at[slot]))
        loads[-1].start()

    barrier = pltpu.get_barrier_semaphore()

    def tell(device):
        pl.semaphore_signal(barrier, inc=1, device_id=device, device_id_type=MESH)

    def tell_source(k, _):
        source = RING * ((ep // RING + 4 + k) % SOURCES) + x

        @pl.when(source != ep)
        def _():
            tell(place(source))

        return 0

    lax.fori_loop(0, SOURCES, tell_source, 0)

    def tell_group(k, _):
        tell(at(z_=RING * group + k))
        return 0

    lax.fori_loop(0, inner, tell_group, 0)
    for k in range(1, RING):
        tell(at(x_=(x + k) % RING))
    for k in (1, 3):
        tell(at(y_=(y + k) % RING))
    tell(at(c_=1 - c))

    for load in loads[2:4]:
        load.wait()
    row_count = rows_ref.shape[0]
    slots = EXPERTS * CAP
    expert_at = iota((EXPERTS, row_count), 0)
    chosen = jnp.zeros((EXPERTS, row_count), F32)
    weight = jnp.zeros((EXPERTS, row_count), F32)
    for k in range(4):
        hit = idx_ref[k : k + 1, :] == expert_at
        chosen = jnp.where(hit, 1.0, chosen)
        weight = jnp.where(hit, wgt_ref[k : k + 1, :], weight)
    earlier = iota((row_count, row_count), 0) < iota((row_count, row_count), 1)
    rank = dot(chosen.astype(BF16), earlier.astype(F32).astype(BF16))
    label = jnp.where(chosen > 0.0, rank, -1.0).astype(BF16)
    slot_s, slot_e = iota((slots, EXPERTS), 0), iota((slots, EXPERTS), 1)
    spread = ((slot_s >= slot_e * CAP) & (slot_s < slot_e * CAP + CAP)).astype(F32)
    within = jnp.sum(spread * (slot_s - slot_e * CAP).astype(F32), axis=1, keepdims=True)
    spread = spread.astype(BF16)
    placed = (dot(spread, label) == within).astype(F32)
    w_hi, w_lo = halves(weight)
    q_hi[...] = (placed * dot(spread, w_hi)).astype(BF16)
    q_lo[...] = (placed * dot(spread, w_lo)).astype(BF16)
    onehot[...] = placed.astype(BF16)

    for load in loads[:2]:
        load.wait()
    rows = rows_ref[...].astype(F32)
    scale = lax.rsqrt(jnp.mean(rows * rows, axis=-1, keepdims=True) + 1.0)
    xn[...] = (rows * scale * egain_ref[...]).astype(BF16)

    @pl.when(own)
    def _():
        features = xn[:, pl.ds(pl.multiple_of(512 * y, 512), 512)]
        packed = dot(onehot[...], features)
        sbuf[...] = packed.reshape(EXPERTS, CAP, 512).astype(BF16)
        rbuf[y, ep // RING] = sbuf[ep]

    pltpu.make_async_copy(gu.at[pl.ds(0, 2)], gu.at[pl.ds(0, 2)], ld.at[10]).wait()

    pl.semaphore_wait(barrier, 5 + 1 + (3 - inner) + 31 * mine)

    def dispatch(e):
        return copy_to(
            sbuf.at[e], rbuf.at[y, ep // RING], dsp_s.at[0], dsp_r.at[ep // RING], place(e)
        )

    @pl.when(own)
    def _():
        dispatch((ep + 16) % EXPERTS).start()

        def send(k, _):
            dispatch((ep + 16 - k) % EXPERTS).start()
            dispatch((ep + 16 + k) % EXPERTS).start()
            return 0

        lax.fori_loop(1, 16, send, 0)

    def ring(piece, first_half, send_sem, recv_sem, p, axis):
        me = y if axis == "y" else x
        right, left, across = (me + 1) % RING, (me + 3) % RING, (me + 2) % RING

        def move(slot, way, to):
            device = at(y_=to) if axis == "y" else at(x_=to)
            return copy_to(piece(slot), piece(slot), send_sem, recv_sem.at[way, p], device)

        def start(way):
            move(me, way, left if way else right).start()

        def relay():
            if first_half:
                move(left, 0, right).wait_recv()
                move(left, 2, right).start()
            else:
                move(right, 1, left).wait_recv()
                move(right, 2, left).start()

        def near():
            if first_half:
                move(right, 1, left).wait_recv()
            else:
                move(left, 0, right).wait_recv()

        def far():
            move(across, 2, right).wait_recv()

        return start, relay, near, far

    weights = [
        ring(lambda s: gu.at[s, pl.ds(0, 64)], True, ws.at[0], wr, 0, "x"),
        ring(lambda s: gu.at[s, pl.ds(64, 64)], False, ws.at[0], wr, 1, "x"),
        ring(lambda s: wd.at[s, pl.ds(0, 512)], True, ws.at[1], wr, 2, "x"),
        ring(lambda s: wd.at[s, pl.ds(512, 512)], False, ws.at[1], wr, 3, "x"),
    ]
    row_ring, row_from = [], []
    for j, away in enumerate((4, 3, 5, 2, 6, 1, 7, 0)):
        k = (ep // RING + away) % SOURCES
        row_ring.append(ring(lambda s, k=k: rbuf.at[s, k], j % 2 == 0, ys.at[0], yr, j, "y"))
        row_from.append(k)
    hid_ring = [
        [
            ring(
                lambda s, h=h, p=p: hid.at[h, s, pl.ds(48 * p, 48)],
                p == 0,
                hs.at[h],
                hr.at[h],
                p,
                "y",
            )
            for p in range(2)
        ]
        for h in range(2)
    ]
    weights[0][0](0)
    weights[1][0](1)
    weights[1][0](0)
    weights[0][0](1)

    for load in loads[4:10]:
        load.wait()
    moves, sums = local_mixer(rec_ref, key_ref, val_ref, dec_ref, rate_ref, off_ref, xg, yf)
    cmap[0] = moves[:64] + pltpu.roll(sums[:64], 64, 1)
    cmap[1] = pltpu.roll(moves[64:], 64, 1) + sums[64:]
    swap = copy_to(cmap.at[1 - c], pmap, ps.at[0], pr.at[0], at(c_=1 - c))
    swap.start()

    pre = dot(cgu[...], xn[...], NT)
    shb[y, x] = (silu(pre[:64]) * pre[64:]).astype(BF16)
    share_x = [
        ring(lambda s: shb.at[y, s, pl.ds(0, 32)], True, sh_s.at[0], sh_r.at[0], 0, "x"),
        ring(lambda s: shb.at[y, s, pl.ds(32, 32)], False, sh_s.at[0], sh_r.at[0], 1, "x"),
    ]
    share_y = [
        ring(lambda s: shb.at[s, pl.ds(0, 2)], True, sh_s.at[1], sh_r.at[1], 0, "y"),
        ring(lambda s: shb.at[s, pl.ds(2, 2)], False, sh_s.at[1], sh_r.at[1], 1, "y"),
    ]

    def start_both(pair):
        pair[0][0](0)
        pair[1][0](1)
        pair[1][0](0)
        pair[0][0](1)

    start_both(share_x)

    swap.wait_recv()
    lane = iota((64, 128), 1)
    first = jnp.where(c == 0, cmap[0], pmap[...])
    second = jnp.where(c == 0, pmap[...], cmap[1])

    def compose(later, earlier):
        stacked = jnp.concatenate([earlier, jnp.zeros_like(earlier)], axis=0)
        moved = dot3(halves(jnp.where(lane < 64, later, 0.0)), halves(stacked))
        return moved + jnp.where(lane < 64, 0.0, later)

    zmine[...] = compose(second, first).astype(BF16)

    def to_group(k):
        return copy_to(zmine, zmap.at[inner], zs.at[k], zr.at[inner], at(z_=RING * group + k))

    def send_group(k, _):
        to_group(k).start()
        return 0

    lax.fori_loop(inner + 1, RING, send_group, 0)

    def forward_rows(j):
        k = row_from[j]

        def arrived():
            copy_to(
                rbuf.at[y, k], rbuf.at[y, k], dsp_s.at[0], dsp_r.at[k], place(RING * k + x)
            ).wait_recv()

        if j < SOURCES - 1:
            arrived()
        else:
            pl.when(jnp.logical_not(own))(arrived)

        row_ring[j][0](0)
        row_ring[j][0](1)

    weights[0][1]()
    weights[1][1]()
    for j in range(4):
        forward_rows(j)
    def advance(step):
        step = step.astype(F32)
        low = jnp.where(lane < 64, step, 0.0)
        twice = (low + pltpu.roll(low, 64, 1)).astype(BF16)
        k_hi, k_lo = halves(keep[...])
        moved = dot(twice, jnp.concatenate([k_hi, k_lo], axis=0))
        keep[...] = moved + jnp.where(lane < 64, 0.0, step)

    def in_group(k, _):
        copy_to(zmine, zmap.at[k], zs.at[0], zr.at[k], at(z_=RING * group + k)).wait_recv()
        advance(zmap[k])
        return 0

    def to_later(k):
        return copy_to(zlast, zall.at[group], zls.at[0], zlr.at[group], at(z_=k))

    keep[...] = (iota((64, 128), 0) == lane).astype(F32)
    lax.fori_loop(0, inner, in_group, 0)
    ahead[...] = keep[...]

    @pl.when(last)
    def _():
        advance(zmine[...])
        zlast[...] = keep[...].astype(BF16)

        def send_later(k, _):
            to_later(k).start()
            return 0

        lax.fori_loop(RING * (group + 1), nz, send_later, 0)

    for j in range(4, 8):
        forward_rows(j)
    pltpu.make_async_copy(wd, wd, ld.at[11]).wait()
    for load in loads[17:]:
        load.wait()
    weights[2][0](0)
    weights[3][0](1)
    weights[3][0](0)
    weights[2][0](1)

    for ring_of in row_ring:
        ring_of[1]()
    share_x[0][1]()
    share_x[1][1]()
    for part in (0, 1):
        weights[part][2]()
        weights[part][3]()

    def product(slot, h):
        taken = [rbuf[slot, row_from[j]].astype(F32) for j in range(4 * h, 4 * h + 4)]
        taken = jnp.concatenate(taken, axis=0).astype(BF16)
        span = pl.ds(pl.multiple_of(512 * slot, 512), 512)
        g = gu[:, 0:64, span].reshape(256, 512)
        u = gu[:, 64:128, span].reshape(256, 512)
        return dot(taken, g, NT), dot(taken, u, NT)

    for h in range(2):
        for ring_of in row_ring[4 * h : 4 * h + 4]:
            ring_of[2]()
            ring_of[3]()
        g0, u0 = product(y, h)
        g1, u1 = product((y + 1) % RING, h)
        g2, u2 = product((y + 3) % RING, h)
        g3, u3 = product((y + 2) % RING, h)
        hidden = silu((g0 + g1) + (g2 + g3)) * ((u0 + u1) + (u2 + u3))
        hid[h, y] = hidden.astype(BF16)
        start_both(hid_ring[h])
        if h == 0:
            weights[2][1]()
            weights[3][1]()

    def over_groups(k, _):
        copy_to(zlast, zall.at[k], zls.at[0], zlr.at[k], at(z_=RING * k + 3)).wait_recv()
        advance(zall[k])
        return 0

    keep[...] = jnp.zeros((64, 128), F32)
    lax.fori_loop(0, group, over_groups, 0)
    state = jnp.where(lane < 64, 0.0, compose(ahead[...], keep[...]))
    passed = jnp.where(lane < 64, 0.0, compose(first, state))
    sts[c] = jnp.where(c == 0, state, passed)
    keep[...] = jnp.where(c == 0, passed, state)
    hand = copy_to(keep, sts.at[c], ps.at[1], pr.at[1], at(c_=1 - c))
    hand.start()
    hid_ring[0][0][1]()
    hid_ring[0][1][1]()
    copy_to(keep, sts.at[1 - c], ps.at[1], pr.at[1], at(c_=1 - c)).wait_recv()

    start = jnp.concatenate([pltpu.roll(sts[0], 64, 1), sts[1]], axis=0)
    readout = dot3(halves(xg[...]), halves(start)) + yf[...]
    same_head = ((iota((128, 128), 0) >> 6) == (iota((128, 128), 1) >> 6)).astype(F32)
    mean_of = (same_head * (1.0 / HEAD)).astype(BF16)
    same_head = same_head.astype(BF16)
    centred = readout - dot_exact_right(readout, mean_of)
    variance = dot_exact_right(centred * centred, mean_of)
    key = key_ref[...].astype(F32)
    bonus = dot_exact_right(rec_ref[...].astype(F32) * key * self_ref[...], same_head)
    mixed = (
        centred * lax.rsqrt(variance + 1.0) * gain_ref[...] + bonus * val_ref[...].astype(F32)
    ) * gate_ref[...].astype(F32)
    mixed = mixed.astype(BF16)

    def reduce_along(n, axis, piece, half, got_half, got_piece):
        me = y if axis == "y" else x
        right, left, across = (me + 1) % RING, (me + 3) % RING, (me + 2) % RING

        def to(way):
            side = left if way else right
            return at(y_=side) if axis == "y" else at(x_=side)

        def far(way):
            return copy_to(
                half(across, way), got_half.at[way], rs_s.at[n], rs_h.at[n, way], to(way)
            )

        def near(way):
            block = piece(left if way else right)
            return copy_to(block, got_piece.at[way], rs_s.at[n], rs_p.at[n, way], to(way))

        def first():
            far(0).start()
            far(1).start()

        def second():
            for way in range(2):
                far(way).wait_recv()
                mine_half = half(left if way else right, way)
                mine_half[...] = (
                    mine_half[...].astype(F32) + got_half[way].astype(F32)
                ).astype(BF16)
                near(way).start()

        def third():
            near(0).wait_recv()
            near(1).wait_recv()
            own_block = piece(me)[...].astype(F32)
            return own_block + got_piece[0].astype(F32) + got_piece[1].astype(F32)

        return first, second, third

    x_first = reduce_along(
        0, "x", lambda t: pb0.at[t], lambda t, h: pb0.at[t, pl.ds(2 * h, 2)], gh0, gp0
    )
    y_first = reduce_along(
        1, "y", lambda t: pb1.at[t], lambda t, h: pb1.at[t, pl.ds(2 * h, 2)], gh1, gp1
    )
    def spread_along(n, axis, blocks, got):
        me = y if axis == "y" else x

        def start():
            for k in (2, 1, 3):
                to = (me + k) % RING
                device = at(y_=to) if axis == "y" else at(x_=to)
                copy_to(blocks.at[to], got.at[k - 1], rs_s.at[n], rs_h.at[n, 0], device).start()

        def finish():
            whole(got, rs_s.at[n], rs_h.at[n, 0]).wait_recv()
            total = blocks[me].astype(F32)
            for k in range(3):
                total = total + got[k].astype(F32)
            return total

        return start, finish

    y_then = spread_along(2, "y", qb0, gp2)
    x_then = spread_along(3, "x", qb1, gp3)

    for block in range(4):
        partial = dot(mixed[64 * block : 64 * block + 64], wout[...])
        partial = partial.reshape(4, 16, 2048).astype(BF16)
        pb1[block] = partial[:, :, 1024:]
        for side in range(4):
            pb0[side, block] = partial[side, :, :1024]
    hid_ring[1][0][1]()
    hid_ring[1][1][1]()
    x_first[0]()
    y_first[0]()

    for part in (2, 3):
        weights[part][2]()
        weights[part][3]()

    def give_back(j, s):
        return copy_to(
            obuf.at[s, j],
            retb.at[ep],
            ret_s.at[0],
            ret_r.at[0],
            place(RING * row_from[j] + x, x_=s),
        )

    def second_product(h):
        for ring_of in hid_ring[h]:
            ring_of[2]()
            ring_of[3]()
        hidden = jnp.concatenate([hid[h, part] for part in range(RING)], axis=1)
        for s in range(RING):
            made = dot(hidden, wd[s])
            obuf[s, 4 * h : 4 * h + 4] = made.reshape(4, CAP, 128).astype(BF16)
            for j in range(4 * h, 4 * h + 4):
                back = give_back(j, s)
                if j < SOURCES - 1:
                    back.start()
                else:
                    pl.when(jnp.logical_not(own & (s == x)))(back.start)

    second_product(0)
    for ring_of in share_x:
        ring_of[2]()
        ring_of[3]()
    second_product(1)
    start_both(share_y)

    @pl.when(own)
    def _():
        retb[ep] = obuf[x, SOURCES - 1]

    x_first[1]()
    y_first[1]()
    qb0[...] = x_first[2]().astype(BF16)
    y_then[0]()
    qb1[...] = y_first[2]().astype(BF16)
    x_then[0]()
    share_y[0][1]()
    share_y[1][1]()
    out0[:, :1024] = y_then[1]().astype(BF16)
    out0[:, 1024:] = x_then[1]().astype(BF16)

    for ring_of in share_y:
        ring_of[2]()
        ring_of[3]()
    shared = dot(shb[...].reshape(1024, 128), cd[...], TN)

    @pl.when(own)
    def _():
        whole(sbuf.at[pl.ds(0, EXPERTS - 1)], dsp_s.at[0], dsp_r.at[0]).wait_send()

    for sent, sem in (
        (shb.at[y, pl.ds(0, 3)], sh_s.at[0]),
        (shb.at[pl.ds(0, 3)], sh_s.at[1]),
        (gu.at[pl.ds(0, 3)], ws.at[0]),
        (wd.at[pl.ds(0, 3)], ws.at[1]),
        (rbuf.at[pl.ds(0, 3)], ys.at[0]),
        (hid.at[0, pl.ds(0, 3)], hs.at[0]),
        (hid.at[1, pl.ds(0, 3)], hs.at[1]),
        (pb0.at[pl.ds(0, 3)], rs_s.at[0]),
        (pb1.at[pl.ds(0, 3)], rs_s.at[1]),
        (qb0.at[pl.ds(0, 3)], rs_s.at[2]),
        (qb1.at[pl.ds(0, 3)], rs_s.at[3]),
    ):
        whole(sent, sem, dsp_r.at[0]).wait_send()
    swap.wait_send()
    hand.wait_send()

    def group_sent(k, _):
        to_group(k).wait_send()
        return 0

    lax.fori_loop(inner + 1, RING, group_sent, 0)
    for k in range(RING - 1):
        @pl.when(last & (group == k))
        def _():
            maps = q_hi.at[pl.ds(0, 64 * (12 - 4 * k))]
            whole(maps, zls.at[0], zlr.at[0]).wait_send()

    @pl.when(own)
    def _():
        whole(retb.at[pl.ds(0, EXPERTS - 1)], ret_s.at[0], ret_r.at[0]).wait()

    @pl.when(jnp.logical_not(own))
    def _():
        whole(retb, ret_s.at[0], ret_r.at[0]).wait()

    copies = retb[...].astype(F32).reshape(slots, 128).astype(BF16)
    merged = dot(q_hi[...], copies, TN) + dot(q_lo[...], copies, TN) + shared
    out1[...] = merged.astype(BF16)


def on_device(
    receptance,
    key_tensor,
    value_tensor,
    decay_data_input,
    correction_rate_input,
    mixer_output_gate,
    decay_channel_offset,
    head_norm_gain,
    self_key_weight,
    mixer_output_weight,
    second_batch_rows,
    routed_expert_index,
    routing_output_weight,
    expert_norm_gain,
    expert_gate_weight,
    expert_up_weight,
    expert_down_weight,
    common_expert_gate,
    common_expert_up,
    common_expert_down,
):
    hbm = pl.BlockSpec(memory_space=pl.ANY)
    vmem = pl.BlockSpec(memory_space=pltpu.VMEM)
    dma = pltpu.SemaphoreType.DMA
    rows = receptance.shape[0]
    scratch = [
        *(pltpu.VMEM((rows, 128), BF16) for _ in range(6)),
        *(pltpu.VMEM((1, 128), F32) for _ in range(3)),
        pltpu.VMEM((128, 2048), BF16),
        pltpu.VMEM((4, 128), jnp.int32),
        pltpu.VMEM((4, 128), F32),
        pltpu.VMEM((1, 2048), F32),
        pltpu.VMEM((128, 2048), BF16),
        pltpu.VMEM((RING, 128, 2048), BF16),
        pltpu.VMEM((RING, 1024, 128), BF16),
        pltpu.VMEM((128, 2048), BF16),
        pltpu.VMEM((1024, 128), BF16),
        pltpu.VMEM((128, 2048), BF16),
        pltpu.VMEM((EXPERTS, CAP, 512), BF16),
        pltpu.VMEM((RING, SOURCES, CAP, 512), BF16),
        pltpu.VMEM((2, RING, SOURCES * CAP // 2, 256), BF16),
        pltpu.VMEM((RING, SOURCES, CAP, 128), BF16),
        pltpu.VMEM((EXPERTS, CAP, 128), BF16),
        pltpu.VMEM((RING, RING, 16, 1024), BF16),
        pltpu.VMEM((RING, RING, 16, 1024), BF16),
        pltpu.VMEM((RING, 16, 1024), BF16),
        pltpu.VMEM((RING, 16, 1024), BF16),
        pltpu.VMEM((2, 2, 16, 1024), BF16),
        pltpu.VMEM((2, 2, 16, 1024), BF16),
        pltpu.VMEM((2, RING, 16, 1024), BF16),
        pltpu.VMEM((2, RING, 16, 1024), BF16),
        pltpu.VMEM((3, 16, 1024), BF16),
        pltpu.VMEM((3, 16, 1024), BF16),
        pltpu.VMEM((RING, RING, 64, 128), BF16),
        pltpu.VMEM((EXPERTS * CAP, 128), BF16),
        pltpu.VMEM((EXPERTS * CAP, 128), BF16),
        pltpu.VMEM((EXPERTS * CAP, 128), BF16),
        pltpu.VMEM((256, 128), F32),
        pltpu.VMEM((256, 128), F32),
        pltpu.VMEM((2, 64, 128), F32),
        pltpu.VMEM((64, 128), F32),
        pltpu.VMEM((64, 128), BF16),
        pltpu.VMEM((RING, 64, 128), BF16),
        pltpu.VMEM((64, 128), BF16),
        pltpu.VMEM((RING, 64, 128), BF16),
        pltpu.VMEM((2, 64, 128), F32),
        pltpu.VMEM((64, 128), F32),
        pltpu.VMEM((64, 128), F32),
        dma((15,)),
        dma((1,)),
        dma((SOURCES,)),
        dma((1,)),
        dma((3, SOURCES)),
        dma((2,)),
        dma((3, 4)),
        dma((2,)),
        dma((2, 3, 2)),
        dma((1,)),
        dma((1,)),
        dma((4,)),
        dma((4, 2)),
        dma((2, 2)),
        dma((2,)),
        dma((2, 3, 2)),
        dma((RING,)),
        dma((RING,)),
        dma((1,)),
        dma((RING,)),
        dma((2,)),
        dma((2,)),
    ]
    return pl.pallas_call(
        kernel,
        out_shape=(
            pltpu.VMEM((16, 2048), BF16),
            pltpu.VMEM((128, 128), BF16),
        ),
        in_specs=[hbm] * 20,
        out_specs=(vmem, vmem),
        scratch_shapes=scratch,
        compiler_params=pltpu.CompilerParams(
            collective_id=0, has_side_effects=True, vmem_limit_bytes=60 * 1024 * 1024
        ),
        name="mixer_and_experts",
    )(
        receptance,
        key_tensor,
        value_tensor,
        decay_data_input,
        correction_rate_input,
        mixer_output_gate,
        decay_channel_offset.reshape(1, 128),
        head_norm_gain.reshape(1, 128),
        self_key_weight.reshape(1, 128),
        mixer_output_weight,
        second_batch_rows,
        routed_expert_index.T,
        routing_output_weight.T,
        expert_norm_gain.reshape(1, 2048),
        expert_gate_weight,
        expert_up_weight,
        expert_down_weight,
        common_expert_gate,
        common_expert_up,
        common_expert_down,
    )


def solution(mesh):
    split = Mesh(mesh.devices.reshape(16, 2, 4, 4), ("z", "c", "y", "x"))
    in_specs = (
        P(EP, TP),
        P(EP, TP),
        P(EP, TP),
        P(EP, TP),
        P(EP, TP),
        P(EP, TP),
        P(TP),
        P(TP),
        P(TP),
        P(TP, None),
        P(EP, None),
        P(EP, None),
        P(EP, None),
        P(),
        P(EP, TP, None),
        P(EP, TP, None),
        P(EP, None, TP),
        P(TP, None),
        P(TP, None),
        P(None, TP),
    )
    out_specs = (P(EP + TP, None), P(EP, TP))
    return jax.shard_map(
        on_device, mesh=split, in_specs=in_specs, out_specs=out_specs, check_vma=False
    )
```

```python
import functools

import jax
import jax.numpy as jnp
from jax import lax
from jax.experimental import pallas as pl
from jax.experimental.pallas import tpu as pltpu
from jax.sharding import Mesh
from jax.sharding import PartitionSpec as P

F32 = jnp.float32
BF16 = jnp.bfloat16
HEAD = 64
CHUNK = 64
RING = 4
CAP = 24
EXPERTS = 32
SOURCES = 8
MESH = pl.DeviceIdType.MESH
EP = ("z", "c")
TP = ("y", "x")
NN = (((1,), (0,)), ((), ()))
NT = (((1,), (1,)), ((), ()))
TN = (((0,), (0,)), ((), ()))


def dot(a, b, dims=NN):
    return lax.dot_general(a, b, dims, preferred_element_type=F32)


def halves(a):
    high = a.astype(BF16)
    return high, (a - high.astype(F32)).astype(BF16)


def dot3(a, b, dims=NN):
    (ah, al), (bh, bl) = a, b
    return dot(ah, bh, dims) + (dot(ah, bl, dims) + dot(al, bh, dims))


def dot_exact_left(a, b):
    b1 = b.astype(BF16)
    rest = b - b1.astype(F32)
    b2 = rest.astype(BF16)
    b3 = (rest - b2.astype(F32)).astype(BF16)
    return dot(a, b1) + (dot(a, b2) + dot(a, b3))


def dot_exact_right(a, b):
    ah, al = halves(a)
    return dot(ah, b) + dot(al, b)


def iota(shape, dim):
    return lax.broadcasted_iota(jnp.int32, shape, dim)


def copy_to(src, dst, send_sem, recv_sem, device):
    return pltpu.make_async_remote_copy(
        src_ref=src,
        dst_ref=dst,
        send_sem=send_sem,
        recv_sem=recv_sem,
        device_id=device,
        device_id_type=MESH,
    )


def silu(v):
    return v / (1.0 + jnp.exp(-v))


def local_mixer(rec_ref, key_ref, val_ref, dec_ref, rate_ref, off_ref, xg, yf):
    n = 2 * CHUNK
    rows = rec_ref.shape[0]
    chunks = rows // CHUNK
    lane_head = iota((1, 128), 1) >> 6
    m0 = (lane_head == 0).astype(F32)
    m1 = 1.0 - m0
    same_head = ((iota((128, 128), 0) >> 6) == (iota((128, 128), 1) >> 6)).astype(BF16)
    i, j = iota((n, n), 0), iota((n, n), 1)
    eye = (i == j).astype(F32)
    same = (i >> 6) == (j >> 6)
    below = (i > j) & same
    upto = (i >= j) & same
    ri, rj = iota((rows, rows), 0), iota((rows, rows), 1)
    tri = ((ri >= rj) & ((ri >> 6) == (rj >> 6))).astype(F32).astype(BF16)

    key = key_ref[...].astype(F32)
    logw = -0.6065306597126334 / (1.0 + jnp.exp(-(off_ref[...] + dec_ref[...].astype(F32))))
    cum = dot_exact_left(tri, logw)
    rate = 1.0 / (1.0 + jnp.exp(-rate_ref[...].astype(F32)))
    unit = key * lax.rsqrt(dot_exact_right(key * key, same_head) + 1.0)
    b = unit * rate
    up = jnp.exp(cum)
    down = jnp.exp(-cum)
    u_t = unit * jnp.exp(cum - logw)
    r_t = rec_ref[...].astype(F32) * up
    k_t = key * down
    b_t = b * down
    value = val_ref[...].astype(F32)

    def part(a, at):
        return a[at * CHUNK : (at + 1) * CHUNK]

    def both(a):
        return jnp.concatenate([a * m0, a * m1], axis=0)

    every = range(chunks)
    end = [jnp.exp(part(cum, at)[CHUNK - 1 :]) for at in every]
    v2 = [both(part(value, at)) for at in every]
    v2h = [a.astype(BF16) for a in v2]
    u2 = [both(part(u_t, at)) for at in every]
    r2 = [both(part(r_t, at)) for at in every]
    b2 = [both(part(b_t, at)) for at in every]
    k2 = [both(part(k_t, at)) for at in every]
    left = [halves(jnp.concatenate([u2[at], r2[at]], axis=0)) for at in every]
    right = [halves(jnp.concatenate([b2[at], k2[at]], axis=0)) for at in every]
    pairs = [dot3(left[at], right[at], NT) for at in every]
    lower = [jnp.where(below, pairs[at][:n, :n], 0.0) for at in every]
    m_uk = [halves(jnp.where(below, pairs[at][:n, n:], 0.0)) for at in every]
    a_b = [halves(jnp.where(upto, pairs[at][n:, :n], 0.0)) for at in every]
    a_k = [halves(jnp.where(upto, pairs[at][n:, n:], 0.0)) for at in every]
    mv = [dot(m_uk[at][0], v2h[at]) + dot(m_uk[at][1], v2h[at]) for at in every]
    akv = [dot(a_k[at][0], v2h[at]) + dot(a_k[at][1], v2h[at]) for at in every]
    inverse = None
    for level in range(6):
        half = (
            ((i >> (level + 1)) == (j >> (level + 1)))
            & (((i >> level) & 1) == 1)
            & (((j >> level) & 1) == 0)
        )
        step = [jnp.where(half, lower[at], 0.0) for at in every]
        if inverse is None:
            inverse = [eye - step[at] for at in every]
        else:
            split = [halves(inverse[at]) for at in every]
            mid = [dot3(halves(step[at]), split[at]) for at in every]
            inverse = [
                inverse[at] - dot3(split[at], halves(mid[at])) for at in every
            ]
    ez = [
        halves(dot3(halves(inverse[at]), halves(jnp.concatenate([u2[at], mv[at]], axis=1))))
        for at in every
    ]
    aez = [dot3(a_b[at], ez[at]) for at in every]
    b_end = [halves(b2[at] * end[at]) for at in every]
    k_end = [halves(k2[at] * end[at]) for at in every]
    bez = [dot3(b_end[at], ez[at], TN) for at in every]
    kv = [dot(k_end[at][0], v2h[at], TN) + dot(k_end[at][1], v2h[at], TN) for at in every]
    total = None
    for at in every:
        xo = r2[at] - aez[at][:, :128]
        yo = akv[at] - aez[at][:, 128:]
        xo = xo[:CHUNK] + xo[CHUNK:]
        yo = yo[:CHUNK] + yo[CHUNK:]
        moves = eye * end[at] - bez[at][:, :128]
        sums = kv[at] - bez[at][:, 128:]
        if total is None:
            xg[pl.ds(at * CHUNK, CHUNK), :] = xo
            yf[pl.ds(at * CHUNK, CHUNK), :] = yo
            total = jnp.concatenate([moves, sums], axis=1)
        else:
            ahead = halves(total)
            read = dot3(halves(xo), ahead)
            xg[pl.ds(at * CHUNK, CHUNK), :] = read[:, :128]
            yf[pl.ds(at * CHUNK, CHUNK), :] = read[:, 128:] + yo
            moved = dot3(halves(moves), ahead)
            total = jnp.concatenate([moved[:, :128], moved[:, 128:] + sums], axis=1)
    return total[:, :128], total[:, 128:]


def kernel(*refs):
    (
        rec_in,
        key_in,
        val_in,
        dec_in,
        rate_in,
        gate_in,
        off_in,
        gain_in,
        self_in,
        wout_in,
        rows_in,
        idx_in,
        wgt_in,
        egain_in,
        eg_in,
        eu_in,
        ed_in,
        cg_in,
        cu_in,
        cd_in,
        out0,
        out1,
    ) = refs[:22]
    (
        rec_ref,
        key_ref,
        val_ref,
        dec_ref,
        rate_ref,
        gate_ref,
        off_ref,
        gain_ref,
        self_ref,
        rows_ref,
        idx_ref,
        wgt_ref,
        egain_ref,
        wout,
        gu,
        wd,
        cgu,
        cd,
        xn,
        sbuf,
        rbuf,
        hid,
        obuf,
        retb,
        pb0,
        pb1,
        qb0,
        qb1,
        gh0,
        gh1,
        gp0,
        gp1,
        gp2,
        gp3,
        shb,
        q_hi,
        q_lo,
        onehot,
        xg,
        yf,
        cmap,
        pmap,
        zmine,
        zmap,
        zlast,
        zall,
        sts,
        keep,
        ahead,
    ) = refs[22:71]
    (
        ld,
        dsp_s,
        dsp_r,
        ys,
        yr,
        ws,
        wr,
        hs,
        hr,
        ret_s,
        ret_r,
        rs_s,
        rs_h,
        rs_p,
        sh_s,
        sh_r,
        zs,
        zr,
        zls,
        zlr,
        ps,
        pr,
    ) = refs[71:]
    z, c = lax.axis_index("z"), lax.axis_index("c")
    y, x = lax.axis_index("y"), lax.axis_index("x")
    nz = lax.axis_size("z")
    ep, tp = 2 * z + c, RING * y + x
    home = ep % RING
    own = home == x
    mine = jnp.where(own, 1, 0)
    group, inner = z // RING, z % RING
    last = inner == RING - 1

    def at(z_=None, c_=None, y_=None, x_=None):
        return {
            "z": z if z_ is None else z_,
            "c": c if c_ is None else c_,
            "y": y if y_ is None else y_,
            "x": x if x_ is None else x_,
        }

    def place(e, y_=None, x_=None):
        return at(e // 2, e % 2, y_, x_)

    def whole(ref, send_sem, recv_sem):
        return copy_to(ref, ref, send_sem, recv_sem, at(c_=1 - c))

    loads = []
    for source, target in (
        (idx_in, idx_ref),
        (wgt_in, wgt_ref),
        (rows_in, rows_ref),
        (egain_in, egain_ref),
        (key_in, key_ref),
        (dec_in, dec_ref),
        (off_in, off_ref),
        (rate_in, rate_ref),
        (rec_in, rec_ref),
        (val_in, val_ref),
        (eg_in.at[0], gu.at[x, pl.ds(0, 64)]),
        (eu_in.at[0], gu.at[x, pl.ds(64, 64)]),
        (cg_in, cgu.at[pl.ds(0, 64)]),
        (cu_in, cgu.at[pl.ds(64, 64)]),
        (ed_in.at[0], wd.at[x]),
        (cd_in, cd),
        (wout_in, wout),
        (gate_in, gate_ref),
        (gain_in, gain_ref),
        (self_in, self_ref),
    ):
        count = len(loads)
        slot = count if count < 10 else 10 if count < 14 else 11 if count < 17 else count - 5
        loads.append(pltpu.make_async_copy(source, target, ld.at[slot]))
        loads[-1].start()

    barrier = pltpu.get_barrier_semaphore()

    def tell(device):
        pl.semaphore_signal(barrier, inc=1, device_id=device, device_id_type=MESH)

    def tell_source(k, _):
        source = RING * ((ep // RING + 4 + k) % SOURCES) + x

        @pl.when(source != ep)
        def _():
            tell(place(source))

        return 0

    lax.fori_loop(0, SOURCES, tell_source, 0)

    def tell_group(k, _):
        tell(at(z_=RING * group + k))
        return 0

    lax.fori_loop(0, inner, tell_group, 0)
    for k in range(1, RING):
        tell(at(x_=(x + k) % RING))
    for k in (1, 3):
        tell(at(y_=(y + k) % RING))
    tell(at(c_=1 - c))

    for load in loads[:2]:
        load.wait()
    row_count = rows_ref.shape[0]
    slots = EXPERTS * CAP
    expert_at = iota((EXPERTS, row_count), 0)
    chosen = jnp.zeros((EXPERTS, row_count), F32)
    weight = jnp.zeros((EXPERTS, row_count), F32)
    for k in range(4):
        hit = idx_ref[k : k + 1, :] == expert_at
        chosen = jnp.where(hit, 1.0, chosen)
        weight = jnp.where(hit, wgt_ref[k : k + 1, :], weight)
    earlier = iota((row_count, row_count), 0) < iota((row_count, row_count), 1)
    rank = dot(chosen.astype(BF16), earlier.astype(F32).astype(BF16))
    label = jnp.where(chosen > 0.0, rank, -1.0).astype(BF16)
    slot_s, slot_e = iota((slots, EXPERTS), 0), iota((slots, EXPERTS), 1)
    spread = ((slot_s >= slot_e * CAP) & (slot_s < slot_e * CAP + CAP)).astype(F32)
    within = jnp.sum(spread * (slot_s - slot_e * CAP).astype(F32), axis=1, keepdims=True)
    spread = spread.astype(BF16)
    placed = (dot(spread, label) == within).astype(F32)
    w_hi, w_lo = halves(weight)
    q_hi[...] = (placed * dot(spread, w_hi)).astype(BF16)
    q_lo[...] = (placed * dot(spread, w_lo)).astype(BF16)
    onehot[...] = placed.astype(BF16)

    for load in loads[2:4]:
        load.wait()
    rows = rows_ref[...].astype(F32)
    scale = lax.rsqrt(jnp.mean(rows * rows, axis=-1, keepdims=True) + 1.0)
    xn[...] = (rows * scale * egain_ref[...]).astype(BF16)

    @pl.when(own)
    def _():
        features = xn[:, pl.ds(pl.multiple_of(512 * y, 512), 512)]
        packed = dot(onehot[...], features)
        sbuf[...] = packed.reshape(EXPERTS, CAP, 512).astype(BF16)
        rbuf[y, ep // RING] = sbuf[ep]

    pltpu.make_async_copy(gu.at[pl.ds(0, 2)], gu.at[pl.ds(0, 2)], ld.at[10]).wait()

    pl.semaphore_wait(barrier, 5 + 1 + (3 - inner) + 31 * mine)

    def dispatch(e):
        return copy_to(
            sbuf.at[e], rbuf.at[y, ep // RING], dsp_s.at[0], dsp_r.at[ep // RING], place(e)
        )

    @pl.when(own)
    def _():
        dispatch((ep + 16) % EXPERTS).start()

        def send(k, _):
            dispatch((ep + 16 - k) % EXPERTS).start()
            dispatch((ep + 16 + k) % EXPERTS).start()
            return 0

        lax.fori_loop(1, 16, send, 0)

    def ring(piece, first_half, send_sem, passed_on, rest, axis):
        me = y if axis == "y" else x
        right, left = (me + 1) % RING, (me + 3) % RING

        def move(slot, way, to):
            device = at(y_=to) if axis == "y" else at(x_=to)
            recv_sem = passed_on if way == (0 if first_half else 1) else rest
            return copy_to(piece(slot), piece(slot), send_sem, recv_sem, device)

        def start(way):
            move(me, way, left if way else right).start()

        def relay():
            if first_half:
                move(left, 0, right).wait_recv()
                move(left, 2, right).start()
            else:
                move(right, 1, left).wait_recv()
                move(right, 2, left).start()

        return start, relay

    weights = [
        ring(lambda s: gu.at[s, pl.ds(0, 64)], True, ws.at[0], wr.at[0], wr.at[4], "x"),
        ring(lambda s: gu.at[s, pl.ds(64, 64)], False, ws.at[0], wr.at[1], wr.at[4], "x"),
        ring(lambda s: wd.at[s, pl.ds(0, 512)], True, ws.at[1], wr.at[2], wr.at[5], "x"),
        ring(lambda s: wd.at[s, pl.ds(512, 512)], False, ws.at[1], wr.at[3], wr.at[5], "x"),
    ]
    row_ring, row_from = [], []
    for j, away in enumerate((4, 3, 5, 2, 6, 1, 7, 0)):
        k = (ep // RING + away) % SOURCES
        row_ring.append(ring(lambda s, k=k: rbuf.at[s, k], j % 2 == 0, ys.at[0], yr.at[j], yr.at[8 + j // 4], "y"))
        row_from.append(k)
    hid_ring = [
        [
            ring(
                lambda s, h=h, p=p: hid.at[h, s, pl.ds(48 * p, 48)],
                p == 0,
                hs.at[h],
                hr.at[h, p],
                hr.at[h, 2],
                "y",
            )
            for p in range(2)
        ]
        for h in range(2)
    ]
    weights[0][0](0)
    weights[1][0](1)
    weights[1][0](0)
    weights[0][0](1)

    for load in loads[4:10]:
        load.wait()
    moves, sums = local_mixer(rec_ref, key_ref, val_ref, dec_ref, rate_ref, off_ref, xg, yf)
    cmap[0] = moves[:64] + pltpu.roll(sums[:64], 64, 1)
    cmap[1] = pltpu.roll(moves[64:], 64, 1) + sums[64:]
    swap = copy_to(cmap.at[1 - c], pmap, ps.at[0], pr.at[0], at(c_=1 - c))
    swap.start()

    pre = dot(cgu[...], xn[...], NT)
    shb[y, x] = (silu(pre[:64]) * pre[64:]).astype(BF16)
    share_x = [
        ring(lambda s: shb.at[y, s, pl.ds(0, 32)], True, sh_s.at[0], sh_r.at[0, 0], sh_r.at[0, 2], "x"),
        ring(lambda s: shb.at[y, s, pl.ds(32, 32)], False, sh_s.at[0], sh_r.at[0, 1], sh_r.at[0, 2], "x"),
    ]
    share_y = [
        ring(lambda s: shb.at[s, pl.ds(0, 2)], True, sh_s.at[1], sh_r.at[1, 0], sh_r.at[1, 2], "y"),
        ring(lambda s: shb.at[s, pl.ds(2, 2)], False, sh_s.at[1], sh_r.at[1, 1], sh_r.at[1, 2], "y"),
    ]

    def start_both(pair):
        pair[0][0](0)
        pair[1][0](1)
        pair[1][0](0)
        pair[0][0](1)

    start_both(share_x)

    swap.wait_recv()
    lane = iota((64, 128), 1)
    first = jnp.where(c == 0, cmap[0], pmap[...])
    second = jnp.where(c == 0, pmap[...], cmap[1])

    def compose(later, earlier):
        stacked = jnp.concatenate([earlier, jnp.zeros_like(earlier)], axis=0)
        moved = dot3(halves(jnp.where(lane < 64, later, 0.0)), halves(stacked))
        return moved + jnp.where(lane < 64, 0.0, later)

    zmine[...] = compose(second, first).astype(BF16)

    def to_group(k):
        return copy_to(zmine, zmap.at[inner], zs.at[k], zr.at[inner], at(z_=RING * group + k))

    def send_group(k, _):
        to_group(k).start()
        return 0

    lax.fori_loop(inner + 1, RING, send_group, 0)

    def forward_rows(j):
        k = row_from[j]

        def arrived():
            copy_to(
                rbuf.at[y, k], rbuf.at[y, k], dsp_s.at[0], dsp_r.at[k], place(RING * k + x)
            ).wait_recv()

        if j < SOURCES - 1:
            arrived()
        else:
            pl.when(jnp.logical_not(own))(arrived)

        row_ring[j][0](0)
        row_ring[j][0](1)

    weights[0][1]()
    weights[1][1]()
    for j in range(4):
        forward_rows(j)
    def advance(step):
        step = step.astype(F32)
        low = jnp.where(lane < 64, step, 0.0)
        twice = (low + pltpu.roll(low, 64, 1)).astype(BF16)
        k_hi, k_lo = halves(keep[...])
        moved = dot(twice, jnp.concatenate([k_hi, k_lo], axis=0))
        keep[...] = moved + jnp.where(lane < 64, 0.0, step)

    def in_group(k, _):
        copy_to(zmine, zmap.at[k], zs.at[0], zr.at[k], at(z_=RING * group + k)).wait_recv()
        advance(zmap[k])
        return 0

    def to_later(k):
        return copy_to(zlast, zall.at[group], zls.at[0], zlr.at[group], at(z_=k))

    keep[...] = (iota((64, 128), 0) == lane).astype(F32)
    lax.fori_loop(0, inner, in_group, 0)
    ahead[...] = keep[...]

    @pl.when(last)
    def _():
        advance(zmine[...])
        zlast[...] = keep[...].astype(BF16)

        def send_later(k, _):
            to_later(k).start()
            return 0

        lax.fori_loop(RING * (group + 1), nz, send_later, 0)

    for j in range(4, 8):
        forward_rows(j)
    pltpu.make_async_copy(wd, wd, ld.at[11]).wait()
    for load in loads[17:]:
        load.wait()
    weights[2][0](0)
    weights[3][0](1)
    weights[3][0](0)
    weights[2][0](1)

    for ring_of in row_ring:
        ring_of[1]()
    share_x[0][1]()
    share_x[1][1]()
    whole(gu.at[pl.ds(0, 2)], ws.at[0], wr.at[4]).wait_recv()

    def product(slot, h):
        taken = [rbuf[slot, row_from[j]].astype(F32) for j in range(4 * h, 4 * h + 4)]
        taken = jnp.concatenate(taken, axis=0).astype(BF16)
        span = pl.ds(pl.multiple_of(512 * slot, 512), 512)
        g = gu[:, 0:64, span].reshape(256, 512)
        u = gu[:, 64:128, span].reshape(256, 512)
        return dot(taken, g, NT), dot(taken, u, NT)

    for h in range(2):
        whole(rbuf.at[0], ys.at[0], yr.at[8 + h]).wait_recv()
        g0, u0 = product(y, h)
        g1, u1 = product((y + 1) % RING, h)
        g2, u2 = product((y + 3) % RING, h)
        g3, u3 = product((y + 2) % RING, h)
        hidden = silu((g0 + g1) + (g2 + g3)) * ((u0 + u1) + (u2 + u3))
        hid[h, y] = hidden.astype(BF16)
        start_both(hid_ring[h])
        if h == 0:
            weights[2][1]()
            weights[3][1]()

    def over_groups(k, _):
        copy_to(zlast, zall.at[k], zls.at[0], zlr.at[k], at(z_=RING * k + 3)).wait_recv()
        advance(zall[k])
        return 0

    keep[...] = jnp.zeros((64, 128), F32)
    lax.fori_loop(0, group, over_groups, 0)
    state = jnp.where(lane < 64, 0.0, compose(ahead[...], keep[...]))
    passed = jnp.where(lane < 64, 0.0, compose(first, state))
    sts[c] = jnp.where(c == 0, state, passed)
    keep[...] = jnp.where(c == 0, passed, state)
    hand = copy_to(keep, sts.at[c], ps.at[1], pr.at[1], at(c_=1 - c))
    hand.start()
    hid_ring[0][0][1]()
    hid_ring[0][1][1]()
    copy_to(keep, sts.at[1 - c], ps.at[1], pr.at[1], at(c_=1 - c)).wait_recv()

    start = jnp.concatenate([pltpu.roll(sts[0], 64, 1), sts[1]], axis=0)
    readout = dot3(halves(xg[...]), halves(start)) + yf[...]
    same_head = ((iota((128, 128), 0) >> 6) == (iota((128, 128), 1) >> 6)).astype(F32)
    mean_of = (same_head * (1.0 / HEAD)).astype(BF16)
    same_head = same_head.astype(BF16)
    centred = readout - dot_exact_right(readout, mean_of)
    variance = dot_exact_right(centred * centred, mean_of)
    key = key_ref[...].astype(F32)
    bonus = dot_exact_right(rec_ref[...].astype(F32) * key * self_ref[...], same_head)
    mixed = (
        centred * lax.rsqrt(variance + 1.0) * gain_ref[...] + bonus * val_ref[...].astype(F32)
    ) * gate_ref[...].astype(F32)
    mixed = mixed.astype(BF16)

    def reduce_along(n, axis, piece, half, got_half, got_piece):
        me = y if axis == "y" else x
        right, left, across = (me + 1) % RING, (me + 3) % RING, (me + 2) % RING

        def to(way):
            side = left if way else right
            return at(y_=side) if axis == "y" else at(x_=side)

        def far(way):
            return copy_to(
                half(across, way), got_half.at[way], rs_s.at[n], rs_h.at[n, way], to(way)
            )

        def near(way):
            block = piece(left if way else right)
            return copy_to(block, got_piece.at[way], rs_s.at[n], rs_p.at[n, way], to(way))

        def first():
            far(0).start()
            far(1).start()

        def second():
            for way in range(2):
                far(way).wait_recv()
                mine_half = half(left if way else right, way)
                mine_half[...] = (
                    mine_half[...].astype(F32) + got_half[way].astype(F32)
                ).astype(BF16)
                near(way).start()

        def third():
            near(0).wait_recv()
            near(1).wait_recv()
            own_block = piece(me)[...].astype(F32)
            return own_block + got_piece[0].astype(F32) + got_piece[1].astype(F32)

        return first, second, third

    x_first = reduce_along(
        0, "x", lambda t: pb0.at[t], lambda t, h: pb0.at[t, pl.ds(2 * h, 2)], gh0, gp0
    )
    y_first = reduce_along(
        1, "y", lambda t: pb1.at[t], lambda t, h: pb1.at[t, pl.ds(2 * h, 2)], gh1, gp1
    )
    def spread_along(n, axis, blocks, got):
        me = y if axis == "y" else x

        def start():
            for k in (2, 1, 3):
                to = (me + k) % RING
                device = at(y_=to) if axis == "y" else at(x_=to)
                copy_to(blocks.at[to], got.at[k - 1], rs_s.at[n], rs_h.at[n, 0], device).start()

        def finish():
            whole(got, rs_s.at[n], rs_h.at[n, 0]).wait_recv()
            total = blocks[me].astype(F32)
            for k in range(3):
                total = total + got[k].astype(F32)
            return total

        return start, finish

    y_then = spread_along(2, "y", qb0, gp2)
    x_then = spread_along(3, "x", qb1, gp3)

    for block in range(4):
        partial = dot(mixed[64 * block : 64 * block + 64], wout[...])
        partial = partial.reshape(4, 16, 2048).astype(BF16)
        pb1[block] = partial[:, :, 1024:]
        for side in range(4):
            pb0[side, block] = partial[side, :, :1024]
    hid_ring[1][0][1]()
    hid_ring[1][1][1]()
    x_first[0]()
    y_first[0]()

    whole(wd.at[pl.ds(0, 2)], ws.at[1], wr.at[5]).wait_recv()

    def give_back(j, s):
        return copy_to(
            obuf.at[s, j],
            retb.at[ep],
            ret_s.at[0],
            ret_r.at[0],
            place(RING * row_from[j] + x, x_=s),
        )

    def second_product(h):
        whole(hid.at[h, pl.ds(0, 2)], hs.at[h], hr.at[h, 2]).wait_recv()
        hidden = jnp.concatenate([hid[h, part] for part in range(RING)], axis=1)
        for s in range(RING):
            made = dot(hidden, wd[s])
            obuf[s, 4 * h : 4 * h + 4] = made.reshape(4, CAP, 128).astype(BF16)
            for j in range(4 * h, 4 * h + 4):
                back = give_back(j, s)
                if j < SOURCES - 1:
                    back.start()
                else:
                    pl.when(jnp.logical_not(own & (s == x)))(back.start)

    second_product(0)
    whole(shb.at[y, pl.ds(0, 2)], sh_s.at[0], sh_r.at[0, 2]).wait_recv()
    second_product(1)
    start_both(share_y)

    @pl.when(own)
    def _():
        retb[ep] = obuf[x, SOURCES - 1]

    x_first[1]()
    y_first[1]()
    qb0[...] = x_first[2]().astype(BF16)
    y_then[0]()
    qb1[...] = y_first[2]().astype(BF16)
    x_then[0]()
    share_y[0][1]()
    share_y[1][1]()
    out0[:, :1024] = y_then[1]().astype(BF16)
    out0[:, 1024:] = x_then[1]().astype(BF16)

    whole(shb.at[pl.ds(0, 2)], sh_s.at[1], sh_r.at[1, 2]).wait_recv()
    shared = dot(shb[...].reshape(1024, 128), cd[...], TN)

    @pl.when(own)
    def _():
        whole(sbuf.at[pl.ds(0, EXPERTS - 1)], dsp_s.at[0], dsp_r.at[0]).wait_send()

    for sent, sem in (
        (shb.at[y, pl.ds(0, 3)], sh_s.at[0]),
        (shb.at[pl.ds(0, 3)], sh_s.at[1]),
        (gu.at[pl.ds(0, 3)], ws.at[0]),
        (wd.at[pl.ds(0, 3)], ws.at[1]),
        (rbuf.at[pl.ds(0, 3)], ys.at[0]),
        (hid.at[0, pl.ds(0, 3)], hs.at[0]),
        (hid.at[1, pl.ds(0, 3)], hs.at[1]),
        (pb0.at[pl.ds(0, 3)], rs_s.at[0]),
        (pb1.at[pl.ds(0, 3)], rs_s.at[1]),
        (qb0.at[pl.ds(0, 3)], rs_s.at[2]),
        (qb1.at[pl.ds(0, 3)], rs_s.at[3]),
    ):
        whole(sent, sem, dsp_r.at[0]).wait_send()
    swap.wait_send()
    hand.wait_send()

    def group_sent(k, _):
        to_group(k).wait_send()
        return 0

    lax.fori_loop(inner + 1, RING, group_sent, 0)
    for k in range(RING - 1):
        @pl.when(last & (group == k))
        def _():
            maps = q_hi.at[pl.ds(0, 64 * (12 - 4 * k))]
            whole(maps, zls.at[0], zlr.at[0]).wait_send()

    @pl.when(own)
    def _():
        whole(retb.at[pl.ds(0, EXPERTS - 1)], ret_s.at[0], ret_r.at[0]).wait()

    @pl.when(jnp.logical_not(own))
    def _():
        whole(retb, ret_s.at[0], ret_r.at[0]).wait()

    copies = retb[...].astype(F32).reshape(slots, 128).astype(BF16)
    merged = dot(q_hi[...], copies, TN) + dot(q_lo[...], copies, TN) + shared
    out1[...] = merged.astype(BF16)


def on_device(
    receptance,
    key_tensor,
    value_tensor,
    decay_data_input,
    correction_rate_input,
    mixer_output_gate,
    decay_channel_offset,
    head_norm_gain,
    self_key_weight,
    mixer_output_weight,
    second_batch_rows,
    routed_expert_index,
    routing_output_weight,
    expert_norm_gain,
    expert_gate_weight,
    expert_up_weight,
    expert_down_weight,
    common_expert_gate,
    common_expert_up,
    common_expert_down,
):
    hbm = pl.BlockSpec(memory_space=pl.ANY)
    vmem = pl.BlockSpec(memory_space=pltpu.VMEM)
    dma = pltpu.SemaphoreType.DMA
    rows = receptance.shape[0]
    scratch = [
        *(pltpu.VMEM((rows, 128), BF16) for _ in range(6)),
        *(pltpu.VMEM((1, 128), F32) for _ in range(3)),
        pltpu.VMEM((128, 2048), BF16),
        pltpu.VMEM((4, 128), jnp.int32),
        pltpu.VMEM((4, 128), F32),
        pltpu.VMEM((1, 2048), F32),
        pltpu.VMEM((128, 2048), BF16),
        pltpu.VMEM((RING, 128, 2048), BF16),
        pltpu.VMEM((RING, 1024, 128), BF16),
        pltpu.VMEM((128, 2048), BF16),
        pltpu.VMEM((1024, 128), BF16),
        pltpu.VMEM((128, 2048), BF16),
        pltpu.VMEM((EXPERTS, CAP, 512), BF16),
        pltpu.VMEM((RING, SOURCES, CAP, 512), BF16),
        pltpu.VMEM((2, RING, SOURCES * CAP // 2, 256), BF16),
        pltpu.VMEM((RING, SOURCES, CAP, 128), BF16),
        pltpu.VMEM((EXPERTS, CAP, 128), BF16),
        pltpu.VMEM((RING, RING, 16, 1024), BF16),
        pltpu.VMEM((RING, RING, 16, 1024), BF16),
        pltpu.VMEM((RING, 16, 1024), BF16),
        pltpu.VMEM((RING, 16, 1024), BF16),
        pltpu.VMEM((2, 2, 16, 1024), BF16),
        pltpu.VMEM((2, 2, 16, 1024), BF16),
        pltpu.VMEM((2, RING, 16, 1024), BF16),
        pltpu.VMEM((2, RING, 16, 1024), BF16),
        pltpu.VMEM((3, 16, 1024), BF16),
        pltpu.VMEM((3, 16, 1024), BF16),
        pltpu.VMEM((RING, RING, 64, 128), BF16),
        pltpu.VMEM((EXPERTS * CAP, 128), BF16),
        pltpu.VMEM((EXPERTS * CAP, 128), BF16),
        pltpu.VMEM((EXPERTS * CAP, 128), BF16),
        pltpu.VMEM((256, 128), F32),
        pltpu.VMEM((256, 128), F32),
        pltpu.VMEM((2, 64, 128), F32),
        pltpu.VMEM((64, 128), F32),
        pltpu.VMEM((64, 128), BF16),
        pltpu.VMEM((RING, 64, 128), BF16),
        pltpu.VMEM((64, 128), BF16),
        pltpu.VMEM((RING, 64, 128), BF16),
        pltpu.VMEM((2, 64, 128), F32),
        pltpu.VMEM((64, 128), F32),
        pltpu.VMEM((64, 128), F32),
        dma((15,)),
        dma((1,)),
        dma((SOURCES,)),
        dma((1,)),
        dma((SOURCES + 2,)),
        dma((2,)),
        dma((6,)),
        dma((2,)),
        dma((2, 3)),
        dma((1,)),
        dma((1,)),
        dma((4,)),
        dma((4, 2)),
        dma((2, 2)),
        dma((2,)),
        dma((2, 3)),
        dma((RING,)),
        dma((RING,)),
        dma((1,)),
        dma((RING,)),
        dma((2,)),
        dma((2,)),
    ]
    return pl.pallas_call(
        kernel,
        out_shape=(
            pltpu.VMEM((16, 2048), BF16),
            pltpu.VMEM((128, 128), BF16),
        ),
        in_specs=[hbm] * 20,
        out_specs=(vmem, vmem),
        scratch_shapes=scratch,
        compiler_params=pltpu.CompilerParams(
            collective_id=0, has_side_effects=True, vmem_limit_bytes=60 * 1024 * 1024
        ),
        name="mixer_and_experts",
    )(
        receptance,
        key_tensor,
        value_tensor,
        decay_data_input,
        correction_rate_input,
        mixer_output_gate,
        decay_channel_offset.reshape(1, 128),
        head_norm_gain.reshape(1, 128),
        self_key_weight.reshape(1, 128),
        mixer_output_weight,
        second_batch_rows,
        routed_expert_index.T,
        routing_output_weight.T,
        expert_norm_gain.reshape(1, 2048),
        expert_gate_weight,
        expert_up_weight,
        expert_down_weight,
        common_expert_gate,
        common_expert_up,
        common_expert_down,
    )


def solution(mesh):
    split = Mesh(mesh.devices.reshape(16, 2, 4, 4), ("z", "c", "y", "x"))
    in_specs = (
        P(EP, TP),
        P(EP, TP),
        P(EP, TP),
        P(EP, TP),
        P(EP, TP),
        P(EP, TP),
        P(TP),
        P(TP),
        P(TP),
        P(TP, None),
        P(EP, None),
        P(EP, None),
        P(EP, None),
        P(),
        P(EP, TP, None),
        P(EP, TP, None),
        P(EP, None, TP),
        P(TP, None),
        P(TP, None),
        P(None, TP),
    )
    out_specs = (P(EP + TP, None), P(EP, TP))
    return jax.shard_map(
        on_device, mesh=split, in_specs=in_specs, out_specs=out_specs, check_vma=False
    )
```

```python
import functools

import jax
import jax.numpy as jnp
from jax import lax
from jax.experimental import pallas as pl
from jax.experimental.pallas import tpu as pltpu
from jax.sharding import Mesh
from jax.sharding import PartitionSpec as P

F32 = jnp.float32
BF16 = jnp.bfloat16
HEAD = 64
CHUNK = 64
RING = 4
CAP = 24
EXPERTS = 32
SOURCES = 8
MESH = pl.DeviceIdType.MESH
EP = ("z", "c")
TP = ("y", "x")
NN = (((1,), (0,)), ((), ()))
NT = (((1,), (1,)), ((), ()))
TN = (((0,), (0,)), ((), ()))


def dot(a, b, dims=NN):
    return lax.dot_general(a, b, dims, preferred_element_type=F32)


def halves(a):
    high = a.astype(BF16)
    return high, (a - high.astype(F32)).astype(BF16)


def dot3(a, b, dims=NN):
    (ah, al), (bh, bl) = a, b
    return dot(ah, bh, dims) + (dot(ah, bl, dims) + dot(al, bh, dims))


def dot_exact_left(a, b):
    b1 = b.astype(BF16)
    rest = b - b1.astype(F32)
    b2 = rest.astype(BF16)
    b3 = (rest - b2.astype(F32)).astype(BF16)
    return dot(a, b1) + (dot(a, b2) + dot(a, b3))


def dot_exact_right(a, b):
    ah, al = halves(a)
    return dot(ah, b) + dot(al, b)


def iota(shape, dim):
    return lax.broadcasted_iota(jnp.int32, shape, dim)


def copy_to(src, dst, send_sem, recv_sem, device):
    return pltpu.make_async_remote_copy(
        src_ref=src,
        dst_ref=dst,
        send_sem=send_sem,
        recv_sem=recv_sem,
        device_id=device,
        device_id_type=MESH,
    )


def silu(v):
    return v / (1.0 + jnp.exp(-v))


def local_mixer(rec_ref, key_ref, val_ref, dec_ref, rate_ref, off_ref, xg, yf):
    n = 2 * CHUNK
    rows = rec_ref.shape[0]
    chunks = rows // CHUNK
    lane_head = iota((1, 128), 1) >> 6
    m0 = (lane_head == 0).astype(F32)
    m1 = 1.0 - m0
    same_head = ((iota((128, 128), 0) >> 6) == (iota((128, 128), 1) >> 6)).astype(BF16)
    i, j = iota((n, n), 0), iota((n, n), 1)
    eye = (i == j).astype(F32)
    same = (i >> 6) == (j >> 6)
    below = (i > j) & same
    upto = (i >= j) & same
    ri, rj = iota((rows, rows), 0), iota((rows, rows), 1)
    tri = ((ri >= rj) & ((ri >> 6) == (rj >> 6))).astype(F32).astype(BF16)

    key = key_ref[...].astype(F32)
    logw = -0.6065306597126334 / (1.0 + jnp.exp(-(off_ref[...] + dec_ref[...].astype(F32))))
    cum = dot_exact_left(tri, logw)
    rate = 1.0 / (1.0 + jnp.exp(-rate_ref[...].astype(F32)))
    unit = key * lax.rsqrt(dot_exact_right(key * key, same_head) + 1.0)
    b = unit * rate
    up = jnp.exp(cum)
    down = jnp.exp(-cum)
    u_t = unit * jnp.exp(cum - logw)
    r_t = rec_ref[...].astype(F32) * up
    k_t = key * down
    b_t = b * down
    value = val_ref[...].astype(F32)

    def part(a, at):
        return a[at * CHUNK : (at + 1) * CHUNK]

    def both(a):
        return jnp.concatenate([a * m0, a * m1], axis=0)

    every = range(chunks)
    end = [jnp.exp(part(cum, at)[CHUNK - 1 :]) for at in every]
    v2 = [both(part(value, at)) for at in every]
    v2h = [a.astype(BF16) for a in v2]
    u2 = [both(part(u_t, at)) for at in every]
    r2 = [both(part(r_t, at)) for at in every]
    b2 = [both(part(b_t, at)) for at in every]
    k2 = [both(part(k_t, at)) for at in every]
    left = [halves(jnp.concatenate([u2[at], r2[at]], axis=0)) for at in every]
    right = [halves(jnp.concatenate([b2[at], k2[at]], axis=0)) for at in every]
    pairs = [dot3(left[at], right[at], NT) for at in every]
    lower = [jnp.where(below, pairs[at][:n, :n], 0.0) for at in every]
    m_uk = [halves(jnp.where(below, pairs[at][:n, n:], 0.0)) for at in every]
    a_b = [halves(jnp.where(upto, pairs[at][n:, :n], 0.0)) for at in every]
    a_k = [halves(jnp.where(upto, pairs[at][n:, n:], 0.0)) for at in every]
    mv = [dot(m_uk[at][0], v2h[at]) + dot(m_uk[at][1], v2h[at]) for at in every]
    akv = [dot(a_k[at][0], v2h[at]) + dot(a_k[at][1], v2h[at]) for at in every]
    inverse = None
    for level in range(6):
        half = (
            ((i >> (level + 1)) == (j >> (level + 1)))
            & (((i >> level) & 1) == 1)
            & (((j >> level) & 1) == 0)
        )
        step = [jnp.where(half, lower[at], 0.0) for at in every]
        if inverse is None:
            inverse = [eye - step[at] for at in every]
        else:
            split = [halves(inverse[at]) for at in every]
            mid = [dot3(halves(step[at]), split[at]) for at in every]
            inverse = [
                inverse[at] - dot3(split[at], halves(mid[at])) for at in every
            ]
    ez = [
        halves(dot3(halves(inverse[at]), halves(jnp.concatenate([u2[at], mv[at]], axis=1))))
        for at in every
    ]
    aez = [dot3(a_b[at], ez[at]) for at in every]
    b_end = [halves(b2[at] * end[at]) for at in every]
    k_end = [halves(k2[at] * end[at]) for at in every]
    bez = [dot3(b_end[at], ez[at], TN) for at in every]
    kv = [dot(k_end[at][0], v2h[at], TN) + dot(k_end[at][1], v2h[at], TN) for at in every]
    total = None
    for at in every:
        xo = r2[at] - aez[at][:, :128]
        yo = akv[at] - aez[at][:, 128:]
        xo = xo[:CHUNK] + xo[CHUNK:]
        yo = yo[:CHUNK] + yo[CHUNK:]
        moves = eye * end[at] - bez[at][:, :128]
        sums = kv[at] - bez[at][:, 128:]
        if total is None:
            xg[pl.ds(at * CHUNK, CHUNK), :] = xo
            yf[pl.ds(at * CHUNK, CHUNK), :] = yo
            total = jnp.concatenate([moves, sums], axis=1)
        else:
            ahead = halves(total)
            read = dot3(halves(xo), ahead)
            xg[pl.ds(at * CHUNK, CHUNK), :] = read[:, :128]
            yf[pl.ds(at * CHUNK, CHUNK), :] = read[:, 128:] + yo
            moved = dot3(halves(moves), ahead)
            total = jnp.concatenate([moved[:, :128], moved[:, 128:] + sums], axis=1)
    return total[:, :128], total[:, 128:]


def kernel(*refs):
    (
        rec_in,
        key_in,
        val_in,
        dec_in,
        rate_in,
        gate_in,
        off_in,
        gain_in,
        self_in,
        wout_in,
        rows_in,
        idx_in,
        wgt_in,
        egain_in,
        eg_in,
        eu_in,
        ed_in,
        cg_in,
        cu_in,
        cd_in,
        out0,
        out1,
    ) = refs[:22]
    (
        rec_ref,
        key_ref,
        val_ref,
        dec_ref,
        rate_ref,
        gate_ref,
        off_ref,
        gain_ref,
        self_ref,
        rows_ref,
        idx_ref,
        wgt_ref,
        egain_ref,
        wout,
        gu,
        wd,
        cgu,
        cd,
        xn,
        sbuf,
        rbuf,
        hid,
        obuf,
        retb,
        pb0,
        pb1,
        qb0,
        qb1,
        gh0,
        gh1,
        gp0,
        gp1,
        gp2,
        gp3,
        shb,
        q_hi,
        q_lo,
        onehot,
        xg,
        yf,
        cmap,
        pmap,
        zmine,
        zmap,
        zlast,
        zall,
        sts,
        keep,
        ahead,
    ) = refs[22:71]
    (
        ld,
        dsp_s,
        dsp_r,
        ys,
        yr,
        ws,
        wr,
        hs,
        hr,
        ret_s,
        ret_r,
        rs_s,
        rs_h,
        rs_p,
        sh_s,
        sh_r,
        zs,
        zr,
        zls,
        zlr,
        ps,
        pr,
    ) = refs[71:]
    z, c = lax.axis_index("z"), lax.axis_index("c")
    y, x = lax.axis_index("y"), lax.axis_index("x")
    nz = lax.axis_size("z")
    ep, tp = 2 * z + c, RING * y + x
    home = ep % RING
    own = home == x
    mine = jnp.where(own, 1, 0)
    group, inner = z // RING, z % RING
    last = inner == RING - 1

    def at(z_=None, c_=None, y_=None, x_=None):
        return {
            "z": z if z_ is None else z_,
            "c": c if c_ is None else c_,
            "y": y if y_ is None else y_,
            "x": x if x_ is None else x_,
        }

    def place(e, y_=None, x_=None):
        return at(e // 2, e % 2, y_, x_)

    def whole(ref, send_sem, recv_sem):
        return copy_to(ref, ref, send_sem, recv_sem, at(c_=1 - c))

    loads = []
    for source, target in (
        (idx_in, idx_ref),
        (wgt_in, wgt_ref),
        (rows_in, rows_ref),
        (egain_in, egain_ref),
        (key_in, key_ref),
        (dec_in, dec_ref),
        (off_in, off_ref),
        (rate_in, rate_ref),
        (rec_in, rec_ref),
        (val_in, val_ref),
        (eg_in.at[0], gu.at[x, pl.ds(0, 64)]),
        (eu_in.at[0], gu.at[x, pl.ds(64, 64)]),
        (cg_in, cgu.at[pl.ds(0, 64)]),
        (cu_in, cgu.at[pl.ds(64, 64)]),
        (ed_in.at[0], wd.at[x]),
        (cd_in, cd),
        (wout_in, wout),
        (gate_in, gate_ref),
        (gain_in, gain_ref),
        (self_in, self_ref),
    ):
        count = len(loads)
        slot = count if count < 10 else 10 if count < 14 else 11 if count < 17 else count - 5
        loads.append(pltpu.make_async_copy(source, target, ld.at[slot]))
        loads[-1].start()

    barrier = pltpu.get_barrier_semaphore()

    def tell(device):
        pl.semaphore_signal(barrier, inc=1, device_id=device, device_id_type=MESH)

    def tell_source(k, _):
        source = RING * ((ep // RING + 4 + k) % SOURCES) + x

        @pl.when(source != ep)
        def _():
            tell(place(source))

        return 0

    lax.fori_loop(0, SOURCES, tell_source, 0)

    def tell_group(k, _):
        tell(at(z_=RING * group + k))
        return 0

    lax.fori_loop(0, inner, tell_group, 0)
    for k in range(1, RING):
        tell(at(x_=(x + k) % RING))
    for k in (1, 3):
        tell(at(y_=(y + k) % RING))
    tell(at(c_=1 - c))

    for load in loads[:2]:
        load.wait()
    row_count = rows_ref.shape[0]
    slots = EXPERTS * CAP
    expert_at = iota((EXPERTS, row_count), 0)
    chosen = jnp.zeros((EXPERTS, row_count), F32)
    weight = jnp.zeros((EXPERTS, row_count), F32)
    for k in range(4):
        hit = idx_ref[k : k + 1, :] == expert_at
        chosen = jnp.where(hit, 1.0, chosen)
        weight = jnp.where(hit, wgt_ref[k : k + 1, :], weight)
    earlier = iota((row_count, row_count), 0) < iota((row_count, row_count), 1)
    rank = dot(chosen.astype(BF16), earlier.astype(F32).astype(BF16))
    label = jnp.where(chosen > 0.0, rank, -1.0).astype(BF16)
    slot_s, slot_e = iota((slots, EXPERTS), 0), iota((slots, EXPERTS), 1)
    spread = ((slot_s >= slot_e * CAP) & (slot_s < slot_e * CAP + CAP)).astype(F32)
    within = jnp.sum(spread * (slot_s - slot_e * CAP).astype(F32), axis=1, keepdims=True)
    spread = spread.astype(BF16)
    placed = (dot(spread, label) == within).astype(F32)
    w_hi, w_lo = halves(weight)
    q_hi[...] = (placed * dot(spread, w_hi)).astype(BF16)
    q_lo[...] = (placed * dot(spread, w_lo)).astype(BF16)
    onehot[...] = placed.astype(BF16)

    for load in loads[2:4]:
        load.wait()
    rows = rows_ref[...].astype(F32)
    scale = lax.rsqrt(jnp.mean(rows * rows, axis=-1, keepdims=True) + 1.0)
    xn[...] = (rows * scale * egain_ref[...]).astype(BF16)

    @pl.when(own)
    def _():
        features = xn[:, pl.ds(pl.multiple_of(512 * y, 512), 512)]
        packed = dot(onehot[...], features)
        sbuf[...] = packed.reshape(EXPERTS, CAP, 512).astype(BF16)
        rbuf[y, ep // RING] = sbuf[ep]

    pltpu.make_async_copy(gu.at[pl.ds(0, 2)], gu.at[pl.ds(0, 2)], ld.at[10]).wait()

    pl.semaphore_wait(barrier, 5 + 1 + (3 - inner) + 31 * mine)

    def dispatch(e):
        return copy_to(
            sbuf.at[e], rbuf.at[y, ep // RING], dsp_s.at[0], dsp_r.at[ep // RING], place(e)
        )

    @pl.when(own)
    def _():
        dispatch((ep + 16) % EXPERTS).start()

        def send(k, _):
            dispatch((ep + 16 - k) % EXPERTS).start()
            dispatch((ep + 16 + k) % EXPERTS).start()
            return 0

        lax.fori_loop(1, 16, send, 0)

    def ring(piece, first_half, send_sem, passed_on, rest, axis):
        me = y if axis == "y" else x
        right, left = (me + 1) % RING, (me + 3) % RING

        def move(slot, way, to):
            device = at(y_=to) if axis == "y" else at(x_=to)
            recv_sem = passed_on if way == (0 if first_half else 1) else rest
            return copy_to(piece(slot), piece(slot), send_sem, recv_sem, device)

        def start(way):
            move(me, way, left if way else right).start()

        def relay():
            if first_half:
                move(left, 0, right).wait_recv()
                move(left, 2, right).start()
            else:
                move(right, 1, left).wait_recv()
                move(right, 2, left).start()

        return start, relay

    weights = [
        ring(lambda s: gu.at[s, pl.ds(0, 64)], True, ws.at[0], wr.at[0], wr.at[4], "x"),
        ring(lambda s: gu.at[s, pl.ds(64, 64)], False, ws.at[0], wr.at[1], wr.at[4], "x"),
        ring(lambda s: wd.at[s, pl.ds(0, 512)], True, ws.at[1], wr.at[2], wr.at[5], "x"),
        ring(lambda s: wd.at[s, pl.ds(512, 512)], False, ws.at[1], wr.at[3], wr.at[5], "x"),
    ]
    row_ring, row_from = [], []
    for j, away in enumerate((4, 3, 5, 2, 6, 1, 7, 0)):
        k = (ep // RING + away) % SOURCES
        row_ring.append(ring(lambda s, k=k: rbuf.at[s, k], j % 2 == 0, ys.at[0], yr.at[j], yr.at[8 + j // 4], "y"))
        row_from.append(k)
    hid_ring = [
        [
            ring(
                lambda s, h=h, p=p: hid.at[h, s, pl.ds(48 * p, 48)],
                p == 0,
                hs.at[h],
                hr.at[h, p],
                hr.at[h, 2],
                "y",
            )
            for p in range(2)
        ]
        for h in range(2)
    ]
    weights[0][0](0)
    weights[1][0](1)
    weights[1][0](0)
    weights[0][0](1)

    for load in loads[4:10]:
        load.wait()
    moves, sums = local_mixer(rec_ref, key_ref, val_ref, dec_ref, rate_ref, off_ref, xg, yf)
    cmap[0] = moves[:64] + pltpu.roll(sums[:64], 64, 1)
    cmap[1] = pltpu.roll(moves[64:], 64, 1) + sums[64:]
    swap = copy_to(cmap.at[1 - c], pmap, ps.at[0], pr.at[0], at(c_=1 - c))
    swap.start()

    pre = dot(cgu[...], xn[...], NT)
    shb[y, x] = (silu(pre[:64]) * pre[64:]).astype(BF16)
    share_x = [
        ring(lambda s: shb.at[y, s, pl.ds(0, 32)], True, sh_s.at[0], sh_r.at[0, 0], sh_r.at[0, 2], "x"),
        ring(lambda s: shb.at[y, s, pl.ds(32, 32)], False, sh_s.at[0], sh_r.at[0, 1], sh_r.at[0, 2], "x"),
    ]
    share_y = [
        ring(lambda s: shb.at[s, pl.ds(0, 2)], True, sh_s.at[1], sh_r.at[1, 0], sh_r.at[1, 2], "y"),
        ring(lambda s: shb.at[s, pl.ds(2, 2)], False, sh_s.at[1], sh_r.at[1, 1], sh_r.at[1, 2], "y"),
    ]

    def start_both(pair):
        pair[0][0](0)
        pair[1][0](1)
        pair[1][0](0)
        pair[0][0](1)

    start_both(share_x)

    swap.wait_recv()
    lane = iota((64, 128), 1)
    first = jnp.where(c == 0, cmap[0], pmap[...])
    second = jnp.where(c == 0, pmap[...], cmap[1])

    def compose(later, earlier):
        stacked = jnp.concatenate([earlier, jnp.zeros_like(earlier)], axis=0)
        moved = dot3(halves(jnp.where(lane < 64, later, 0.0)), halves(stacked))
        return moved + jnp.where(lane < 64, 0.0, later)

    zmine[...] = compose(second, first).astype(BF16)

    def to_group(k):
        return copy_to(zmine, zmap.at[inner], zs.at[k], zr.at[inner], at(z_=RING * group + k))

    def send_group(k, _):
        to_group(k).start()
        return 0

    lax.fori_loop(inner + 1, RING, send_group, 0)

    def forward_rows(j):
        k = row_from[j]

        def arrived():
            copy_to(
                rbuf.at[y, k], rbuf.at[y, k], dsp_s.at[0], dsp_r.at[k], place(RING * k + x)
            ).wait_recv()

        if j < SOURCES - 1:
            arrived()
        else:
            pl.when(jnp.logical_not(own))(arrived)

        row_ring[j][0](0)
        row_ring[j][0](1)

    weights[0][1]()
    weights[1][1]()
    for j in range(4):
        forward_rows(j)
    def advance(step):
        step = step.astype(F32)
        low = jnp.where(lane < 64, step, 0.0)
        twice = (low + pltpu.roll(low, 64, 1)).astype(BF16)
        k_hi, k_lo = halves(keep[...])
        moved = dot(twice, jnp.concatenate([k_hi, k_lo], axis=0))
        keep[...] = moved + jnp.where(lane < 64, 0.0, step)

    def in_group(k, _):
        copy_to(zmine, zmap.at[k], zs.at[0], zr.at[k], at(z_=RING * group + k)).wait_recv()
        advance(zmap[k])
        return 0

    def to_later(k):
        return copy_to(zlast, zall.at[group], zls.at[0], zlr.at[group], at(z_=k))

    keep[...] = (iota((64, 128), 0) == lane).astype(F32)
    lax.fori_loop(0, inner, in_group, 0)
    ahead[...] = keep[...]

    @pl.when(last)
    def _():
        advance(zmine[...])
        zlast[...] = keep[...].astype(BF16)

        def send_later(k, _):
            to_later(k).start()
            return 0

        lax.fori_loop(RING * (group + 1), nz, send_later, 0)

    for j in range(4, 8):
        forward_rows(j)
    pltpu.make_async_copy(wd, wd, ld.at[11]).wait()
    for load in loads[17:]:
        load.wait()
    weights[2][0](0)
    weights[3][0](1)
    weights[3][0](0)
    weights[2][0](1)

    for ring_of in row_ring:
        ring_of[1]()
    share_x[0][1]()
    share_x[1][1]()
    whole(gu.at[pl.ds(0, 2)], ws.at[0], wr.at[4]).wait_recv()

    def product(slot, h):
        taken = [rbuf[slot, row_from[j]].astype(F32) for j in range(4 * h, 4 * h + 4)]
        taken = jnp.concatenate(taken, axis=0).astype(BF16)
        span = pl.ds(pl.multiple_of(512 * slot, 512), 512)
        g = gu[:, 0:64, span].reshape(256, 512)
        u = gu[:, 64:128, span].reshape(256, 512)
        return dot(taken, g, NT), dot(taken, u, NT)

    for h in range(2):
        whole(rbuf.at[0], ys.at[0], yr.at[8 + h]).wait_recv()
        g0, u0 = product(y, h)
        g1, u1 = product((y + 1) % RING, h)
        g2, u2 = product((y + 3) % RING, h)
        g3, u3 = product((y + 2) % RING, h)
        hidden = silu((g0 + g1) + (g2 + g3)) * ((u0 + u1) + (u2 + u3))
        hid[h, y] = hidden.astype(BF16)
        start_both(hid_ring[h])
        if h == 0:
            weights[2][1]()
            weights[3][1]()

    def over_groups(k, _):
        copy_to(zlast, zall.at[k], zls.at[0], zlr.at[k], at(z_=RING * k + 3)).wait_recv()
        advance(zall[k])
        return 0

    keep[...] = jnp.zeros((64, 128), F32)
    lax.fori_loop(0, group, over_groups, 0)
    state = jnp.where(lane < 64, 0.0, compose(ahead[...], keep[...]))
    passed = jnp.where(lane < 64, 0.0, compose(first, state))
    sts[c] = jnp.where(c == 0, state, passed)
    keep[...] = jnp.where(c == 0, passed, state)
    hand = copy_to(keep, sts.at[c], ps.at[1], pr.at[1], at(c_=1 - c))
    hand.start()
    hid_ring[0][0][1]()
    hid_ring[0][1][1]()
    copy_to(keep, sts.at[1 - c], ps.at[1], pr.at[1], at(c_=1 - c)).wait_recv()

    hid_ring[1][0][1]()
    hid_ring[1][1][1]()
    start = jnp.concatenate([pltpu.roll(sts[0], 64, 1), sts[1]], axis=0)
    readout = dot3(halves(xg[...]), halves(start)) + yf[...]
    same_head = ((iota((128, 128), 0) >> 6) == (iota((128, 128), 1) >> 6)).astype(F32)
    mean_of = (same_head * (1.0 / HEAD)).astype(BF16)
    same_head = same_head.astype(BF16)
    centred = readout - dot_exact_right(readout, mean_of)
    variance = dot_exact_right(centred * centred, mean_of)
    key = key_ref[...].astype(F32)
    bonus = dot_exact_right(rec_ref[...].astype(F32) * key * self_ref[...], same_head)
    mixed = (
        centred * lax.rsqrt(variance + 1.0) * gain_ref[...] + bonus * val_ref[...].astype(F32)
    ) * gate_ref[...].astype(F32)
    mixed = mixed.astype(BF16)

    def reduce_along(n, axis, piece, half, got_half, got_piece):
        me = y if axis == "y" else x
        right, left, across = (me + 1) % RING, (me + 3) % RING, (me + 2) % RING

        def to(way):
            side = left if way else right
            return at(y_=side) if axis == "y" else at(x_=side)

        def far(way):
            return copy_to(
                half(across, way), got_half.at[way], rs_s.at[n], rs_h.at[n, way], to(way)
            )

        def near(way):
            block = piece(left if way else right)
            return copy_to(block, got_piece.at[way], rs_s.at[n], rs_p.at[n, way], to(way))

        def first():
            far(0).start()
            far(1).start()

        def second():
            for way in range(2):
                far(way).wait_recv()
                mine_half = half(left if way else right, way)
                mine_half[...] = (
                    mine_half[...].astype(F32) + got_half[way].astype(F32)
                ).astype(BF16)
                near(way).start()

        def third():
            near(0).wait_recv()
            near(1).wait_recv()
            own_block = piece(me)[...].astype(F32)
            return own_block + got_piece[0].astype(F32) + got_piece[1].astype(F32)

        return first, second, third

    x_first = reduce_along(
        0, "x", lambda t: pb0.at[t], lambda t, h: pb0.at[t, pl.ds(2 * h, 2)], gh0, gp0
    )
    y_first = reduce_along(
        1, "y", lambda t: pb1.at[t], lambda t, h: pb1.at[t, pl.ds(2 * h, 2)], gh1, gp1
    )
    def spread_along(n, axis, blocks, got):
        me = y if axis == "y" else x

        def start():
            for k in (2, 1, 3):
                to = (me + k) % RING
                device = at(y_=to) if axis == "y" else at(x_=to)
                copy_to(blocks.at[to], got.at[k - 1], rs_s.at[n], rs_h.at[n, 0], device).start()

        def finish():
            whole(got, rs_s.at[n], rs_h.at[n, 0]).wait_recv()
            total = blocks[me].astype(F32)
            for k in range(3):
                total = total + got[k].astype(F32)
            return total

        return start, finish

    y_then = spread_along(2, "y", qb0, gp2)
    x_then = spread_along(3, "x", qb1, gp3)

    for block in range(4):
        partial = dot(mixed[64 * block : 64 * block + 64], wout[...])
        partial = partial.reshape(4, 16, 2048).astype(BF16)
        pb1[block] = partial[:, :, 1024:]
        for side in range(4):
            pb0[side, block] = partial[side, :, :1024]
    x_first[0]()
    y_first[0]()

    whole(wd.at[pl.ds(0, 2)], ws.at[1], wr.at[5]).wait_recv()

    def give_back(j, s):
        return copy_to(
            obuf.at[s, j],
            retb.at[ep],
            ret_s.at[0],
            ret_r.at[0],
            place(RING * row_from[j] + x, x_=s),
        )

    def second_product(h):
        whole(hid.at[h, pl.ds(0, 2)], hs.at[h], hr.at[h, 2]).wait_recv()
        hidden = jnp.concatenate([hid[h, part] for part in range(RING)], axis=1)
        for s in range(RING):
            made = dot(hidden, wd[s])
            obuf[s, 4 * h : 4 * h + 4] = made.reshape(4, CAP, 128).astype(BF16)
            for j in range(4 * h, 4 * h + 4):
                back = give_back(j, s)
                if j < SOURCES - 1:
                    back.start()
                else:
                    pl.when(jnp.logical_not(own & (s == x)))(back.start)

    second_product(0)
    whole(shb.at[y, pl.ds(0, 2)], sh_s.at[0], sh_r.at[0, 2]).wait_recv()
    second_product(1)
    start_both(share_y)

    @pl.when(own)
    def _():
        retb[ep] = obuf[x, SOURCES - 1]

    x_first[1]()
    y_first[1]()
    qb0[...] = x_first[2]().astype(BF16)
    y_then[0]()
    qb1[...] = y_first[2]().astype(BF16)
    x_then[0]()
    share_y[0][1]()
    share_y[1][1]()
    out0[:, :1024] = y_then[1]().astype(BF16)
    out0[:, 1024:] = x_then[1]().astype(BF16)

    whole(shb.at[pl.ds(0, 2)], sh_s.at[1], sh_r.at[1, 2]).wait_recv()
    shared = dot(shb[...].reshape(1024, 128), cd[...], TN)

    @pl.when(own)
    def _():
        whole(sbuf.at[pl.ds(0, EXPERTS - 1)], dsp_s.at[0], dsp_r.at[0]).wait_send()

    for sent, sem in (
        (shb.at[y, pl.ds(0, 3)], sh_s.at[0]),
        (shb.at[pl.ds(0, 3)], sh_s.at[1]),
        (gu.at[pl.ds(0, 3)], ws.at[0]),
        (wd.at[pl.ds(0, 3)], ws.at[1]),
        (rbuf.at[pl.ds(0, 3)], ys.at[0]),
        (hid.at[0, pl.ds(0, 3)], hs.at[0]),
        (hid.at[1, pl.ds(0, 3)], hs.at[1]),
        (pb0.at[pl.ds(0, 3)], rs_s.at[0]),
        (pb1.at[pl.ds(0, 3)], rs_s.at[1]),
        (qb0.at[pl.ds(0, 3)], rs_s.at[2]),
        (qb1.at[pl.ds(0, 3)], rs_s.at[3]),
    ):
        whole(sent, sem, dsp_r.at[0]).wait_send()
    swap.wait_send()
    hand.wait_send()

    def group_sent(k, _):
        to_group(k).wait_send()
        return 0

    lax.fori_loop(inner + 1, RING, group_sent, 0)
    for k in range(RING - 1):
        @pl.when(last & (group == k))
        def _():
            maps = q_hi.at[pl.ds(0, 64 * (12 - 4 * k))]
            whole(maps, zls.at[0], zlr.at[0]).wait_send()

    @pl.when(own)
    def _():
        whole(retb.at[pl.ds(0, EXPERTS - 1)], ret_s.at[0], ret_r.at[0]).wait()

    @pl.when(jnp.logical_not(own))
    def _():
        whole(retb, ret_s.at[0], ret_r.at[0]).wait()

    copies = retb[...].astype(F32).reshape(slots, 128).astype(BF16)
    merged = dot(q_hi[...], copies, TN) + dot(q_lo[...], copies, TN) + shared
    out1[...] = merged.astype(BF16)


def on_device(
    receptance,
    key_tensor,
    value_tensor,
    decay_data_input,
    correction_rate_input,
    mixer_output_gate,
    decay_channel_offset,
    head_norm_gain,
    self_key_weight,
    mixer_output_weight,
    second_batch_rows,
    routed_expert_index,
    routing_output_weight,
    expert_norm_gain,
    expert_gate_weight,
    expert_up_weight,
    expert_down_weight,
    common_expert_gate,
    common_expert_up,
    common_expert_down,
):
    hbm = pl.BlockSpec(memory_space=pl.ANY)
    vmem = pl.BlockSpec(memory_space=pltpu.VMEM)
    dma = pltpu.SemaphoreType.DMA
    rows = receptance.shape[0]
    scratch = [
        *(pltpu.VMEM((rows, 128), BF16) for _ in range(6)),
        *(pltpu.VMEM((1, 128), F32) for _ in range(3)),
        pltpu.VMEM((128, 2048), BF16),
        pltpu.VMEM((4, 128), jnp.int32),
        pltpu.VMEM((4, 128), F32),
        pltpu.VMEM((1, 2048), F32),
        pltpu.VMEM((128, 2048), BF16),
        pltpu.VMEM((RING, 128, 2048), BF16),
        pltpu.VMEM((RING, 1024, 128), BF16),
        pltpu.VMEM((128, 2048), BF16),
        pltpu.VMEM((1024, 128), BF16),
        pltpu.VMEM((128, 2048), BF16),
        pltpu.VMEM((EXPERTS, CAP, 512), BF16),
        pltpu.VMEM((RING, SOURCES, CAP, 512), BF16),
        pltpu.VMEM((2, RING, SOURCES * CAP // 2, 256), BF16),
        pltpu.VMEM((RING, SOURCES, CAP, 128), BF16),
        pltpu.VMEM((EXPERTS, CAP, 128), BF16),
        pltpu.VMEM((RING, RING, 16, 1024), BF16),
        pltpu.VMEM((RING, RING, 16, 1024), BF16),
        pltpu.VMEM((RING, 16, 1024), BF16),
        pltpu.VMEM((RING, 16, 1024), BF16),
        pltpu.VMEM((2, 2, 16, 1024), BF16),
        pltpu.VMEM((2, 2, 16, 1024), BF16),
        pltpu.VMEM((2, RING, 16, 1024), BF16),
        pltpu.VMEM((2, RING, 16, 1024), BF16),
        pltpu.VMEM((3, 16, 1024), BF16),
        pltpu.VMEM((3, 16, 1024), BF16),
        pltpu.VMEM((RING, RING, 64, 128), BF16),
        pltpu.VMEM((EXPERTS * CAP, 128), BF16),
        pltpu.VMEM((EXPERTS * CAP, 128), BF16),
        pltpu.VMEM((EXPERTS * CAP, 128), BF16),
        pltpu.VMEM((256, 128), F32),
        pltpu.VMEM((256, 128), F32),
        pltpu.VMEM((2, 64, 128), F32),
        pltpu.VMEM((64, 128), F32),
        pltpu.VMEM((64, 128), BF16),
        pltpu.VMEM((RING, 64, 128), BF16),
        pltpu.VMEM((64, 128), BF16),
        pltpu.VMEM((RING, 64, 128), BF16),
        pltpu.VMEM((2, 64, 128), F32),
        pltpu.VMEM((64, 128), F32),
        pltpu.VMEM((64, 128), F32),
        dma((15,)),
        dma((1,)),
        dma((SOURCES,)),
        dma((1,)),
        dma((SOURCES + 2,)),
        dma((2,)),
        dma((6,)),
        dma((2,)),
        dma((2, 3)),
        dma((1,)),
        dma((1,)),
        dma((4,)),
        dma((4, 2)),
        dma((2, 2)),
        dma((2,)),
        dma((2, 3)),
        dma((RING,)),
        dma((RING,)),
        dma((1,)),
        dma((RING,)),
        dma((2,)),
        dma((2,)),
    ]
    return pl.pallas_call(
        kernel,
        out_shape=(
            pltpu.VMEM((16, 2048), BF16),
            pltpu.VMEM((128, 128), BF16),
        ),
        in_specs=[hbm] * 20,
        out_specs=(vmem, vmem),
        scratch_shapes=scratch,
        compiler_params=pltpu.CompilerParams(
            collective_id=0, has_side_effects=True, vmem_limit_bytes=60 * 1024 * 1024
        ),
        name="mixer_and_experts",
    )(
        receptance,
        key_tensor,
        value_tensor,
        decay_data_input,
        correction_rate_input,
        mixer_output_gate,
        decay_channel_offset.reshape(1, 128),
        head_norm_gain.reshape(1, 128),
        self_key_weight.reshape(1, 128),
        mixer_output_weight,
        second_batch_rows,
        routed_expert_index.T,
        routing_output_weight.T,
        expert_norm_gain.reshape(1, 2048),
        expert_gate_weight,
        expert_up_weight,
        expert_down_weight,
        common_expert_gate,
        common_expert_up,
        common_expert_down,
    )


def solution(mesh):
    split = Mesh(mesh.devices.reshape(16, 2, 4, 4), ("z", "c", "y", "x"))
    in_specs = (
        P(EP, TP),
        P(EP, TP),
        P(EP, TP),
        P(EP, TP),
        P(EP, TP),
        P(EP, TP),
        P(TP),
        P(TP),
        P(TP),
        P(TP, None),
        P(EP, None),
        P(EP, None),
        P(EP, None),
        P(),
        P(EP, TP, None),
        P(EP, TP, None),
        P(EP, None, TP),
        P(TP, None),
        P(TP, None),
        P(None, TP),
    )
    out_specs = (P(EP + TP, None), P(EP, TP))
    return jax.shard_map(
        on_device, mesh=split, in_specs=in_specs, out_specs=out_specs, check_vma=False
    )
```
